32 devices in a mesh: sp: 4 (over z), fs: 4 (over y, x), tp: 2 (over core).
Axes of the slice: x: 2, y: 2, z: 4, core: 2. Of those that a mesh axis runs over, the one named last changes fastest.
Arguments:
- tokens: bfloat16 [4, 512, 4096], P('fs', 'sp', 'tp'), may hold values from -6 to 6
- norm_gain: float32 [4096], replicated, may hold values from 0.1 to 1.9
- w_state_in: bfloat16 [4096, 2048], P(('sp', 'fs'), 'tp'), may hold values from -0.09375 to 0.09375
- w_query: bfloat16 [4096, 2048], P(('sp', 'fs'), 'tp'), may hold values from -0.3125 to 0.3125
- w_key: bfloat16 [4096, 2048], P(('sp', 'fs'), 'tp'), may hold values from -0.3125 to 0.3125
- w_value: bfloat16 [4096, 2048], P(('sp', 'fs'), 'tp'), may hold values from -0.09375 to 0.09375
- decay_re: float32 [128, 64], P('tp'), may hold values from -0.034 to -9.765625e-05
- decay_im: float32 [128, 64], P('tp'), may hold values from -3.140625 to 3.140625
- log_step: float32 [128], P('tp'), may hold values from -3.5 to -1.5
- decay_shift: float32 [4, 128, 512], P('fs', 'tp', 'sp'), may hold values from -2 to 0
- in_re: float32 [128, 64, 16], P('tp'), may hold values from -2 to 2
- in_im: float32 [128, 64, 16], P('tp'), may hold values from -2 to 2
- output_real: float32 [128, 16, 64], P('tp'), may hold values from -0.75 to 0.75
- output_imaginary: float32 [128, 16, 64], P('tp'), may hold values from -0.75 to 0.75
- skip: float32 [2048], P('tp'), may hold values from -1.2 to 1.2
- mix_weight: float32 [8], P('tp'), may hold values from 0.3 to 0.8
- head_gain: float32 [256], replicated, may hold values from 0.1 to 1.9
- w_out_state: bfloat16 [2048, 4096], P('tp'), may hold values from -0.125 to 0.125
- w_out_attn: bfloat16 [2048, 4096], P('tp'), may hold values from -0.125 to 0.125
Outputs:
- mixed: bfloat16 [4, 512, 4096], P('fs', ('sp', 'tp'))
- log_totals: float32 [4, 8, 2, 512], P('fs', 'tp', None, 'sp')
The draws below stay inside these ranges and needn't reach their ends.
All inputs are finite; a program needn't handle non-finite values.
Results may differ from the reference program's by a relative error of at most 0.015.
Values may be sent and summed in bfloat16 or wider, within the bound.
A program may use at most 128 MiB of HBM per device.

```python
import math
import jax
import jax.numpy as jnp
from jax import lax

D = 4096
SW = 2048
GROUP_CH = 16
STATE = 64
HEADS = 8
HD = 128
CHANNEL_GROUPS = 128
VD = 256
SEQUENCE_LENGTH = 512
SEQUENCE_COUNT = 4
N_TP = 2


def query_base(key):
    base = jax.random.normal(jax.random.fold_in(key, 101), (D, 2 * HEADS * HD), jnp.float32)
    return jnp.clip(base, -6.0, 6.0)


def draw_w_query(key, part):
    scale = 1.3 * D ** (-0.5)
    return (query_base(key) * scale).astype(jnp.bfloat16)


def draw_w_key(key, part):
    scale = 1.3 * D ** (-0.5)
    other = jnp.clip(jax.random.normal(jax.random.fold_in(key, 102), (D, 2 * HEADS * HD), jnp.float32), -6.0, 6.0)
    mixed = other * scale
    return jnp.clip(mixed, -20.0 * D ** (-0.5), 20.0 * D ** (-0.5)).astype(jnp.bfloat16)


def draw_decay_re(key, part):
    share = 0.5
    slow = jax.random.uniform(jax.random.fold_in(key, 201), (CHANNEL_GROUPS, 1), jnp.float32) < share
    slow_rate = jnp.exp(jax.random.uniform(jax.random.fold_in(key, 202), (CHANNEL_GROUPS, STATE), jnp.float32, jnp.log(0.05), jnp.log(0.3))) / SEQUENCE_LENGTH
    fast_rate = jnp.exp(jax.random.uniform(jax.random.fold_in(key, 203), (CHANNEL_GROUPS, STATE), jnp.float32, jnp.log(1.0 / 100.0), jnp.log(1.0 / 30.0)))
    return -jnp.where(slow, slow_rate, fast_rate)


def draw_decay_shift(key, part):
    block_count = 16
    span = SEQUENCE_LENGTH // block_count
    rates = jnp.exp(jax.random.uniform(jax.random.fold_in(key, 301), (SEQUENCE_COUNT, CHANNEL_GROUPS, block_count), jnp.float32, jnp.log(0.3), jnp.log(3.0))) / SEQUENCE_LENGTH
    position_indices = jnp.arange(SEQUENCE_LENGTH, dtype=jnp.int32)
    block_index = jnp.minimum(position_indices // span, block_count - 1).astype(jnp.int32)
    spread_decay_rates = jnp.take(rates, block_index, axis=2)
    spike_position = jax.random.randint(jax.random.fold_in(key, 302), (SEQUENCE_COUNT, CHANNEL_GROUPS, 2), 0, SEQUENCE_LENGTH)
    spike_depth = jnp.log(jax.random.uniform(jax.random.fold_in(key, 303), (SEQUENCE_COUNT, CHANNEL_GROUPS, 2), jnp.float32, 0.6, 0.85))
    spike_hits = position_indices[None, None, None, :] == spike_position[..., None]
    spike_events = jnp.sum(jnp.where(spike_hits, spike_depth[..., None], 0.0), axis=2)
    return -spread_decay_rates + spike_events


def shard_levels(own_key, shape, pieces, least, largest):
    factor_of, own = 1.0, jax.random.fold_in(own_key, 6)
    for position, parts in pieces:
        heights = jnp.exp(jax.random.uniform(jax.random.fold_in(own, position), (parts,), jnp.float32, least / len(pieces), largest / len(pieces)))
        factor_of = factor_of * jnp.repeat(heights, shape[position] // parts).reshape([-1 if axis == position else 1 for axis in range(len(shape))])
    return factor_of


def normal_values(key, dims, scale, reach, shards=(), kind=jnp.bfloat16):
    drawn = jax.random.normal(key, dims, jnp.float32) * scale
    if len(shards) > 0:
        drawn = shard_levels(key, dims, shards, -0.22, 0.18) * drawn
    return jnp.clip(drawn, min=-reach, max=reach).astype(kind)


def setup_inputs(seed: int = 0) -> dict:
    seeds = jax.random.split(jax.random.key(seed), 20)
    return {
        "tokens": normal_values(seeds[0], (SEQUENCE_COUNT, SEQUENCE_LENGTH, D), 1.0, 6.0, ((0, 4), (1, 4), (2, 2))),
        "norm_gain": jnp.clip(1.0 + 0.18 * jax.random.normal(seeds[1], (D,), jnp.float32), 0.1, 1.9),
        "w_state_in": normal_values(seeds[2], (D, SW), D ** -0.5, 0.09375, ((0, 16), (1, 2))),
        "w_query": draw_w_query(jax.random.fold_in(seeds[19], 71), 0),
        "w_key": draw_w_key(jax.random.fold_in(seeds[19], 71), 0),
        "w_value": normal_values(seeds[5], (D, HEADS * VD), D ** -0.5, 0.09375, ((0, 16), (1, 2))),
        "decay_re": draw_decay_re(jax.random.fold_in(seeds[19], 71), 0),
        "decay_im": jnp.clip(jax.random.uniform(seeds[7], (CHANNEL_GROUPS, STATE), jnp.float32, -3.140625, 3.140625), -3.140625, 3.140625),
        "log_step": jnp.clip(-3.5 + 2.0 * jax.random.uniform(seeds[8], (CHANNEL_GROUPS,), jnp.float32) ** shard_levels(seeds[8], (CHANNEL_GROUPS,), ((0, 2),), -0.2, 0.2), -3.5, -1.5),
        "decay_shift": draw_decay_shift(jax.random.fold_in(seeds[19], 71), 0),
        "in_re": normal_values(seeds[10], (CHANNEL_GROUPS, STATE, GROUP_CH), ((0.25 / GROUP_CH) ** 0.5), 2.0, ((0, 2),), jnp.float32),
        "in_im": normal_values(seeds[11], (CHANNEL_GROUPS, STATE, GROUP_CH), ((0.25 / GROUP_CH) ** 0.5), 2.0, ((0, 2),), jnp.float32),
        "output_real": normal_values(seeds[12], (CHANNEL_GROUPS, GROUP_CH, STATE), STATE ** -0.5, 0.75, ((0, 2),), jnp.float32),
        "output_imaginary": normal_values(seeds[13], (CHANNEL_GROUPS, GROUP_CH, STATE), STATE ** -0.5, 0.75, ((0, 2),), jnp.float32),
        "skip": normal_values(seeds[14], (SW,), 0.3, 1.2, ((0, 2),), jnp.float32),
        "mix_weight": jnp.clip(0.3 + 0.5 * jax.random.uniform(seeds[15], (HEADS,), jnp.float32) ** shard_levels(seeds[15], (HEADS,), ((0, 2),), -0.2, 0.2), 0.3, 0.8),
        "head_gain": jnp.clip(1.0 + 0.18 * jax.random.normal(seeds[16], (VD,), jnp.float32), 0.1, 1.9),
        "w_out_state": normal_values(seeds[17], (SW, D), SW ** -0.5, 0.125, ((0, 2),)),
        "w_out_attn": normal_values(seeds[18], (HEADS * VD, D), (HEADS * VD) ** -0.5, 0.125, ((0, 2),)),
    }


def compose(earlier, later):
    early_scale_re, early_scale_im, early_shift_re, early_shift_im = earlier
    late_scale_re, late_scale_im, late_shift_re, late_shift_im = later
    scale_re = late_scale_re * early_scale_re - late_scale_im * early_scale_im
    scale_im = late_scale_re * early_scale_im + late_scale_im * early_scale_re
    shift_re = late_scale_re * early_shift_re - late_scale_im * early_shift_im + late_shift_re
    shift_im = late_scale_re * early_shift_im + late_scale_im * early_shift_re + late_shift_im
    return (scale_re, scale_im, shift_re, shift_im)

def input_matrices(decay_re, decay_im, log_step, in_re, in_im):
    step_size = jnp.exp(log_step)[:, None]
    numer_re = jnp.expm1(decay_re) * jnp.cos(decay_im) - 2.0 * jnp.sin(0.5 * decay_im) ** 2
    numer_im = jnp.exp(decay_re) * jnp.sin(decay_im)
    modulus = decay_re * decay_re + decay_im * decay_im
    coef_re = step_size * (numer_re * decay_re + numer_im * decay_im) / modulus
    coef_im = step_size * (numer_im * decay_re - numer_re * decay_im) / modulus
    matrix_re = coef_re[..., None] * in_re - coef_im[..., None] * in_im
    matrix_im = coef_re[..., None] * in_im + coef_im[..., None] * in_re
    return (matrix_re, matrix_im)

def reference(tokens, norm_gain, w_state_in, w_query, w_key, w_value, decay_re, decay_im, log_step, decay_shift, in_re, in_im, output_real, output_imaginary, skip, mix_weight, head_gain, w_out_state, w_out_attn):
    upper_limit = lax.Precision.HIGHEST
    seq_count, seq_len, width = tokens.shape
    floats = tokens.astype(jnp.float32)
    normed = (floats * lax.rsqrt(lax.optimization_barrier(jnp.mean(floats * floats, axis=-1, keepdims=True)) + 1e-06) * norm_gain).astype(jnp.bfloat16)
    flat = normed.reshape(seq_count * seq_len, width)
    state_in = jnp.dot(flat, w_state_in, preferred_element_type=jnp.float32).astype(jnp.bfloat16)
    queries = jnp.dot(flat, w_query, preferred_element_type=jnp.float32).astype(jnp.bfloat16)
    keys = jnp.dot(flat, w_key, preferred_element_type=jnp.float32).astype(jnp.bfloat16)
    values = jnp.dot(flat, w_value, preferred_element_type=jnp.float32).astype(jnp.bfloat16)
    matrix_re, matrix_im = input_matrices(decay_re, decay_im, log_step, in_re, in_im)
    grouped = state_in.astype(jnp.float32).reshape(seq_count, seq_len, CHANNEL_GROUPS, GROUP_CH).transpose(2, 0, 1, 3)
    skip_grouped = skip.reshape(CHANNEL_GROUPS, GROUP_CH)

    def one_group(items):
        inputs, mat_re, mat_im, rate_re, rate_im, shift, read_re, read_im, direct = items
        drive_re = jnp.einsum('pc,slc->slp', mat_re, inputs, precision=upper_limit)
        drive_im = jnp.einsum('pc,slc->slp', mat_im, inputs, precision=upper_limit)
        magnitude = jnp.exp(rate_re[None, None, :] + shift[:, :, None])
        factor_re = magnitude * jnp.cos(rate_im)[None, None, :]
        factor_im = magnitude * jnp.sin(rate_im)[None, None, :]
        scanned = lax.associative_scan(compose, (factor_re, factor_im, drive_re, drive_im), axis=1)
        result = jnp.einsum('cp,slp->slc', read_re, scanned[2], precision=upper_limit) - jnp.einsum('cp,slp->slc', read_im, scanned[3], precision=upper_limit) + direct[None, None, :] * inputs
        return result
    group_out = lax.map(one_group, (grouped, matrix_re, matrix_im, decay_re, decay_im, decay_shift.transpose(1, 0, 2), output_real, output_imaginary, skip_grouped))
    state_out = group_out.transpose(1, 2, 0, 3).reshape(seq_count * seq_len, SW).astype(jnp.bfloat16)
    head_queries = queries.reshape(seq_count, seq_len, HEADS, 2, HD).transpose(0, 2, 1, 3, 4).reshape(seq_count * HEADS, seq_len, 2, HD)
    head_keys = keys.reshape(seq_count, seq_len, HEADS, 2, HD).transpose(0, 2, 1, 3, 4).reshape(seq_count * HEADS, seq_len, 2, HD)
    head_values = values.reshape(seq_count, seq_len, HEADS, VD).transpose(0, 2, 1, 3).reshape(seq_count * HEADS, seq_len, VD)
    head_mix = jnp.tile(mix_weight, seq_count)
    block = math.gcd(seq_len, 512)
    key_pos = jnp.arange(seq_len, dtype=jnp.int32)

    def one_head(items):
        query_all, key_all, value_all, lam = items
        key_float = key_all.astype(jnp.float32)
        value_float = value_all.astype(jnp.float32)

        def one_block(index):
            start = index * block
            query_block = lax.dynamic_slice_in_dim(query_all, start, block, 0).astype(jnp.float32)
            scores = jnp.einsum('qmd,kmd->mqk', query_block, key_float, precision=upper_limit) * HD ** (-0.5)
            query_pos = start + jnp.arange(block, dtype=jnp.int32)
            allowed = key_pos[None, :] <= query_pos[:, None]
            masked = jnp.where(allowed[None], scores, -1e+30)
            row_max = lax.optimization_barrier(jnp.max(masked, axis=-1))
            weights = jnp.where(allowed[None], jnp.exp(masked - row_max[..., None]), 0.0)
            total = lax.optimization_barrier(jnp.sum(weights, axis=-1))
            rounded = lax.optimization_barrier(weights.astype(jnp.bfloat16)).astype(jnp.float32)
            numer = jnp.einsum('mqk,kd->mqd', rounded, value_float, precision=upper_limit)
            head_raw = numer[0] / total[0][:, None] - lam * numer[1] / total[1][:, None]
            normed_head = head_raw * lax.rsqrt(lax.optimization_barrier(jnp.mean(head_raw * head_raw, axis=-1, keepdims=True)) + 1e-05) * head_gain
            return (normed_head.astype(jnp.bfloat16), row_max + jnp.log(total))
        outs, logs = lax.map(one_block, jnp.arange(seq_len // block, dtype=jnp.int32))
        return (outs.reshape(seq_len, VD), logs.transpose(1, 0, 2).reshape(2, seq_len))
    head_out, head_logs = lax.map(one_head, (head_queries, head_keys, head_values, head_mix))
    attn_out = head_out.reshape(seq_count, HEADS, seq_len, VD).transpose(0, 2, 1, 3).reshape(seq_count * seq_len, HEADS * VD)
    log_totals = head_logs.reshape(seq_count, HEADS, 2, seq_len)
    state_parts = state_out.reshape(seq_count * seq_len, N_TP, SW // N_TP)
    attn_parts = attn_out.reshape(seq_count * seq_len, N_TP, HEADS * VD // N_TP)
    state_weights = w_out_state.reshape(N_TP, SW // N_TP, width)
    attn_weights = w_out_attn.reshape(N_TP, HEADS * VD // N_TP, width)

    def add_part(total, index):
        term = jnp.dot(state_parts[:, index], state_weights[index], preferred_element_type=jnp.float32) + jnp.dot(attn_parts[:, index], attn_weights[index], preferred_element_type=jnp.float32)
        rounded = lax.optimization_barrier(term.astype(jnp.bfloat16)).astype(jnp.float32)
        return (total + rounded, None)
    summed, _ = lax.scan(add_part, jnp.zeros((seq_count * seq_len, width), jnp.float32), jnp.arange(N_TP, dtype=jnp.int32))
    mixed = summed.astype(jnp.bfloat16).reshape(seq_count, seq_len, width)
    return (mixed, log_totals)
```

```python
import functools
import math

import jax
import jax.numpy as jnp
from jax import lax
from jax.experimental import pallas as pl
from jax.experimental.pallas import tpu as pltpu
from jax.sharding import PartitionSpec as P


def prefix(x, axis, combine, identity):
    size, here = (lax.axis_size(axis), lax.axis_index(axis))
    everything = jax.tree.map(lambda part: lax.all_gather(part, axis), x)
    start = jax.tree.map(
        lambda part, zero: jnp.broadcast_to(jnp.asarray(zero, part.dtype), part.shape), x, identity
    )

    def hop(k, before):
        reached = k < here
        new = combine(before, jax.tree.map(lambda part: part[k], everything))
        return jax.tree.map(lambda a, b: jnp.where(reached, a, b), new, before)

    return lax.fori_loop(0, size, hop, start)


def compose(earlier, later):
    early_scale_re, early_scale_im, early_shift_re, early_shift_im = earlier
    late_scale_re, late_scale_im, late_shift_re, late_shift_im = later
    scale_re = late_scale_re * early_scale_re - late_scale_im * early_scale_im
    scale_im = late_scale_re * early_scale_im + late_scale_im * early_scale_re
    shift_re = late_scale_re * early_shift_re - late_scale_im * early_shift_im + late_shift_re
    shift_im = late_scale_re * early_shift_im + late_scale_im * early_shift_re + late_shift_im
    return (scale_re, scale_im, shift_re, shift_im)


def state_branch(
    state_in,
    decay_re,
    decay_im,
    log_step,
    decay_shift,
    in_re,
    in_im,
    output_real,
    output_imaginary,
    skip,
):
    upper_limit = lax.Precision.HIGHEST
    tok_rows = state_in.shape[0]
    group_count, state_size = decay_re.shape
    group_width = in_re.shape[2]
    flat_width = group_count * state_size
    step_size = jnp.exp(log_step)[:, None]
    numer_re = jnp.expm1(decay_re) * jnp.cos(decay_im) - 2.0 * jnp.sin(0.5 * decay_im) ** 2
    numer_im = jnp.exp(decay_re) * jnp.sin(decay_im)
    modulus = decay_re * decay_re + decay_im * decay_im
    coef_re = step_size * (numer_re * decay_re + numer_im * decay_im) / modulus
    coef_im = step_size * (numer_im * decay_re - numer_re * decay_im) / modulus
    matrix_re = coef_re[..., None] * in_re - coef_im[..., None] * in_im
    matrix_im = coef_re[..., None] * in_im + coef_im[..., None] * in_re
    inputs = state_in.astype(jnp.float32).reshape(tok_rows, group_count, group_width)
    flat_shape = (tok_rows, flat_width)
    drive_re = jnp.einsum("gpc,tgc->tgp", matrix_re, inputs, precision=upper_limit).reshape(
        flat_shape
    )
    drive_im = jnp.einsum("gpc,tgc->tgp", matrix_im, inputs, precision=upper_limit).reshape(
        flat_shape
    )
    magnitude = jnp.exp(decay_re[None] + decay_shift[0].T[:, :, None])
    factor_re = (magnitude * jnp.cos(decay_im)[None]).reshape(flat_shape)
    factor_im = (magnitude * jnp.sin(decay_im)[None]).reshape(flat_shape)
    span = math.gcd(tok_rows, 16)
    block_count = tok_rows // span

    def to_blocks(values):
        return values.reshape(block_count, span, flat_width).transpose(1, 0, 2)

    rows_in = tuple((to_blocks(values) for values in (factor_re, factor_im, drive_re, drive_im)))
    ones_blocks = jnp.ones((block_count, flat_width), jnp.float32)
    zero_blocks = jnp.zeros((block_count, flat_width), jnp.float32)

    def row_step(carry, row):
        joined = compose(carry, row)
        return (joined, joined)

    block_totals, local = lax.scan(
        row_step, (ones_blocks, zero_blocks, zero_blocks, zero_blocks), rows_in
    )
    ones_row = jnp.ones((flat_width,), jnp.float32)
    zero_row = jnp.zeros((flat_width,), jnp.float32)

    def block_step(carry, row):
        return (compose(carry, row), carry)

    totals, before = lax.scan(block_step, (ones_row, zero_row, zero_row, zero_row), block_totals)
    carried = prefix(totals, "sp", compose, (ones_row, zero_row, zero_row, zero_row))
    start_re, start_im = (carried[2], carried[3])
    enter_re = before[0] * start_re[None] - before[1] * start_im[None] + before[2]
    enter_im = before[0] * start_im[None] + before[1] * start_re[None] + before[3]
    state_real = local[2] + local[0] * enter_re[None] - local[1] * enter_im[None]
    state_imaginary = local[3] + local[0] * enter_im[None] + local[1] * enter_re[None]
    group_layout_shape = (tok_rows, group_count, state_size)
    state_real = state_real.transpose(1, 0, 2).reshape(group_layout_shape)
    state_imaginary = state_imaginary.transpose(1, 0, 2).reshape(group_layout_shape)
    result = (
        jnp.einsum("hsv,jhv->jhs", output_real, state_real, precision=upper_limit)
        - jnp.einsum("hsv,jhv->jhs", output_imaginary, state_imaginary, precision=upper_limit)
        + skip.reshape(group_count, group_width)[None] * inputs
    )
    return result.reshape(tok_rows, group_count * group_width).astype(jnp.bfloat16)


def attention_branch(queries, keys_local, values_local, mix_weight, head_gain):
    tok_rows = queries.shape[0]
    head_count = mix_weight.shape[0]
    head_dim = queries.shape[1] // (2 * head_count)
    value_dim = values_local.shape[1] // head_count
    scale = head_dim ** (-0.5)
    first_pos = lax.axis_index("sp") * tok_rows
    query_pos = first_pos + jnp.arange(tok_rows, dtype=jnp.int32)
    query_heads = queries.reshape(tok_rows, head_count, 2, head_dim)
    initial = (
        jnp.full((head_count, 2, tok_rows), -1e30, jnp.float32),
        jnp.zeros((head_count, 2, tok_rows), jnp.float32),
        jnp.zeros((head_count, 2, tok_rows, value_dim), jnp.float32),
    )
    key_piece = lax.all_gather(keys_local, "sp", axis=0, tiled=True)
    value_piece = lax.all_gather(values_local, "sp", axis=0, tiled=True)
    count = key_piece.shape[0]
    block = math.gcd(count, 512)

    def one_block(index, inner):
        run_max, run_total, run_accum = inner
        offset = index * block
        key_block = lax.dynamic_slice_in_dim(key_piece, offset, block, 0).reshape(
            block, head_count, 2, head_dim
        )
        value_block = lax.dynamic_slice_in_dim(value_piece, offset, block, 0).reshape(
            block, head_count, value_dim
        )
        key_pos = offset + jnp.arange(block, dtype=jnp.int32)
        scores = (
            jnp.einsum(
                "qhmd,khmd->hmqk", query_heads, key_block, preferred_element_type=jnp.float32
            )
            * scale
        )
        allowed = key_pos[None, :] <= query_pos[:, None]
        masked = jnp.where(allowed, scores, -1e30)
        new_max = jnp.maximum(run_max, jnp.max(masked, axis=-1))
        weights = jnp.where(allowed, jnp.exp(masked - new_max[..., None]), 0.0)
        rescale = jnp.exp(run_max - new_max)
        new_total = run_total * rescale + jnp.sum(weights, axis=-1)
        product = jnp.einsum(
            "hmqk,khd->hmqd",
            weights.astype(jnp.bfloat16),
            value_block,
            preferred_element_type=jnp.float32,
        )
        return (new_max, new_total, run_accum * rescale[..., None] + product)

    def visit(inner):
        return lax.fori_loop(0, count // block, one_block, inner)

    def keep_carry(inner):
        return inner

    maxima, totals, accum = lax.cond(
        jnp.int32(0) <= first_pos + tok_rows - 1, visit, keep_carry, initial
    )
    log_totals = maxima + jnp.log(totals)
    head_raw = (
        accum[:, 0] / totals[:, 0, :, None]
        - mix_weight[:, None, None] * accum[:, 1] / totals[:, 1, :, None]
    )
    normed_heads = (
        head_raw
        * lax.rsqrt(jnp.mean(head_raw * head_raw, axis=-1, keepdims=True) + 1e-05)
        * head_gain
    )
    attn_out = (
        normed_heads.transpose(1, 0, 2)
        .reshape(tok_rows, head_count * value_dim)
        .astype(jnp.bfloat16)
    )
    return (attn_out, log_totals)


def per_device(
    tokens,
    norm_gain,
    w_state_in,
    w_query,
    w_key,
    w_value,
    decay_re,
    decay_im,
    log_step,
    decay_shift,
    in_re,
    in_im,
    output_real,
    output_imaginary,
    skip,
    mix_weight,
    head_gain,
    w_out_state,
    w_out_attn,
):
    whole = lax.all_gather(tokens, "tp", axis=2, tiled=True)[0]
    floats = whole.astype(jnp.float32)
    normed = (
        floats * lax.rsqrt(jnp.mean(floats * floats, axis=-1, keepdims=True) + 1e-06) * norm_gain
    ).astype(jnp.bfloat16)
    pieces = (
        lax.all_gather(w_state_in, ("sp", "fs"), axis=0, tiled=True),
        lax.all_gather(w_query, ("sp", "fs"), axis=0, tiled=True),
        lax.all_gather(w_key, ("sp", "fs"), axis=0, tiled=True),
        lax.all_gather(w_value, ("sp", "fs"), axis=0, tiled=True),
    )
    sums = tuple((jnp.dot(normed, piece, preferred_element_type=jnp.float32) for piece in pieces))
    state_in = sums[0].astype(jnp.bfloat16)
    queries = sums[1].astype(jnp.bfloat16)
    keys_local = sums[2].astype(jnp.bfloat16)
    values_local = sums[3].astype(jnp.bfloat16)
    attn_out, log_totals = attention_branch(
        queries, keys_local, values_local, mix_weight, head_gain
    )
    state_out = state_branch(
        state_in,
        decay_re,
        decay_im,
        log_step,
        decay_shift,
        in_re,
        in_im,
        output_real,
        output_imaginary,
        skip,
    )
    summed = lax.psum_scatter(
        (
            jnp.dot(state_out, w_out_state, preferred_element_type=jnp.float32)
            + jnp.dot(attn_out, w_out_attn, preferred_element_type=jnp.float32)
        ).astype(jnp.bfloat16),
        "tp",
        scatter_dimension=0,
        tiled=True,
    )
    return (summed[None], log_totals[None])


def nt_dot(a, b):
    return lax.dot_general(a, b, (((1,), (1,)), ((), ())), preferred_element_type=jnp.float32)


def split_pair(x):
    high = x.astype(jnp.bfloat16)
    low = (x - high.astype(jnp.float32)).astype(jnp.bfloat16)
    return (high, low)


def small_expm1(x):
    total = jnp.ones_like(x)
    for n in range(9, 1, -1):
        total = 1.0 + total * x * (1.0 / n)
    return total * x


def fused_kernel(
    sizes,
    tok_ref,
    gain_ref,
    ws_ref,
    wq_ref,
    wk_ref,
    wv_ref,
    dre_ref,
    dim_ref,
    logstep_ref,
    shift_ref,
    inre_ref,
    inim_ref,
    outre_ref,
    outim_ref,
    skip_ref,
    mix_ref,
    hgain_ref,
    wos_ref,
    woa_ref,
    mixed_ref,
    logt_ref,
    stat_send,
    stat_recv,
    nbuf,
    xbuf,
    wl,
    wbuf,
    ykeep,
    ysend,
    yrecv,
    fin,
    shsend,
    shbuf,
    inbuf,
    outbuf,
    coef,
    etab,
    bcat,
    ccat,
    srow,
    yacc,
    wts,
    stb,
    atb,
    sto,
    ato,
    ltb,
    lto,
    wo,
    acc,
    poutb,
    precb,
    loc_sem,
    wo_sem,
    w_loc,
    w_own,
    stat_sem,
    x_src,
    x_part,
    x_cross,
    x_rel,
    x_recv,
    wd_send,
    wy_send,
    w_recv,
    y_send,
    y_recv,
    sh_send,
    sh_recv,
    st_send,
    st_recv,
    at_send,
    at_recv,
    lt_send,
    lt_recv,
    p_send,
    p_recv,
):
    NS, NT, L, D, CW = sizes
    KW = D // 2
    KB = D // (NS * 4)
    FW = D // NT
    HC = CW // NS
    SEQ = NS * L
    G = HC // 16
    MESH = pl.DeviceIdType.MESH
    s, f, c = (lax.axis_index("sp"), lax.axis_index("fs"), lax.axis_index("tp"))
    zh, zl = (s // 2, lax.rem(s, 2))
    y, x = (f // 2, lax.rem(f, 2))
    s1 = s + 1 - 2 * zl
    s2 = lax.rem(s + 2, NS)
    fx = f + 1 - 2 * x
    fy = lax.rem(f + 2, 4)
    fd = 3 - f
    keep = zh + x - 2 * zh * x
    give = 1 - keep
    hq = 2 * x + zl
    home = 2 * y + keep
    partner = {"tp": 1 - c}

    def remote(src, dst, send, recv, where):
        return pltpu.make_async_remote_copy(
            src_ref=src, dst_ref=dst, send_sem=send, recv_sem=recv, device_id=where, device_id_type=MESH
        )

    g0 = pl.multiple_of(hq * G, G)
    kbo = zl * 4 + f

    def head_columns(h):
        return pl.ds(pl.multiple_of(h * HC, HC), HC)

    w_refs = (ws_ref, wq_ref, wk_ref, wv_ref)
    load_w = [pltpu.make_async_copy(ref, wl.at[m], w_loc.at[m]) for m, ref in enumerate(w_refs)]
    for copy in load_w:
        copy.start()
    own_w = [
        pltpu.make_async_copy(ref.at[:, head_columns(hq)], wbuf.at[m, kbo], w_own.at[m])
        for m, ref in enumerate(w_refs)
    ]
    for copy in own_w:
        copy.start()
    own_p = [
        pltpu.make_async_copy(ref.at[pl.ds(g0, G)], dst, loc_sem.at[i])
        for i, (ref, dst) in enumerate(
            (
                (inre_ref, inbuf.at[0]),
                (inim_ref, inbuf.at[1]),
                (outre_ref, outbuf.at[0]),
                (outim_ref, outbuf.at[1]),
            )
        )
    ]
    for copy in own_p:
        copy.start()
    big = [pltpu.make_async_copy(ref, wo.at[i], wo_sem.at[i]) for i, ref in enumerate((wos_ref, woa_ref))]
    for copy in big:
        copy.start()

    barrier = pltpu.get_barrier_semaphore()
    pl.semaphore_signal(barrier, inc=1, device_id={"fs": fy}, device_id_type=MESH)
    for k in range(NS):
        for there in (f, fx):
            for core in (c, 1 - c):
                if k == 0 and there is f and core is c:
                    continue
                pl.semaphore_signal(
                    barrier,
                    inc=1,
                    device_id={"sp": lax.rem(s + k, NS), "fs": there, "tp": core},
                    device_id_type=MESH,
                )
    tokens = tok_ref[0].astype(jnp.float32)
    square = jnp.sum(tokens * tokens, axis=1, keepdims=True)
    stat_send[...] = jnp.broadcast_to(square, (L, 128))
    pl.semaphore_wait(barrier, 4 * NS)
    stat = remote(stat_send, stat_recv, stat_sem.at[0], stat_sem.at[1], partner)
    stat.start()

    direct = (
        ((1 - x) * 2 + zl, {"fs": fx}),
        (x * 2 + 1 - zl, {"sp": s1}),
        ((1 - x) * 2 + 1 - zl, {"sp": s1, "fs": fx}),
    )
    arrive = (zl * 4 + fx, (1 - zl) * 4 + f, (1 - zl) * 4 + fx)
    across = (zl * 4 + fy, zl * 4 + fd, (1 - zl) * 4 + fy, (1 - zl) * 4 + fd)

    def w_direct(m, j):
        h, where = direct[j]
        return remote(
            wl.at[m, :, head_columns(h)], wbuf.at[m, kbo], wd_send.at[m, j], w_recv.at[m, kbo], where
        )

    def w_own_y(m):
        return remote(
            wl.at[m, :, head_columns(hq)], wbuf.at[m, kbo], wy_send.at[m, 3], w_recv.at[m, kbo], {"fs": fy}
        )

    def w_forward(m, j):
        part = wbuf.at[m, arrive[j]]
        return remote(part, part, wy_send.at[m, j], w_recv.at[m, arrive[j]], {"fs": fy})

    def w_arrival(m, kb):
        part = wbuf.at[m, kb]
        return remote(part, part, wy_send.at[m, 0], w_recv.at[m, kb], {"fs": fy})

    def start_direct(m):
        for j in (2, 1, 0):
            w_direct(m, j).start()

    def forward_all(m):
        for j in range(3):
            w_arrival(m, arrive[j]).wait_recv()
            w_forward(m, j).start()

    def wait_across(m):
        for kb in across:
            w_arrival(m, kb).wait_recv()

    load_w[0].wait()
    start_direct(0)
    w_own_y(0).start()
    load_w[1].wait()
    w_own_y(1).start()

    def shift_copy(xd, zd):
        zhd = xd + x - 2 * xd * x
        h = 2 * xd + zd
        return remote(
            shsend.at[h], shbuf.at[s], sh_send.at[h], sh_recv.at[s], {"sp": 2 * zhd + zd, "fs": 2 * y + xd}
        )

    def to_self(xd, zd):
        return jnp.logical_and(zh == 0, jnp.logical_and(x == xd, zl == zd))

    for h in range(NS):
        shsend[h] = shift_ref[0, h * G : (h + 1) * G, :]
    for xd in range(2):
        for zd in range(2):
            @pl.when(jnp.logical_not(to_self(xd, zd)))
            def _():
                shift_copy(xd, zd).start()

    @pl.when(zh == 0)
    def _():
        shbuf[s] = shsend[hq]

    stat.wait()
    mean = (square + stat_recv[:, 0:1]) * (1.0 / D)
    gain = gain_ref[:, pl.ds(pl.multiple_of(c * FW, FW), FW)]
    normed = (tok_ref[0].astype(jnp.float32) * lax.rsqrt(mean + 1e-06) * gain).astype(jnp.bfloat16)
    nbuf[...] = normed
    mine_half = c == zh
    q2 = 2 * (1 - zh) + zh
    order = (s, s1, q2, 2 * (1 - zh) + 1 - zh)
    duty = (zh, 1 - zh, zh, 1 - zh)
    near_s = 1 + c
    first_s = 2 - c
    near_core = jnp.where(s == first_s, c, 1 - c)

    def x_source(where):
        return remote(nbuf, xbuf.at[x, s], x_src, x_recv.at[x, s], where)

    far_target = {"sp": near_s, "tp": near_core}
    pair_target = {"sp": s1, "tp": 1 - zh}

    def x_part_copy(slot, i, q):
        part = xbuf.at[slot, q]
        return remote(part, part, x_part.at[slot, i], x_recv.at[slot, q], partner)

    def x_cross_copy(i):
        part = xbuf.at[x, order[i]]
        return remote(part, part, x_cross.at[i], x_recv.at[x, order[i]], {"fs": fx})

    def x_relay_copy(i):
        part = xbuf.at[x, order[i]]
        return remote(part, part, x_rel.at[i - 2], x_recv.at[x, order[i]], {"sp": s1})

    def x_arrival(slot, q):
        part = xbuf.at[slot, q]
        return remote(part, part, x_src, x_recv.at[slot, q], partner)

    relays = zl == 1 - zh

    @pl.when(mine_half)
    def _():
        xbuf[x, s] = nbuf[...]
        x_source(pair_target).start()
        remote(nbuf, xbuf.at[x, s], x_cross.at[0], x_recv.at[x, s], {"fs": fx}).start()
        remote(nbuf, xbuf.at[x, s], x_part.at[x, 0], x_recv.at[x, s], partner).start()

    @pl.when(jnp.logical_not(mine_half))
    def _():
        x_source(far_target).start()

    def x_own(i):
        q = order[i]
        if i == 0:
            @pl.when(jnp.logical_not(mine_half))
            def _():
                x_arrival(x, q).wait_recv()
            return
        x_arrival(x, q).wait_recv()

        @pl.when(c == duty[i])
        def _():
            if i >= 2:
                @pl.when(relays)
                def _():
                    x_relay_copy(i).start()
            x_cross_copy(i).start()
            x_part_copy(x, i, q).start()

    def x_other(i):
        q = order[i]
        x_arrival(1 - x, q).wait_recv()

        @pl.when(c == duty[i])
        def _():
            x_part_copy(1 - x, i, q).start()

    re16 = dre_ref[pl.ds(g0, G), :]
    im16 = dim_ref[pl.ds(g0, G), :]
    re16 = jnp.concatenate([re16, re16], axis=1)
    im16 = jnp.concatenate([im16, im16], axis=1)
    numer_re = small_expm1(re16) * jnp.cos(im16) - 2.0 * jnp.sin(0.5 * im16) ** 2
    numer_im = jnp.exp(re16) * jnp.sin(im16)
    modulus = re16 * re16 + im16 * im16
    coef[0] = re16
    coef[1] = im16
    coef[2] = (numer_re * re16 + numer_im * im16) / modulus
    coef[3] = (numer_im * re16 - numer_re * im16) / modulus
    for copy in own_p:
        copy.wait()
    lane = lax.broadcasted_iota(jnp.int32, (128, 16), 0)
    chan = lax.broadcasted_iota(jnp.int32, (128, 16), 1)
    steps = lax.broadcasted_iota(jnp.int32, (L, 128), 0).astype(jnp.float32) + 1.0

    def table(g, carry):
        zr = coef[0, pl.ds(g, 1), :]
        zi = coef[1, pl.ds(g, 1), :]
        step = jnp.exp(jnp.full((1, 128), logstep_ref[g0 + g], jnp.float32))
        cr = coef[2, pl.ds(g, 1), :] * step
        ci = coef[3, pl.ds(g, 1), :] * step
        angle = steps * zi
        cosine, sine = (jnp.cos(angle), jnp.sin(angle))
        shrink = jnp.exp(steps * zr)
        grow = jnp.exp(-(steps * zr))
        etab[0, g] = grow * (cosine * cr + sine * ci)
        etab[1, g] = grow * (cosine * ci - sine * cr)
        etab[2, g] = shrink * cosine
        etab[3, g] = shrink * sine
        pick = (lane == lax.rem(g, 8) * 16 + chan).astype(jnp.bfloat16)
        ir, ii = (inbuf[0, g], inbuf[1, g])
        raw = jnp.concatenate([ir, ii, -ii, ir], axis=1)
        hi, lo = split_pair(raw)
        bcat[g] = jnp.concatenate(
            [
                jnp.dot(pick, hi, preferred_element_type=jnp.float32).astype(jnp.bfloat16),
                jnp.dot(pick, lo, preferred_element_type=jnp.float32).astype(jnp.bfloat16),
            ],
            axis=0,
        )
        cr_, ci_ = (outbuf[0, g], outbuf[1, g])
        rawc = jnp.concatenate([cr_, -ci_, -ci_, -cr_], axis=1)
        hi, lo = split_pair(rawc)
        ccat[g] = jnp.concatenate(
            [
                jnp.dot(pick, hi, preferred_element_type=jnp.float32).astype(jnp.bfloat16),
                jnp.dot(pick, lo, preferred_element_type=jnp.float32).astype(jnp.bfloat16),
            ],
            axis=0,
        )
        return carry

    lax.fori_loop(0, G // 2, table, 0)
    forward_all(0)
    start_direct(1)
    lax.fori_loop(G // 2, G, table, 0)
    x_own(0)
    x_own(1)
    x_other(0)
    for m in (2, 3):
        load_w[m].wait()
    forward_all(1)
    w_own_y(2).start()
    start_direct(2)

    def weights(m):
        return wbuf[m].reshape(KW, HC)

    def y_copy(m, rows, i):
        return remote(ysend.at[m, rows], yrecv.at[m, rows], y_send.at[m, i], y_recv.at[m, i], {"sp": s2})

    def give_block(m, q, i):
        rows = pl.ds(pl.multiple_of(q * L, L), L)
        part = jnp.dot(xbuf[give, q], weights(m), preferred_element_type=jnp.float32)
        ysend[m, rows] = part.astype(jnp.bfloat16)
        y_copy(m, rows, q).start()

    def give_all(m):
        def one(i, carry):
            rows = pl.ds(pl.multiple_of(i * 2 * L, 2 * L), 2 * L)
            part = jnp.dot(
                xbuf[give, pl.ds(2 * i, 2)].reshape(2 * L, KW), weights(m), preferred_element_type=jnp.float32
            )
            ysend[m, rows] = part.astype(jnp.bfloat16)
            y_copy(m, rows, i).start()
            return carry

        lax.fori_loop(0, 2, one, 0)

    def keep_all(m):
        def one(i, carry):
            rows = pl.ds(pl.multiple_of(i * 2 * L, 2 * L), 2 * L)
            ykeep[m, rows] = jnp.dot(
                xbuf[keep, pl.ds(2 * i, 2)].reshape(2 * L, KW), weights(m), preferred_element_type=jnp.float32
            )
            return carry

        lax.fori_loop(0, 2, one, 0)

    def finish(m):
        for i in range(4 if m == 0 else 2):
            size = SEQ // (4 if m == 0 else 2)
            rows = pl.ds(i * size, size)
            y_copy(m, rows, i).wait_recv()
            fin[m, rows] = (ykeep[m, rows] + yrecv[m, rows].astype(jnp.float32)).astype(jnp.bfloat16)

    own_w[0].wait()
    wait_across(0)
    for i in range(4):
        if i >= 2:
            x_own(i)

        @pl.when(zh == 1)
        def _():
            give_block(0, order[i], i)

        if i >= 1:
            x_other(i)

        @pl.when(zh == 0)
        def _():
            give_block(0, order[i], i)

    own_w[1].wait()
    wait_across(1)
    give_all(1)
    forward_all(2)
    w_own_y(3).start()
    start_direct(3)
    keep_all(0)
    keep_all(1)

    for k in range(NS):
        @pl.when(jnp.logical_not(jnp.logical_and(zh == 0, s == k)))
        def _():
            remote(shsend.at[k], shbuf.at[k], sh_send.at[k], sh_recv.at[k], {"sp": s1}).wait_recv()
    row_i = lax.broadcasted_iota(jnp.int32, (L, L), 0)
    col_i = lax.broadcasted_iota(jnp.int32, (L, L), 1)
    upper = (row_i <= col_i).astype(jnp.float32)
    for k in range(NS):
        srow[k] = jnp.dot(
            shbuf[k], upper, precision=lax.Precision.HIGHEST, preferred_element_type=jnp.float32
        )

    own_w[2].wait()
    wait_across(2)
    give_all(2)

    finish(0)
    sign = jnp.where(lax.broadcasted_iota(jnp.int32, (8, 128), 1) < 64, -1.0, 1.0)
    lower = row_i >= col_i

    def lane_block(b, carry):
        lanes = pl.ds(pl.multiple_of(b * 128, 128), 128)
        u = fin[0, :, lanes]
        uu = jnp.concatenate([u, u], axis=1)
        yacc[...] = jnp.zeros_like(yacc)

        def group(g8, inner):
            g = b * 8 + g8
            drives = jnp.dot(uu, bcat[g], preferred_element_type=jnp.float32)
            h = jnp.zeros((1, 128), jnp.float32)
            er, ei, fr, fi = (etab[0, g], etab[1, g], etab[2, g], etab[3, g])
            for k in range(NS):
                d = drives[k * L : (k + 1) * L]
                x = er * d[:, :128] + ei * d[:, 128:]
                xh, xl = split_pair(x)
                xx = jnp.concatenate([xh, xl], axis=1)
                rhs = jnp.concatenate([xx, xx], axis=0)
                sr = jnp.broadcast_to(srow[k, pl.ds(g, 1), :], (L, L))
                sc = sr.T
                mask = jnp.where(lower, jnp.exp(jnp.minimum(sc - sr, 0.0)), 0.0)
                mh, ml = split_pair(mask)
                w2 = jnp.dot(
                    jnp.concatenate([mh, ml], axis=1), rhs, preferred_element_type=jnp.float32
                )
                q = w2[:, :128] + w2[:, 128:] + jnp.exp(sc) * h
                p1 = q * fr
                p2 = q * fi
                tail = p1[L - 8 :] + sign * pltpu.roll(p2[L - 8 :], 64, 1)
                h = tail[7:8]
                ph, plow = split_pair(jnp.concatenate([p1, p2], axis=1))
                y2 = nt_dot(ph, ccat[g]) + nt_dot(plow, ccat[g])
                yacc[k * L : (k + 1) * L, :] += y2[:, :128] + y2[:, 128:]
            return inner

        lax.fori_loop(0, 8, group, 0)
        through = skip_ref[:, pl.ds(pl.multiple_of(hq * HC + b * 128, 128), 128)]
        out = (yacc[...] + through * u.astype(jnp.float32)).astype(jnp.bfloat16)
        for k in range(NS):
            stb[k, :, lanes] = out[k * L : (k + 1) * L]
        return carry

    half_blocks = HC // 256
    lax.fori_loop(0, half_blocks, lane_block, 0)
    forward_all(3)
    lax.fori_loop(half_blocks, HC // 128, lane_block, 0)
    own_w[3].wait()
    wait_across(3)
    give_all(3)

    def result_copy(src, dst, send, recv, d):
        return remote(src.at[d], dst.at[hq], send.at[d], recv.at[hq], {"sp": d, "fs": home})

    def result_arrival(src, dst, send, recv, h):
        return remote(src.at[h], dst.at[h], send.at[h], recv.at[h], {"sp": s1})

    def here(d):
        return jnp.logical_and(zh == 0, s == d)

    def send_results(src, dst, send, recv):
        for d in range(NS):
            @pl.when(jnp.logical_not(here(d)))
            def _():
                result_copy(src, dst, send, recv, d).start()

        @pl.when(zh == 0)
        def _():
            dst[hq] = src[s]

    def wait_results(src, dst, send, recv):
        for h in range(NS):
            @pl.when(jnp.logical_not(jnp.logical_and(zh == 0, hq == h)))
            def _():
                result_arrival(src, dst, send, recv, h).wait_recv()

    send_results(stb, sto, st_send, st_recv)
    keep_all(2)
    keep_all(3)

    hd = HC // 2
    finish(1)
    finish(2)
    lam = mix_ref[hq]
    totals = []
    for i in range(NS):
        width = (i + 1) * L
        for m in range(2):
            sc = nt_dot(
                fin[1, i * L : (i + 1) * L, m * hd : (m + 1) * hd], fin[2, 0:width, m * hd : (m + 1) * hd]
            ) * (hd ** (-0.5))
            qpos = lax.broadcasted_iota(jnp.int32, (L, width), 0) + i * L
            kpos = lax.broadcasted_iota(jnp.int32, (L, width), 1)
            allowed = kpos <= qpos
            sc = jnp.where(allowed, sc, -1e30)
            top = jnp.max(sc, axis=1, keepdims=True)
            weights_i = jnp.where(allowed, jnp.exp(sc - top), 0.0)
            total = jnp.sum(weights_i, axis=1, keepdims=True)
            wts[m, i * L : (i + 1) * L, 0:width] = weights_i.astype(jnp.bfloat16)
            totals.append(1.0 / total)
            logs = jnp.broadcast_to(top + jnp.log(total), (L, L)).T
            ltb[i, m : m + 1, :] = logs[0:1]
    send_results(ltb, lto, lt_send, lt_recv)
    finish(3)
    for i in range(NS):
        width = (i + 1) * L
        heads = [
            jnp.dot(
                wts[m, i * L : (i + 1) * L, 0:width], fin[3, 0:width, :], preferred_element_type=jnp.float32
            )
            * totals[2 * i + m]
            for m in range(2)
        ]
        raw = heads[0] - lam * heads[1]
        scale = lax.rsqrt(jnp.mean(raw * raw, axis=1, keepdims=True) + 1e-05)
        atb[i] = (raw * scale * hgain_ref[...]).astype(jnp.bfloat16)

    send_results(atb, ato, at_send, at_recv)

    for copy in big:
        copy.wait()
    wait_results(stb, sto, st_send, st_recv)
    tiles = poutb.shape[0]
    width = D // tiles
    st_lhs = jnp.concatenate([sto[q] for q in range(NS)], axis=1)

    def state_tile(n, carry):
        columns = pl.ds(pl.multiple_of(n * width, width), width)
        acc[:, columns] = jnp.dot(st_lhs, wo[0, :, columns], preferred_element_type=jnp.float32)
        return carry

    lax.fori_loop(0, tiles, state_tile, 0)
    wait_results(atb, ato, at_send, at_recv)
    at_lhs = jnp.concatenate([ato[q] for q in range(NS)], axis=1)
    rows = L // NT
    mine = pl.ds(pl.multiple_of(c * rows, rows), rows)

    def p_copy(n):
        theirs = pl.ds(pl.multiple_of((1 - c) * rows, rows), rows)
        return remote(poutb.at[n, theirs], precb.at[n], p_send.at[n], p_recv.at[n], partner)

    def attn_tile(n, carry):
        columns = pl.ds(pl.multiple_of(n * width, width), width)
        part = acc[:, columns] + jnp.dot(at_lhs, wo[1, :, columns], preferred_element_type=jnp.float32)
        poutb[n] = part.astype(jnp.bfloat16)
        p_copy(n).start()
        return carry

    lax.fori_loop(0, tiles, attn_tile, 0)

    def last_tile(n, carry):
        columns = pl.ds(pl.multiple_of(n * width, width), width)
        p_copy(n).wait()
        mixed_ref[0, :, columns] = (
            poutb[n, mine, :].astype(jnp.float32) + precb[n].astype(jnp.float32)
        ).astype(jnp.bfloat16)
        return carry

    lax.fori_loop(0, tiles, last_tile, 0)
    wait_results(ltb, lto, lt_send, lt_recv)
    logt_ref[0] = lto[...]

    for m in range(4):
        for j in range(3):
            w_direct(m, j).wait_send()
            w_forward(m, j).wait_send()
        w_own_y(m).wait_send()
        for i in range(4 if m == 0 else 2):
            size = SEQ // (4 if m == 0 else 2)
            y_copy(m, pl.ds(i * size, size), i).wait_send()

    @pl.when(mine_half)
    def _():
        x_source(pair_target).wait_send()
        x_cross_copy(0).wait_send()
        x_part_copy(x, 0, s).wait_send()
        x_part_copy(1 - x, 0, s).wait_send()

    @pl.when(jnp.logical_not(mine_half))
    def _():
        x_source(far_target).wait_send()

    for i in range(1, 4):
        @pl.when(c == duty[i])
        def _():
            if i >= 2:
                @pl.when(relays)
                def _():
                    x_relay_copy(i).wait_send()
            x_cross_copy(i).wait_send()
            x_part_copy(x, i, order[i]).wait_send()
            x_part_copy(1 - x, i, order[i]).wait_send()

    for xd in range(2):
        for zd in range(2):
            @pl.when(jnp.logical_not(to_self(xd, zd)))
            def _():
                shift_copy(xd, zd).wait_send()
    for src, dst, send, recv in (
        (stb, sto, st_send, st_recv), (atb, ato, at_send, at_recv), (ltb, lto, lt_send, lt_recv)
    ):
        for d in range(NS):
            @pl.when(jnp.logical_not(here(d)))
            def _():
                result_copy(src, dst, send, recv, d).wait_send()


def fused_device(sizes, *args):
    (tokens, norm_gain, ws, wq, wk, wv, dre, dim, logstep, shift, inre, inim, outre, outim, skip, mix, hgain, wos, woa) = args
    NS, NT, L, D, CW = sizes
    KW, KB, HC = (D // 2, ws.shape[0], CW // NS)
    SEQ, G = (NS * L, HC // 16)
    tiles = 8
    bf, f32 = (jnp.bfloat16, jnp.float32)
    V = pltpu.VMEM
    DMA = pltpu.SemaphoreType.DMA
    vmem = pl.BlockSpec(memory_space=pltpu.VMEM)
    smem = pl.BlockSpec(memory_space=pltpu.SMEM)
    hbm = pl.BlockSpec(memory_space=pl.ANY)
    scratch = [
        V((L, 128), f32),
        V((L, 128), f32),
        V((L, KW), bf),
        V((2, NS, L, KW), bf),
        V((4, KB, CW), bf),
        V((4, KW // KB, KB, HC), bf),
        V((4, SEQ, HC), f32),
        V((4, SEQ, HC), bf),
        V((4, SEQ, HC), bf),
        V((4, SEQ, HC), bf),
        V((NS, G, L), f32),
        V((NS, G, L), f32),
        V((2, G, 16, 64), f32),
        V((2, G, 16, 64), f32),
        V((4, G, 128), f32),
        V((4, G, L, 128), f32),
        V((G, 256, 256), bf),
        V((G, 256, 256), bf),
        V((NS, G, L), f32),
        V((SEQ, 128), f32),
        V((2, SEQ, SEQ), bf),
        V((NS, L, HC), bf),
        V((NS, L, HC), bf),
        V((NS, L, HC), bf),
        V((NS, L, HC), bf),
        V((NS, 2, L), f32),
        V((NS, 2, L), f32),
        V((2, CW, D), bf),
        V((L, D), f32),
        V((tiles, L, D // tiles), bf),
        V((tiles, L // NT, D // tiles), bf),
        DMA((4,)),
        DMA((2,)),
        DMA((4,)),
        DMA((4,)),
        DMA((2,)),
        DMA,
        DMA((2, 4)),
        DMA((4,)),
        DMA((2,)),
        DMA((2, NS)),
        DMA((4, 3)),
        DMA((4, 4)),
        DMA((4, 8)),
        DMA((4, 4)),
        DMA((4, 4)),
    ]
    scratch += [DMA((NS,))] * 8
    scratch += [DMA((tiles,))] * 2
    call = pl.pallas_call(
        functools.partial(fused_kernel, sizes),
        out_shape=(
            jax.ShapeDtypeStruct((1, L // NT, D), bf),
            jax.ShapeDtypeStruct((1, NS, 2, L), f32),
        ),
        in_specs=[vmem, vmem, hbm, hbm, hbm, hbm, vmem, vmem, smem, vmem, hbm, hbm, hbm, hbm, vmem, smem, vmem, hbm, hbm],
        out_specs=(vmem, vmem),
        scratch_shapes=scratch,
        compiler_params=pltpu.CompilerParams(
            collective_id=0, has_side_effects=True, vmem_limit_bytes=67043328
        ),
    )
    return call(
        tokens, norm_gain.reshape(1, -1), ws, wq, wk, wv, dre, dim, logstep, shift,
        inre.transpose(0, 2, 1), inim.transpose(0, 2, 1), outre, outim,
        skip.reshape(1, -1), mix, hgain.reshape(1, -1), wos, woa,
    )


def choose_device(sp, fs, tp, *args):
    tokens, ws, dre, inre, mix = (args[0], args[2], args[6], args[10], args[15])
    L, D = (tokens.shape[1], ws.shape[0] * sp * fs)
    CW = ws.shape[1]
    fits = (
        sp == 4
        and fs == 4
        and tp == 2
        and mix.shape[0] == sp
        and L == 128
        and CW == sp * 256
        and dre.shape == (sp * 16, 64)
        and inre.shape[2] == 16
        and D == sp * 4 * ws.shape[0]
        and ws.shape[0] % 128 == 0
    )
    if fits:
        return fused_device((sp, tp, L, D, CW), *args)
    return per_device(*args)


def solution(mesh):
    in_specs = (
        P("fs", "sp", "tp"),
        P(),
        P(("sp", "fs"), "tp"),
        P(("sp", "fs"), "tp"),
        P(("sp", "fs"), "tp"),
        P(("sp", "fs"), "tp"),
        P("tp", None),
        P("tp", None),
        P("tp"),
        P("fs", "tp", "sp"),
        P("tp", None, None),
        P("tp", None, None),
        P("tp", None, None),
        P("tp", None, None),
        P("tp"),
        P("tp"),
        P(),
        P("tp", None),
        P("tp", None),
    )
    out_specs = (P("fs", ("sp", "tp"), None), P("fs", "tp", None, "sp"))
    body = functools.partial(choose_device, mesh.shape["sp"], mesh.shape["fs"], mesh.shape["tp"])
    return jax.shard_map(
        body, mesh=mesh, in_specs=in_specs, out_specs=out_specs, check_vma=False
    )
```

```python
import functools
import math

import jax
import jax.numpy as jnp
from jax import lax
from jax.experimental import pallas as pl
from jax.experimental.pallas import tpu as pltpu
from jax.sharding import PartitionSpec as P


def prefix(x, axis, combine, identity):
    size, here = (lax.axis_size(axis), lax.axis_index(axis))
    everything = jax.tree.map(lambda part: lax.all_gather(part, axis), x)
    start = jax.tree.map(
        lambda part, zero: jnp.broadcast_to(jnp.asarray(zero, part.dtype), part.shape), x, identity
    )

    def hop(k, before):
        reached = k < here
        new = combine(before, jax.tree.map(lambda part: part[k], everything))
        return jax.tree.map(lambda a, b: jnp.where(reached, a, b), new, before)

    return lax.fori_loop(0, size, hop, start)


def compose(earlier, later):
    early_scale_re, early_scale_im, early_shift_re, early_shift_im = earlier
    late_scale_re, late_scale_im, late_shift_re, late_shift_im = later
    scale_re = late_scale_re * early_scale_re - late_scale_im * early_scale_im
    scale_im = late_scale_re * early_scale_im + late_scale_im * early_scale_re
    shift_re = late_scale_re * early_shift_re - late_scale_im * early_shift_im + late_shift_re
    shift_im = late_scale_re * early_shift_im + late_scale_im * early_shift_re + late_shift_im
    return (scale_re, scale_im, shift_re, shift_im)


def state_branch(
    state_in,
    decay_re,
    decay_im,
    log_step,
    decay_shift,
    in_re,
    in_im,
    output_real,
    output_imaginary,
    skip,
):
    upper_limit = lax.Precision.HIGHEST
    tok_rows = state_in.shape[0]
    group_count, state_size = decay_re.shape
    group_width = in_re.shape[2]
    flat_width = group_count * state_size
    step_size = jnp.exp(log_step)[:, None]
    numer_re = jnp.expm1(decay_re) * jnp.cos(decay_im) - 2.0 * jnp.sin(0.5 * decay_im) ** 2
    numer_im = jnp.exp(decay_re) * jnp.sin(decay_im)
    modulus = decay_re * decay_re + decay_im * decay_im
    coef_re = step_size * (numer_re * decay_re + numer_im * decay_im) / modulus
    coef_im = step_size * (numer_im * decay_re - numer_re * decay_im) / modulus
    matrix_re = coef_re[..., None] * in_re - coef_im[..., None] * in_im
    matrix_im = coef_re[..., None] * in_im + coef_im[..., None] * in_re
    inputs = state_in.astype(jnp.float32).reshape(tok_rows, group_count, group_width)
    flat_shape = (tok_rows, flat_width)
    drive_re = jnp.einsum("gpc,tgc->tgp", matrix_re, inputs, precision=upper_limit).reshape(
        flat_shape
    )
    drive_im = jnp.einsum("gpc,tgc->tgp", matrix_im, inputs, precision=upper_limit).reshape(
        flat_shape
    )
    magnitude = jnp.exp(decay_re[None] + decay_shift[0].T[:, :, None])
    factor_re = (magnitude * jnp.cos(decay_im)[None]).reshape(flat_shape)
    factor_im = (magnitude * jnp.sin(decay_im)[None]).reshape(flat_shape)
    span = math.gcd(tok_rows, 16)
    block_count = tok_rows // span

    def to_blocks(values):
        return values.reshape(block_count, span, flat_width).transpose(1, 0, 2)

    rows_in = tuple((to_blocks(values) for values in (factor_re, factor_im, drive_re, drive_im)))
    ones_blocks = jnp.ones((block_count, flat_width), jnp.float32)
    zero_blocks = jnp.zeros((block_count, flat_width), jnp.float32)

    def row_step(carry, row):
        joined = compose(carry, row)
        return (joined, joined)

    block_totals, local = lax.scan(
        row_step, (ones_blocks, zero_blocks, zero_blocks, zero_blocks), rows_in
    )
    ones_row = jnp.ones((flat_width,), jnp.float32)
    zero_row = jnp.zeros((flat_width,), jnp.float32)

    def block_step(carry, row):
        return (compose(carry, row), carry)

    totals, before = lax.scan(block_step, (ones_row, zero_row, zero_row, zero_row), block_totals)
    carried = prefix(totals, "sp", compose, (ones_row, zero_row, zero_row, zero_row))
    start_re, start_im = (carried[2], carried[3])
    enter_re = before[0] * start_re[None] - before[1] * start_im[None] + before[2]
    enter_im = before[0] * start_im[None] + before[1] * start_re[None] + before[3]
    state_real = local[2] + local[0] * enter_re[None] - local[1] * enter_im[None]
    state_imaginary = local[3] + local[0] * enter_im[None] + local[1] * enter_re[None]
    group_layout_shape = (tok_rows, group_count, state_size)
    state_real = state_real.transpose(1, 0, 2).reshape(group_layout_shape)
    state_imaginary = state_imaginary.transpose(1, 0, 2).reshape(group_layout_shape)
    result = (
        jnp.einsum("hsv,jhv->jhs", output_real, state_real, precision=upper_limit)
        - jnp.einsum("hsv,jhv->jhs", output_imaginary, state_imaginary, precision=upper_limit)
        + skip.reshape(group_count, group_width)[None] * inputs
    )
    return result.reshape(tok_rows, group_count * group_width).astype(jnp.bfloat16)


def attention_branch(queries, keys_local, values_local, mix_weight, head_gain):
    tok_rows = queries.shape[0]
    head_count = mix_weight.shape[0]
    head_dim = queries.shape[1] // (2 * head_count)
    value_dim = values_local.shape[1] // head_count
    scale = head_dim ** (-0.5)
    first_pos = lax.axis_index("sp") * tok_rows
    query_pos = first_pos + jnp.arange(tok_rows, dtype=jnp.int32)
    query_heads = queries.reshape(tok_rows, head_count, 2, head_dim)
    initial = (
        jnp.full((head_count, 2, tok_rows), -1e30, jnp.float32),
        jnp.zeros((head_count, 2, tok_rows), jnp.float32),
        jnp.zeros((head_count, 2, tok_rows, value_dim), jnp.float32),
    )
    key_piece = lax.all_gather(keys_local, "sp", axis=0, tiled=True)
    value_piece = lax.all_gather(values_local, "sp", axis=0, tiled=True)
    count = key_piece.shape[0]
    block = math.gcd(count, 512)

    def one_block(index, inner):
        run_max, run_total, run_accum = inner
        offset = index * block
        key_block = lax.dynamic_slice_in_dim(key_piece, offset, block, 0).reshape(
            block, head_count, 2, head_dim
        )
        value_block = lax.dynamic_slice_in_dim(value_piece, offset, block, 0).reshape(
            block, head_count, value_dim
        )
        key_pos = offset + jnp.arange(block, dtype=jnp.int32)
        scores = (
            jnp.einsum(
                "qhmd,khmd->hmqk", query_heads, key_block, preferred_element_type=jnp.float32
            )
            * scale
        )
        allowed = key_pos[None, :] <= query_pos[:, None]
        masked = jnp.where(allowed, scores, -1e30)
        new_max = jnp.maximum(run_max, jnp.max(masked, axis=-1))
        weights = jnp.where(allowed, jnp.exp(masked - new_max[..., None]), 0.0)
        rescale = jnp.exp(run_max - new_max)
        new_total = run_total * rescale + jnp.sum(weights, axis=-1)
        product = jnp.einsum(
            "hmqk,khd->hmqd",
            weights.astype(jnp.bfloat16),
            value_block,
            preferred_element_type=jnp.float32,
        )
        return (new_max, new_total, run_accum * rescale[..., None] + product)

    def visit(inner):
        return lax.fori_loop(0, count // block, one_block, inner)

    def keep_carry(inner):
        return inner

    maxima, totals, accum = lax.cond(
        jnp.int32(0) <= first_pos + tok_rows - 1, visit, keep_carry, initial
    )
    log_totals = maxima + jnp.log(totals)
    head_raw = (
        accum[:, 0] / totals[:, 0, :, None]
        - mix_weight[:, None, None] * accum[:, 1] / totals[:, 1, :, None]
    )
    normed_heads = (
        head_raw
        * lax.rsqrt(jnp.mean(head_raw * head_raw, axis=-1, keepdims=True) + 1e-05)
        * head_gain
    )
    attn_out = (
        normed_heads.transpose(1, 0, 2)
        .reshape(tok_rows, head_count * value_dim)
        .astype(jnp.bfloat16)
    )
    return (attn_out, log_totals)


def per_device(
    tokens,
    norm_gain,
    w_state_in,
    w_query,
    w_key,
    w_value,
    decay_re,
    decay_im,
    log_step,
    decay_shift,
    in_re,
    in_im,
    output_real,
    output_imaginary,
    skip,
    mix_weight,
    head_gain,
    w_out_state,
    w_out_attn,
):
    whole = lax.all_gather(tokens, "tp", axis=2, tiled=True)[0]
    floats = whole.astype(jnp.float32)
    normed = (
        floats * lax.rsqrt(jnp.mean(floats * floats, axis=-1, keepdims=True) + 1e-06) * norm_gain
    ).astype(jnp.bfloat16)
    pieces = (
        lax.all_gather(w_state_in, ("sp", "fs"), axis=0, tiled=True),
        lax.all_gather(w_query, ("sp", "fs"), axis=0, tiled=True),
        lax.all_gather(w_key, ("sp", "fs"), axis=0, tiled=True),
        lax.all_gather(w_value, ("sp", "fs"), axis=0, tiled=True),
    )
    sums = tuple((jnp.dot(normed, piece, preferred_element_type=jnp.float32) for piece in pieces))
    state_in = sums[0].astype(jnp.bfloat16)
    queries = sums[1].astype(jnp.bfloat16)
    keys_local = sums[2].astype(jnp.bfloat16)
    values_local = sums[3].astype(jnp.bfloat16)
    attn_out, log_totals = attention_branch(
        queries, keys_local, values_local, mix_weight, head_gain
    )
    state_out = state_branch(
        state_in,
        decay_re,
        decay_im,
        log_step,
        decay_shift,
        in_re,
        in_im,
        output_real,
        output_imaginary,
        skip,
    )
    summed = lax.psum_scatter(
        (
            jnp.dot(state_out, w_out_state, preferred_element_type=jnp.float32)
            + jnp.dot(attn_out, w_out_attn, preferred_element_type=jnp.float32)
        ).astype(jnp.bfloat16),
        "tp",
        scatter_dimension=0,
        tiled=True,
    )
    return (summed[None], log_totals[None])


def nt_dot(a, b):
    return lax.dot_general(a, b, (((1,), (1,)), ((), ())), preferred_element_type=jnp.float32)


def split_pair(x):
    high = x.astype(jnp.bfloat16)
    low = (x - high.astype(jnp.float32)).astype(jnp.bfloat16)
    return (high, low)


def small_expm1(x):
    total = jnp.ones_like(x)
    for n in range(9, 1, -1):
        total = 1.0 + total * x * (1.0 / n)
    return total * x


def fused_kernel(
    sizes,
    tok_ref,
    gain_ref,
    ws_ref,
    wq_ref,
    wk_ref,
    wv_ref,
    dre_ref,
    dim_ref,
    logstep_ref,
    shift_ref,
    inre_ref,
    inim_ref,
    outre_ref,
    outim_ref,
    skip_ref,
    mix_ref,
    hgain_ref,
    wos_ref,
    woa_ref,
    mixed_ref,
    logt_ref,
    stat_send,
    stat_recv,
    nbuf,
    xbuf,
    wl,
    wbuf,
    ykeep,
    ysend,
    yrecv,
    fin,
    shsend,
    shbuf,
    inbuf,
    outbuf,
    coef,
    etab,
    bcat,
    ccat,
    srow,
    yacc,
    wts,
    stb,
    atb,
    sto,
    ato,
    ltb,
    lto,
    wo,
    acc,
    poutb,
    precb,
    loc_sem,
    wo_sem,
    w_loc,
    w_own,
    stat_sem,
    x_src,
    x_part,
    x_cross,
    x_rel,
    x_recv,
    wd_send,
    wy_send,
    w_recv,
    y_send,
    y_recv,
    sh_send,
    sh_recv,
    st_send,
    st_recv,
    at_send,
    at_recv,
    lt_send,
    lt_recv,
    p_send,
    p_recv,
):
    NS, NT, L, D, CW = sizes
    KW = D // 2
    KB = D // (NS * 4)
    FW = D // NT
    HC = CW // NS
    SEQ = NS * L
    G = HC // 16
    MESH = pl.DeviceIdType.MESH
    s, f, c = (lax.axis_index("sp"), lax.axis_index("fs"), lax.axis_index("tp"))
    zh, zl = (s // 2, lax.rem(s, 2))
    y, x = (f // 2, lax.rem(f, 2))
    s1 = s + 1 - 2 * zl
    s2 = lax.rem(s + 2, NS)
    fx = f + 1 - 2 * x
    fy = lax.rem(f + 2, 4)
    fd = 3 - f
    keep = zh + x - 2 * zh * x
    give = 1 - keep
    hq = 2 * x + zl
    home = 2 * y + keep
    partner = {"tp": 1 - c}

    def remote(src, dst, send, recv, where):
        return pltpu.make_async_remote_copy(
            src_ref=src, dst_ref=dst, send_sem=send, recv_sem=recv, device_id=where, device_id_type=MESH
        )

    g0 = pl.multiple_of(hq * G, G)
    kbo = zl * 4 + f

    def head_columns(h):
        return pl.ds(pl.multiple_of(h * HC, HC), HC)

    w_refs = (ws_ref, wq_ref, wk_ref, wv_ref)
    load_w = [pltpu.make_async_copy(ref, wl.at[m], w_loc.at[m]) for m, ref in enumerate(w_refs)]
    for copy in load_w:
        copy.start()
    own_w = [
        pltpu.make_async_copy(ref.at[:, head_columns(hq)], wbuf.at[m, kbo], w_own.at[m])
        for m, ref in enumerate(w_refs)
    ]
    for copy in own_w:
        copy.start()
    own_p = [
        pltpu.make_async_copy(ref.at[pl.ds(g0, G)], dst, loc_sem.at[i])
        for i, (ref, dst) in enumerate(
            (
                (inre_ref, inbuf.at[0]),
                (inim_ref, inbuf.at[1]),
                (outre_ref, outbuf.at[0]),
                (outim_ref, outbuf.at[1]),
            )
        )
    ]
    for copy in own_p:
        copy.start()
    big = [pltpu.make_async_copy(ref, wo.at[i], wo_sem.at[i]) for i, ref in enumerate((wos_ref, woa_ref))]
    for copy in big:
        copy.start()

    barrier = pltpu.get_barrier_semaphore()
    pl.semaphore_signal(barrier, inc=1, device_id={"fs": fy}, device_id_type=MESH)
    for k in range(NS):
        for there in (f, fx):
            for core in (c, 1 - c):
                if k == 0 and there is f and core is c:
                    continue
                pl.semaphore_signal(
                    barrier,
                    inc=1,
                    device_id={"sp": lax.rem(s + k, NS), "fs": there, "tp": core},
                    device_id_type=MESH,
                )
    tokens = tok_ref[0].astype(jnp.float32)
    square = jnp.sum(tokens * tokens, axis=1, keepdims=True)
    stat_send[...] = jnp.broadcast_to(square, (L, 128))
    pl.semaphore_wait(barrier, 4 * NS)
    stat = remote(stat_send, stat_recv, stat_sem.at[0], stat_sem.at[1], partner)
    stat.start()

    direct = (
        ((1 - x) * 2 + zl, {"fs": fx}),
        (x * 2 + 1 - zl, {"sp": s1}),
        ((1 - x) * 2 + 1 - zl, {"sp": s1, "fs": fx}),
    )
    arrive = (zl * 4 + fx, (1 - zl) * 4 + f, (1 - zl) * 4 + fx)
    across = (zl * 4 + fy, zl * 4 + fd, (1 - zl) * 4 + fy, (1 - zl) * 4 + fd)

    def w_direct(m, j):
        h, where = direct[j]
        return remote(
            wl.at[m, :, head_columns(h)], wbuf.at[m, kbo], wd_send.at[m, j], w_recv.at[m, kbo], where
        )

    def w_own_y(m):
        return remote(
            wl.at[m, :, head_columns(hq)], wbuf.at[m, kbo], wy_send.at[m, 3], w_recv.at[m, kbo], {"fs": fy}
        )

    def w_forward(m, j):
        part = wbuf.at[m, arrive[j]]
        return remote(part, part, wy_send.at[m, j], w_recv.at[m, arrive[j]], {"fs": fy})

    def w_arrival(m, kb):
        part = wbuf.at[m, kb]
        return remote(part, part, wy_send.at[m, 0], w_recv.at[m, kb], {"fs": fy})

    def start_direct(m):
        for j in (2, 1, 0):
            w_direct(m, j).start()

    def forward_all(m):
        for j in range(3):
            w_arrival(m, arrive[j]).wait_recv()
            w_forward(m, j).start()

    def wait_across(m):
        for kb in across:
            w_arrival(m, kb).wait_recv()

    load_w[0].wait()
    start_direct(0)
    w_own_y(0).start()
    load_w[1].wait()
    w_own_y(1).start()

    def shift_copy(xd, zd):
        zhd = xd + x - 2 * xd * x
        h = 2 * xd + zd
        return remote(
            shsend.at[h], shbuf.at[s], sh_send.at[h], sh_recv.at[s], {"sp": 2 * zhd + zd, "fs": 2 * y + xd}
        )

    def to_self(xd, zd):
        return jnp.logical_and(zh == 0, jnp.logical_and(x == xd, zl == zd))

    for h in range(NS):
        shsend[h] = shift_ref[0, h * G : (h + 1) * G, :]
    for xd in range(2):
        for zd in range(2):
            @pl.when(jnp.logical_not(to_self(xd, zd)))
            def _():
                shift_copy(xd, zd).start()

    @pl.when(zh == 0)
    def _():
        shbuf[s] = shsend[hq]

    stat.wait()
    mean = (square + stat_recv[:, 0:1]) * (1.0 / D)
    gain = gain_ref[:, pl.ds(pl.multiple_of(c * FW, FW), FW)]
    normed = (tok_ref[0].astype(jnp.float32) * lax.rsqrt(mean + 1e-06) * gain).astype(jnp.bfloat16)
    nbuf[...] = normed
    mine_half = c == zh
    q2 = 2 * (1 - zh) + zh
    order = (s, s1, q2, 2 * (1 - zh) + 1 - zh)
    duty = (zh, 1 - zh, zh, 1 - zh)
    near_s = 1 + c
    first_s = 2 - c
    near_core = jnp.where(s == first_s, c, 1 - c)

    parts = x_src.shape[0]
    strip = L // parts

    def piece(n):
        return pl.ds(n * strip, strip)

    def x_copy(src, slot, q, n, send, where):
        return remote(src, xbuf.at[slot, q, piece(n)], send, x_recv.at[slot, q, n], where)

    far_target = {"sp": near_s, "tp": near_core}
    pair_target = {"sp": s1, "tp": 1 - zh}

    def x_source(n, where):
        return x_copy(nbuf.at[piece(n)], x, s, n, x_src.at[n], where)

    def x_first(n):
        return (
            x_copy(nbuf.at[piece(n)], x, s, n, x_cross.at[0, n], {"fs": fx}),
            x_copy(nbuf.at[piece(n)], x, s, n, x_part.at[x, 0, n], partner),
        )

    def x_pass(slot, i, n):
        q = order[i]
        part = xbuf.at[slot, q, piece(n)]
        return x_copy(part, slot, q, n, x_part.at[slot, i, n], partner)

    def x_cross_copy(i, n):
        q = order[i]
        return x_copy(xbuf.at[x, q, piece(n)], x, q, n, x_cross.at[i, n], {"fs": fx})

    def x_relay_copy(i, n):
        q = order[i]
        return x_copy(xbuf.at[x, q, piece(n)], x, q, n, x_rel.at[i - 2, n], {"sp": s1})

    def x_wait(slot, q, n):
        x_copy(xbuf.at[slot, q, piece(n)], slot, q, n, x_src.at[n], partner).wait_recv()

    relays = zl == 1 - zh

    @pl.when(mine_half)
    def _():
        xbuf[x, s] = nbuf[...]
        for n in range(parts):
            x_source(n, pair_target).start()
            for copy in x_first(n):
                copy.start()

    @pl.when(jnp.logical_not(mine_half))
    def _():
        for n in range(parts):
            x_source(n, far_target).start()

    def x_own(i):
        @pl.when(c == duty[i])
        def _():
            for n in range(parts):
                x_wait(x, order[i], n)
                if i >= 2:
                    @pl.when(relays)
                    def _():
                        x_relay_copy(i, n).start()
                x_cross_copy(i, n).start()
                x_pass(x, i, n).start()

    def x_other(i):
        @pl.when(c == duty[i])
        def _():
            for n in range(parts):
                x_wait(1 - x, order[i], n)
                x_pass(1 - x, i, n).start()

    def x_need(i):
        @pl.when(c != duty[i])
        def _():
            for n in range(parts):
                x_wait(x, order[i], n)

    def x_need_other(i):
        @pl.when(c != duty[i])
        def _():
            for n in range(parts):
                x_wait(1 - x, order[i], n)

    re16 = dre_ref[pl.ds(g0, G), :]
    im16 = dim_ref[pl.ds(g0, G), :]
    re16 = jnp.concatenate([re16, re16], axis=1)
    im16 = jnp.concatenate([im16, im16], axis=1)
    numer_re = small_expm1(re16) * jnp.cos(im16) - 2.0 * jnp.sin(0.5 * im16) ** 2
    numer_im = jnp.exp(re16) * jnp.sin(im16)
    modulus = re16 * re16 + im16 * im16
    coef[0] = re16
    coef[1] = im16
    coef[2] = (numer_re * re16 + numer_im * im16) / modulus
    coef[3] = (numer_im * re16 - numer_re * im16) / modulus
    for copy in own_p:
        copy.wait()
    lane = lax.broadcasted_iota(jnp.int32, (128, 16), 0)
    chan = lax.broadcasted_iota(jnp.int32, (128, 16), 1)
    steps = lax.broadcasted_iota(jnp.int32, (L, 128), 0).astype(jnp.float32) + 1.0

    def table(g, carry):
        zr = coef[0, pl.ds(g, 1), :]
        zi = coef[1, pl.ds(g, 1), :]
        step = jnp.exp(jnp.full((1, 128), logstep_ref[g0 + g], jnp.float32))
        cr = coef[2, pl.ds(g, 1), :] * step
        ci = coef[3, pl.ds(g, 1), :] * step
        angle = steps * zi
        cosine, sine = (jnp.cos(angle), jnp.sin(angle))
        shrink = jnp.exp(steps * zr)
        grow = jnp.exp(-(steps * zr))
        etab[0, g] = grow * (cosine * cr + sine * ci)
        etab[1, g] = grow * (cosine * ci - sine * cr)
        etab[2, g] = shrink * cosine
        etab[3, g] = shrink * sine
        pick = (lane == lax.rem(g, 8) * 16 + chan).astype(jnp.bfloat16)
        ir, ii = (inbuf[0, g], inbuf[1, g])
        raw = jnp.concatenate([ir, ii, -ii, ir], axis=1)
        hi, lo = split_pair(raw)
        bcat[g] = jnp.concatenate(
            [
                jnp.dot(pick, hi, preferred_element_type=jnp.float32).astype(jnp.bfloat16),
                jnp.dot(pick, lo, preferred_element_type=jnp.float32).astype(jnp.bfloat16),
            ],
            axis=0,
        )
        cr_, ci_ = (outbuf[0, g], outbuf[1, g])
        rawc = jnp.concatenate([cr_, -ci_, -ci_, -cr_], axis=1)
        hi, lo = split_pair(rawc)
        ccat[g] = jnp.concatenate(
            [
                jnp.dot(pick, hi, preferred_element_type=jnp.float32).astype(jnp.bfloat16),
                jnp.dot(pick, lo, preferred_element_type=jnp.float32).astype(jnp.bfloat16),
            ],
            axis=0,
        )
        return carry

    lax.fori_loop(0, G // 2, table, 0)
    forward_all(0)
    for m in (2, 3):
        load_w[m].wait()
        w_own_y(m).start()
    lax.fori_loop(G // 2, G, table, 0)
    x_own(1)
    x_own(2)
    x_own(3)
    start_direct(1)
    x_other(0)
    x_other(1)

    def weights(m):
        return wbuf[m].reshape(KW, HC)

    def y_copy(m, rows, i):
        return remote(ysend.at[m, rows], yrecv.at[m, rows], y_send.at[m, i], y_recv.at[m, i], {"sp": s2})

    def give_block(m, q, i):
        rows = pl.ds(pl.multiple_of(q * L, L), L)
        part = jnp.dot(xbuf[give, q], weights(m), preferred_element_type=jnp.float32)
        ysend[m, rows] = part.astype(jnp.bfloat16)
        y_copy(m, rows, q).start()

    def give_all(m):
        def one(i, carry):
            rows = pl.ds(pl.multiple_of(i * 2 * L, 2 * L), 2 * L)
            part = jnp.dot(
                xbuf[give, pl.ds(2 * i, 2)].reshape(2 * L, KW), weights(m), preferred_element_type=jnp.float32
            )
            ysend[m, rows] = part.astype(jnp.bfloat16)
            y_copy(m, rows, i).start()
            return carry

        lax.fori_loop(0, 2, one, 0)

    def keep_all(m):
        def one(i, carry):
            rows = pl.ds(pl.multiple_of(i * 2 * L, 2 * L), 2 * L)
            ykeep[m, rows] = jnp.dot(
                xbuf[keep, pl.ds(2 * i, 2)].reshape(2 * L, KW), weights(m), preferred_element_type=jnp.float32
            )
            return carry

        lax.fori_loop(0, 2, one, 0)

    def finish(m):
        for i in range(4 if m == 0 else 2):
            size = SEQ // (4 if m == 0 else 2)
            rows = pl.ds(i * size, size)
            y_copy(m, rows, i).wait_recv()
            fin[m, rows] = (ykeep[m, rows] + yrecv[m, rows].astype(jnp.float32)).astype(jnp.bfloat16)

    own_w[0].wait()
    wait_across(0)
    x_need(0)
    x_need(1)
    x_need_other(0)
    x_need_other(1)
    give_block(0, order[0], 0)
    give_block(0, order[1], 1)
    x_other(2)
    x_other(3)
    forward_all(1)
    start_direct(2)
    x_need(2)
    x_need(3)
    x_need_other(2)
    x_need_other(3)
    give_block(0, order[2], 2)
    give_block(0, order[3], 3)
    own_w[1].wait()
    wait_across(1)
    give_all(1)
    forward_all(2)
    start_direct(3)
    keep_all(0)
    keep_all(1)

    for k in range(NS):
        @pl.when(jnp.logical_not(jnp.logical_and(zh == 0, s == k)))
        def _():
            remote(shsend.at[k], shbuf.at[k], sh_send.at[k], sh_recv.at[k], {"sp": s1}).wait_recv()
    row_i = lax.broadcasted_iota(jnp.int32, (L, L), 0)
    col_i = lax.broadcasted_iota(jnp.int32, (L, L), 1)
    upper = (row_i <= col_i).astype(jnp.float32)
    for k in range(NS):
        srow[k] = jnp.dot(
            shbuf[k], upper, precision=lax.Precision.HIGHEST, preferred_element_type=jnp.float32
        )

    own_w[2].wait()
    wait_across(2)
    give_all(2)

    finish(0)
    sign = jnp.where(lax.broadcasted_iota(jnp.int32, (8, 128), 1) < 64, -1.0, 1.0)
    lower = row_i >= col_i

    def lane_block(b, carry):
        lanes = pl.ds(pl.multiple_of(b * 128, 128), 128)
        u = fin[0, :, lanes]
        uu = jnp.concatenate([u, u], axis=1)
        yacc[...] = jnp.zeros_like(yacc)

        def group(g8, inner):
            g = b * 8 + g8
            drives = jnp.dot(uu, bcat[g], preferred_element_type=jnp.float32)
            h = jnp.zeros((1, 128), jnp.float32)
            er, ei, fr, fi = (etab[0, g], etab[1, g], etab[2, g], etab[3, g])
            for k in range(NS):
                d = drives[k * L : (k + 1) * L]
                x = er * d[:, :128] + ei * d[:, 128:]
                xh, xl = split_pair(x)
                xx = jnp.concatenate([xh, xl], axis=1)
                rhs = jnp.concatenate([xx, xx], axis=0)
                sr = jnp.broadcast_to(srow[k, pl.ds(g, 1), :], (L, L))
                sc = sr.T
                mask = jnp.where(lower, jnp.exp(jnp.minimum(sc - sr, 0.0)), 0.0)
                mh, ml = split_pair(mask)
                w2 = jnp.dot(
                    jnp.concatenate([mh, ml], axis=1), rhs, preferred_element_type=jnp.float32
                )
                q = w2[:, :128] + w2[:, 128:] + jnp.exp(sc) * h
                p1 = q * fr
                p2 = q * fi
                tail = p1[L - 8 :] + sign * pltpu.roll(p2[L - 8 :], 64, 1)
                h = tail[7:8]
                ph, plow = split_pair(jnp.concatenate([p1, p2], axis=1))
                y2 = nt_dot(ph, ccat[g]) + nt_dot(plow, ccat[g])
                yacc[k * L : (k + 1) * L, :] += y2[:, :128] + y2[:, 128:]
            return inner

        lax.fori_loop(0, 8, group, 0)
        through = skip_ref[:, pl.ds(pl.multiple_of(hq * HC + b * 128, 128), 128)]
        out = (yacc[...] + through * u.astype(jnp.float32)).astype(jnp.bfloat16)
        for k in range(NS):
            stb[k, :, lanes] = out[k * L : (k + 1) * L]
        return carry

    half_blocks = HC // 256
    lax.fori_loop(0, half_blocks, lane_block, 0)
    forward_all(3)
    lax.fori_loop(half_blocks, HC // 128, lane_block, 0)
    own_w[3].wait()
    wait_across(3)
    give_all(3)

    def result_copy(src, dst, send, recv, d):
        return remote(src.at[d], dst.at[hq], send.at[d], recv.at[hq], {"sp": d, "fs": home})

    def result_arrival(src, dst, send, recv, h):
        return remote(src.at[h], dst.at[h], send.at[h], recv.at[h], {"sp": s1})

    def here(d):
        return jnp.logical_and(zh == 0, s == d)

    def send_results(src, dst, send, recv):
        for d in range(NS):
            @pl.when(jnp.logical_not(here(d)))
            def _():
                result_copy(src, dst, send, recv, d).start()

        @pl.when(zh == 0)
        def _():
            dst[hq] = src[s]

    def wait_results(src, dst, send, recv):
        for h in range(NS):
            @pl.when(jnp.logical_not(jnp.logical_and(zh == 0, hq == h)))
            def _():
                result_arrival(src, dst, send, recv, h).wait_recv()

    send_results(stb, sto, st_send, st_recv)
    keep_all(2)
    keep_all(3)

    hd = HC // 2
    finish(1)
    finish(2)
    lam = mix_ref[hq]
    totals = []
    for i in range(NS):
        width = (i + 1) * L
        for m in range(2):
            sc = nt_dot(
                fin[1, i * L : (i + 1) * L, m * hd : (m + 1) * hd], fin[2, 0:width, m * hd : (m + 1) * hd]
            ) * (hd ** (-0.5))
            qpos = lax.broadcasted_iota(jnp.int32, (L, width), 0) + i * L
            kpos = lax.broadcasted_iota(jnp.int32, (L, width), 1)
            allowed = kpos <= qpos
            sc = jnp.where(allowed, sc, -1e30)
            top = jnp.max(sc, axis=1, keepdims=True)
            weights_i = jnp.where(allowed, jnp.exp(sc - top), 0.0)
            total = jnp.sum(weights_i, axis=1, keepdims=True)
            wts[m, i * L : (i + 1) * L, 0:width] = weights_i.astype(jnp.bfloat16)
            totals.append(1.0 / total)
            logs = jnp.broadcast_to(top + jnp.log(total), (L, L)).T
            ltb[i, m : m + 1, :] = logs[0:1]
    send_results(ltb, lto, lt_send, lt_recv)
    finish(3)
    for i in range(NS):
        width = (i + 1) * L
        heads = [
            jnp.dot(
                wts[m, i * L : (i + 1) * L, 0:width], fin[3, 0:width, :], preferred_element_type=jnp.float32
            )
            * totals[2 * i + m]
            for m in range(2)
        ]
        raw = heads[0] - lam * heads[1]
        scale = lax.rsqrt(jnp.mean(raw * raw, axis=1, keepdims=True) + 1e-05)
        atb[i] = (raw * scale * hgain_ref[...]).astype(jnp.bfloat16)

    send_results(atb, ato, at_send, at_recv)

    for copy in big:
        copy.wait()
    wait_results(stb, sto, st_send, st_recv)
    tiles = poutb.shape[0]
    width = D // tiles
    st_lhs = jnp.concatenate([sto[q] for q in range(NS)], axis=1)

    def state_tile(n, carry):
        columns = pl.ds(pl.multiple_of(n * width, width), width)
        acc[:, columns] = jnp.dot(st_lhs, wo[0, :, columns], preferred_element_type=jnp.float32)
        return carry

    lax.fori_loop(0, tiles, state_tile, 0)
    wait_results(atb, ato, at_send, at_recv)
    at_lhs = jnp.concatenate([ato[q] for q in range(NS)], axis=1)
    rows = L // NT
    mine = pl.ds(pl.multiple_of(c * rows, rows), rows)

    def p_copy(n):
        theirs = pl.ds(pl.multiple_of((1 - c) * rows, rows), rows)
        return remote(poutb.at[n, theirs], precb.at[n], p_send.at[n], p_recv.at[n], partner)

    def attn_tile(n, carry):
        columns = pl.ds(pl.multiple_of(n * width, width), width)
        part = acc[:, columns] + jnp.dot(at_lhs, wo[1, :, columns], preferred_element_type=jnp.float32)
        poutb[n] = part.astype(jnp.bfloat16)
        p_copy(n).start()
        return carry

    lax.fori_loop(0, tiles, attn_tile, 0)

    def last_tile(n, carry):
        columns = pl.ds(pl.multiple_of(n * width, width), width)
        p_copy(n).wait()
        mixed_ref[0, :, columns] = (
            poutb[n, mine, :].astype(jnp.float32) + precb[n].astype(jnp.float32)
        ).astype(jnp.bfloat16)
        return carry

    lax.fori_loop(0, tiles, last_tile, 0)
    wait_results(ltb, lto, lt_send, lt_recv)
    logt_ref[0] = lto[...]

    for m in range(4):
        for j in range(3):
            w_direct(m, j).wait_send()
            w_forward(m, j).wait_send()
        w_own_y(m).wait_send()
        for i in range(4 if m == 0 else 2):
            size = SEQ // (4 if m == 0 else 2)
            y_copy(m, pl.ds(i * size, size), i).wait_send()

    @pl.when(mine_half)
    def _():
        for n in range(parts):
            x_source(n, pair_target).wait_send()
            for copy in x_first(n):
                copy.wait_send()
            x_pass(1 - x, 0, n).wait_send()

    @pl.when(jnp.logical_not(mine_half))
    def _():
        for n in range(parts):
            x_source(n, far_target).wait_send()

    for i in range(1, 4):
        @pl.when(c == duty[i])
        def _():
            for n in range(parts):
                if i >= 2:
                    @pl.when(relays)
                    def _():
                        x_relay_copy(i, n).wait_send()
                x_cross_copy(i, n).wait_send()
                x_pass(x, i, n).wait_send()
                x_pass(1 - x, i, n).wait_send()

    for xd in range(2):
        for zd in range(2):
            @pl.when(jnp.logical_not(to_self(xd, zd)))
            def _():
                shift_copy(xd, zd).wait_send()
    for src, dst, send, recv in (
        (stb, sto, st_send, st_recv), (atb, ato, at_send, at_recv), (ltb, lto, lt_send, lt_recv)
    ):
        for d in range(NS):
            @pl.when(jnp.logical_not(here(d)))
            def _():
                result_copy(src, dst, send, recv, d).wait_send()


def fused_device(sizes, *args):
    (tokens, norm_gain, ws, wq, wk, wv, dre, dim, logstep, shift, inre, inim, outre, outim, skip, mix, hgain, wos, woa) = args
    NS, NT, L, D, CW = sizes
    KW, KB, HC = (D // 2, ws.shape[0], CW // NS)
    SEQ, G = (NS * L, HC // 16)
    tiles, pieces = (8, 2)
    bf, f32 = (jnp.bfloat16, jnp.float32)
    V = pltpu.VMEM
    DMA = pltpu.SemaphoreType.DMA
    vmem = pl.BlockSpec(memory_space=pltpu.VMEM)
    smem = pl.BlockSpec(memory_space=pltpu.SMEM)
    hbm = pl.BlockSpec(memory_space=pl.ANY)
    scratch = [
        V((L, 128), f32),
        V((L, 128), f32),
        V((L, KW), bf),
        V((2, NS, L, KW), bf),
        V((4, KB, CW), bf),
        V((4, KW // KB, KB, HC), bf),
        V((4, SEQ, HC), f32),
        V((4, SEQ, HC), bf),
        V((4, SEQ, HC), bf),
        V((4, SEQ, HC), bf),
        V((NS, G, L), f32),
        V((NS, G, L), f32),
        V((2, G, 16, 64), f32),
        V((2, G, 16, 64), f32),
        V((4, G, 128), f32),
        V((4, G, L, 128), f32),
        V((G, 256, 256), bf),
        V((G, 256, 256), bf),
        V((NS, G, L), f32),
        V((SEQ, 128), f32),
        V((2, SEQ, SEQ), bf),
        V((NS, L, HC), bf),
        V((NS, L, HC), bf),
        V((NS, L, HC), bf),
        V((NS, L, HC), bf),
        V((NS, 2, L), f32),
        V((NS, 2, L), f32),
        V((2, CW, D), bf),
        V((L, D), f32),
        V((tiles, L, D // tiles), bf),
        V((tiles, L // NT, D // tiles), bf),
        DMA((4,)),
        DMA((2,)),
        DMA((4,)),
        DMA((4,)),
        DMA((2,)),
        DMA((pieces,)),
        DMA((2, 4, pieces)),
        DMA((4, pieces)),
        DMA((2, pieces)),
        DMA((2, NS, pieces)),
        DMA((4, 3)),
        DMA((4, 4)),
        DMA((4, 8)),
        DMA((4, 4)),
        DMA((4, 4)),
    ]
    scratch += [DMA((NS,))] * 8
    scratch += [DMA((tiles,))] * 2
    call = pl.pallas_call(
        functools.partial(fused_kernel, sizes),
        out_shape=(
            jax.ShapeDtypeStruct((1, L // NT, D), bf),
            jax.ShapeDtypeStruct((1, NS, 2, L), f32),
        ),
        in_specs=[vmem, vmem, hbm, hbm, hbm, hbm, vmem, vmem, smem, vmem, hbm, hbm, hbm, hbm, vmem, smem, vmem, hbm, hbm],
        out_specs=(vmem, vmem),
        scratch_shapes=scratch,
        compiler_params=pltpu.CompilerParams(
            collective_id=0, has_side_effects=True, vmem_limit_bytes=67043328
        ),
    )
    return call(
        tokens, norm_gain.reshape(1, -1), ws, wq, wk, wv, dre, dim, logstep, shift,
        inre.transpose(0, 2, 1), inim.transpose(0, 2, 1), outre, outim,
        skip.reshape(1, -1), mix, hgain.reshape(1, -1), wos, woa,
    )


def choose_device(sp, fs, tp, *args):
    tokens, ws, dre, inre, mix = (args[0], args[2], args[6], args[10], args[15])
    L, D = (tokens.shape[1], ws.shape[0] * sp * fs)
    CW = ws.shape[1]
    fits = (
        sp == 4
        and fs == 4
        and tp == 2
        and mix.shape[0] == sp
        and L == 128
        and CW == sp * 256
        and dre.shape == (sp * 16, 64)
        and inre.shape[2] == 16
        and D == sp * 4 * ws.shape[0]
        and ws.shape[0] % 128 == 0
    )
    if fits:
        return fused_device((sp, tp, L, D, CW), *args)
    return per_device(*args)


def solution(mesh):
    in_specs = (
        P("fs", "sp", "tp"),
        P(),
        P(("sp", "fs"), "tp"),
        P(("sp", "fs"), "tp"),
        P(("sp", "fs"), "tp"),
        P(("sp", "fs"), "tp"),
        P("tp", None),
        P("tp", None),
        P("tp"),
        P("fs", "tp", "sp"),
        P("tp", None, None),
        P("tp", None, None),
        P("tp", None, None),
        P("tp", None, None),
        P("tp"),
        P("tp"),
        P(),
        P("tp", None),
        P("tp", None),
    )
    out_specs = (P("fs", ("sp", "tp"), None), P("fs", "tp", None, "sp"))
    body = functools.partial(choose_device, mesh.shape["sp"], mesh.shape["fs"], mesh.shape["tp"])
    return jax.shard_map(
        body, mesh=mesh, in_specs=in_specs, out_specs=out_specs, check_vma=False
    )
```

```python
import functools
import math

import jax
import jax.numpy as jnp
from jax import lax
from jax.experimental import pallas as pl
from jax.experimental.pallas import tpu as pltpu
from jax.sharding import PartitionSpec as P


def prefix(x, axis, combine, identity):
    size, here = (lax.axis_size(axis), lax.axis_index(axis))
    everything = jax.tree.map(lambda part: lax.all_gather(part, axis), x)
    start = jax.tree.map(
        lambda part, zero: jnp.broadcast_to(jnp.asarray(zero, part.dtype), part.shape), x, identity
    )

    def hop(k, before):
        reached = k < here
        new = combine(before, jax.tree.map(lambda part: part[k], everything))
        return jax.tree.map(lambda a, b: jnp.where(reached, a, b), new, before)

    return lax.fori_loop(0, size, hop, start)


def compose(earlier, later):
    early_scale_re, early_scale_im, early_shift_re, early_shift_im = earlier
    late_scale_re, late_scale_im, late_shift_re, late_shift_im = later
    scale_re = late_scale_re * early_scale_re - late_scale_im * early_scale_im
    scale_im = late_scale_re * early_scale_im + late_scale_im * early_scale_re
    shift_re = late_scale_re * early_shift_re - late_scale_im * early_shift_im + late_shift_re
    shift_im = late_scale_re * early_shift_im + late_scale_im * early_shift_re + late_shift_im
    return (scale_re, scale_im, shift_re, shift_im)


def state_branch(
    state_in,
    decay_re,
    decay_im,
    log_step,
    decay_shift,
    in_re,
    in_im,
    output_real,
    output_imaginary,
    skip,
):
    upper_limit = lax.Precision.HIGHEST
    tok_rows = state_in.shape[0]
    group_count, state_size = decay_re.shape
    group_width = in_re.shape[2]
    flat_width = group_count * state_size
    step_size = jnp.exp(log_step)[:, None]
    numer_re = jnp.expm1(decay_re) * jnp.cos(decay_im) - 2.0 * jnp.sin(0.5 * decay_im) ** 2
    numer_im = jnp.exp(decay_re) * jnp.sin(decay_im)
    modulus = decay_re * decay_re + decay_im * decay_im
    coef_re = step_size * (numer_re * decay_re + numer_im * decay_im) / modulus
    coef_im = step_size * (numer_im * decay_re - numer_re * decay_im) / modulus
    matrix_re = coef_re[..., None] * in_re - coef_im[..., None] * in_im
    matrix_im = coef_re[..., None] * in_im + coef_im[..., None] * in_re
    inputs = state_in.astype(jnp.float32).reshape(tok_rows, group_count, group_width)
    flat_shape = (tok_rows, flat_width)
    drive_re = jnp.einsum("gpc,tgc->tgp", matrix_re, inputs, precision=upper_limit).reshape(
        flat_shape
    )
    drive_im = jnp.einsum("gpc,tgc->tgp", matrix_im, inputs, precision=upper_limit).reshape(
        flat_shape
    )
    magnitude = jnp.exp(decay_re[None] + decay_shift[0].T[:, :, None])
    factor_re = (magnitude * jnp.cos(decay_im)[None]).reshape(flat_shape)
    factor_im = (magnitude * jnp.sin(decay_im)[None]).reshape(flat_shape)
    span = math.gcd(tok_rows, 16)
    block_count = tok_rows // span

    def to_blocks(values):
        return values.reshape(block_count, span, flat_width).transpose(1, 0, 2)

    rows_in = tuple((to_blocks(values) for values in (factor_re, factor_im, drive_re, drive_im)))
    ones_blocks = jnp.ones((block_count, flat_width), jnp.float32)
    zero_blocks = jnp.zeros((block_count, flat_width), jnp.float32)

    def row_step(carry, row):
        joined = compose(carry, row)
        return (joined, joined)

    block_totals, local = lax.scan(
        row_step, (ones_blocks, zero_blocks, zero_blocks, zero_blocks), rows_in
    )
    ones_row = jnp.ones((flat_width,), jnp.float32)
    zero_row = jnp.zeros((flat_width,), jnp.float32)

    def block_step(carry, row):
        return (compose(carry, row), carry)

    totals, before = lax.scan(block_step, (ones_row, zero_row, zero_row, zero_row), block_totals)
    carried = prefix(totals, "sp", compose, (ones_row, zero_row, zero_row, zero_row))
    start_re, start_im = (carried[2], carried[3])
    enter_re = before[0] * start_re[None] - before[1] * start_im[None] + before[2]
    enter_im = before[0] * start_im[None] + before[1] * start_re[None] + before[3]
    state_real = local[2] + local[0] * enter_re[None] - local[1] * enter_im[None]
    state_imaginary = local[3] + local[0] * enter_im[None] + local[1] * enter_re[None]
    group_layout_shape = (tok_rows, group_count, state_size)
    state_real = state_real.transpose(1, 0, 2).reshape(group_layout_shape)
    state_imaginary = state_imaginary.transpose(1, 0, 2).reshape(group_layout_shape)
    result = (
        jnp.einsum("hsv,jhv->jhs", output_real, state_real, precision=upper_limit)
        - jnp.einsum("hsv,jhv->jhs", output_imaginary, state_imaginary, precision=upper_limit)
        + skip.reshape(group_count, group_width)[None] * inputs
    )
    return result.reshape(tok_rows, group_count * group_width).astype(jnp.bfloat16)


def attention_branch(queries, keys_local, values_local, mix_weight, head_gain):
    tok_rows = queries.shape[0]
    head_count = mix_weight.shape[0]
    head_dim = queries.shape[1] // (2 * head_count)
    value_dim = values_local.shape[1] // head_count
    scale = head_dim ** (-0.5)
    first_pos = lax.axis_index("sp") * tok_rows
    query_pos = first_pos + jnp.arange(tok_rows, dtype=jnp.int32)
    query_heads = queries.reshape(tok_rows, head_count, 2, head_dim)
    initial = (
        jnp.full((head_count, 2, tok_rows), -1e30, jnp.float32),
        jnp.zeros((head_count, 2, tok_rows), jnp.float32),
        jnp.zeros((head_count, 2, tok_rows, value_dim), jnp.float32),
    )
    key_piece = lax.all_gather(keys_local, "sp", axis=0, tiled=True)
    value_piece = lax.all_gather(values_local, "sp", axis=0, tiled=True)
    count = key_piece.shape[0]
    block = math.gcd(count, 512)

    def one_block(index, inner):
        run_max, run_total, run_accum = inner
        offset = index * block
        key_block = lax.dynamic_slice_in_dim(key_piece, offset, block, 0).reshape(
            block, head_count, 2, head_dim
        )
        value_block = lax.dynamic_slice_in_dim(value_piece, offset, block, 0).reshape(
            block, head_count, value_dim
        )
        key_pos = offset + jnp.arange(block, dtype=jnp.int32)
        scores = (
            jnp.einsum(
                "qhmd,khmd->hmqk", query_heads, key_block, preferred_element_type=jnp.float32
            )
            * scale
        )
        allowed = key_pos[None, :] <= query_pos[:, None]
        masked = jnp.where(allowed, scores, -1e30)
        new_max = jnp.maximum(run_max, jnp.max(masked, axis=-1))
        weights = jnp.where(allowed, jnp.exp(masked - new_max[..., None]), 0.0)
        rescale = jnp.exp(run_max - new_max)
        new_total = run_total * rescale + jnp.sum(weights, axis=-1)
        product = jnp.einsum(
            "hmqk,khd->hmqd",
            weights.astype(jnp.bfloat16),
            value_block,
            preferred_element_type=jnp.float32,
        )
        return (new_max, new_total, run_accum * rescale[..., None] + product)

    def visit(inner):
        return lax.fori_loop(0, count // block, one_block, inner)

    def keep_carry(inner):
        return inner

    maxima, totals, accum = lax.cond(
        jnp.int32(0) <= first_pos + tok_rows - 1, visit, keep_carry, initial
    )
    log_totals = maxima + jnp.log(totals)
    head_raw = (
        accum[:, 0] / totals[:, 0, :, None]
        - mix_weight[:, None, None] * accum[:, 1] / totals[:, 1, :, None]
    )
    normed_heads = (
        head_raw
        * lax.rsqrt(jnp.mean(head_raw * head_raw, axis=-1, keepdims=True) + 1e-05)
        * head_gain
    )
    attn_out = (
        normed_heads.transpose(1, 0, 2)
        .reshape(tok_rows, head_count * value_dim)
        .astype(jnp.bfloat16)
    )
    return (attn_out, log_totals)


def per_device(
    tokens,
    norm_gain,
    w_state_in,
    w_query,
    w_key,
    w_value,
    decay_re,
    decay_im,
    log_step,
    decay_shift,
    in_re,
    in_im,
    output_real,
    output_imaginary,
    skip,
    mix_weight,
    head_gain,
    w_out_state,
    w_out_attn,
):
    whole = lax.all_gather(tokens, "tp", axis=2, tiled=True)[0]
    floats = whole.astype(jnp.float32)
    normed = (
        floats * lax.rsqrt(jnp.mean(floats * floats, axis=-1, keepdims=True) + 1e-06) * norm_gain
    ).astype(jnp.bfloat16)
    pieces = (
        lax.all_gather(w_state_in, ("sp", "fs"), axis=0, tiled=True),
        lax.all_gather(w_query, ("sp", "fs"), axis=0, tiled=True),
        lax.all_gather(w_key, ("sp", "fs"), axis=0, tiled=True),
        lax.all_gather(w_value, ("sp", "fs"), axis=0, tiled=True),
    )
    sums = tuple((jnp.dot(normed, piece, preferred_element_type=jnp.float32) for piece in pieces))
    state_in = sums[0].astype(jnp.bfloat16)
    queries = sums[1].astype(jnp.bfloat16)
    keys_local = sums[2].astype(jnp.bfloat16)
    values_local = sums[3].astype(jnp.bfloat16)
    attn_out, log_totals = attention_branch(
        queries, keys_local, values_local, mix_weight, head_gain
    )
    state_out = state_branch(
        state_in,
        decay_re,
        decay_im,
        log_step,
        decay_shift,
        in_re,
        in_im,
        output_real,
        output_imaginary,
        skip,
    )
    summed = lax.psum_scatter(
        (
            jnp.dot(state_out, w_out_state, preferred_element_type=jnp.float32)
            + jnp.dot(attn_out, w_out_attn, preferred_element_type=jnp.float32)
        ).astype(jnp.bfloat16),
        "tp",
        scatter_dimension=0,
        tiled=True,
    )
    return (summed[None], log_totals[None])


def nt_dot(a, b):
    return lax.dot_general(a, b, (((1,), (1,)), ((), ())), preferred_element_type=jnp.float32)


def split_pair(x):
    high = x.astype(jnp.bfloat16)
    low = (x - high.astype(jnp.float32)).astype(jnp.bfloat16)
    return (high, low)


def small_expm1(x):
    total = jnp.ones_like(x)
    for n in range(9, 1, -1):
        total = 1.0 + total * x * (1.0 / n)
    return total * x


def fused_kernel(
    sizes,
    tok_ref,
    gain_ref,
    ws_ref,
    wq_ref,
    wk_ref,
    wv_ref,
    dre_ref,
    dim_ref,
    logstep_ref,
    shift_ref,
    inre_ref,
    inim_ref,
    outre_ref,
    outim_ref,
    skip_ref,
    mix_ref,
    hgain_ref,
    wos_ref,
    woa_ref,
    mixed_ref,
    logt_ref,
    stat_send,
    stat_recv,
    nbuf,
    xbuf,
    wl,
    wbuf,
    ykeep,
    ysend,
    yrecv,
    fin,
    shsend,
    shbuf,
    inbuf,
    outbuf,
    coef,
    etab,
    bcat,
    ccat,
    srow,
    yacc,
    wts,
    stb,
    atb,
    sto,
    ato,
    ltb,
    lto,
    wo,
    acc,
    poutb,
    precb,
    obuf,
    o_sem,
    loc_sem,
    wo_sem,
    w_loc,
    w_own,
    stat_sem,
    x_send,
    x_recv,
    w_send,
    w_recv,
    y_send,
    y_recv,
    sh_send,
    sh_recv,
    st_send,
    st_recv,
    at_send,
    at_recv,
    lt_send,
    lt_recv,
    p_send,
    p_recv,
):
    NS, NT, L, D, CW = sizes
    KW = D // 2
    KB = D // (NS * 4)
    FW = D // NT
    HC = CW // NS
    SEQ = NS * L
    G = HC // 16
    MESH = pl.DeviceIdType.MESH
    s, f, c = (lax.axis_index("sp"), lax.axis_index("fs"), lax.axis_index("tp"))
    zh, zl = (s // 2, lax.rem(s, 2))
    y, x = (f // 2, lax.rem(f, 2))
    s1 = s + 1 - 2 * zl
    s2 = lax.rem(s + 2, NS)
    fx = f + 1 - 2 * x
    fy = lax.rem(f + 2, 4)
    fd = 3 - f
    keep = zh + x - 2 * zh * x
    give = 1 - keep
    hq = 2 * x + zl
    home = 2 * y + keep
    partner = {"tp": 1 - c}

    def remote(src, dst, send, recv, where):
        return pltpu.make_async_remote_copy(
            src_ref=src, dst_ref=dst, send_sem=send, recv_sem=recv, device_id=where, device_id_type=MESH
        )

    def drain_send(part, sem):
        remote(part, part, sem, stat_sem.at[1], partner).wait_send()

    def drain_recv(part, sem):
        remote(part, part, stat_sem.at[0], sem, partner).wait_recv()

    def drain_four(drain, ref, sem):
        @pl.when(zh == 0)
        def _():
            drain(ref.at[0 : NS - 1], sem)

        @pl.when(zh == 1)
        def _():
            drain(ref, sem)

    g0 = pl.multiple_of(hq * G, G)
    kbo = zl * 4 + f

    def head_columns(h):
        return pl.ds(pl.multiple_of(h * HC, HC), HC)

    w_refs = (ws_ref, wq_ref, wk_ref, wv_ref)
    load_w = [pltpu.make_async_copy(ref, wl.at[m], w_loc.at[m]) for m, ref in enumerate(w_refs)]
    for copy in load_w:
        copy.start()
    own_w = [
        pltpu.make_async_copy(ref.at[:, head_columns(hq)], wbuf.at[m, kbo], w_own.at[m])
        for m, ref in enumerate(w_refs)
    ]
    for copy in own_w:
        copy.start()
    own_p = [
        pltpu.make_async_copy(ref.at[pl.ds(g0, G)], dst, loc_sem.at[i])
        for i, (ref, dst) in enumerate(
            (
                (inre_ref, inbuf.at[0]),
                (inim_ref, inbuf.at[1]),
                (outre_ref, outbuf.at[0]),
                (outim_ref, outbuf.at[1]),
            )
        )
    ]
    for copy in own_p:
        copy.start()
    big = [pltpu.make_async_copy(ref, wo.at[i], wo_sem.at[i]) for i, ref in enumerate((wos_ref, woa_ref))]
    for copy in big:
        copy.start()

    barrier = pltpu.get_barrier_semaphore()
    pl.semaphore_signal(barrier, inc=1, device_id={"fs": fy}, device_id_type=MESH)
    for k in range(NS):
        for there in (f, fx):
            for core in (c, 1 - c):
                if k == 0 and there is f and core is c:
                    continue
                pl.semaphore_signal(
                    barrier,
                    inc=1,
                    device_id={"sp": lax.rem(s + k, NS), "fs": there, "tp": core},
                    device_id_type=MESH,
                )
    tokens = tok_ref[0].astype(jnp.float32)
    square = jnp.sum(tokens * tokens, axis=1, keepdims=True)
    stat_send[...] = jnp.broadcast_to(square, (L, 128))
    pl.semaphore_wait(barrier, 4 * NS)
    stat = remote(stat_send, stat_recv, stat_sem.at[0], stat_sem.at[1], partner)
    stat.start()

    direct = (
        ((1 - x) * 2 + zl, {"fs": fx}),
        (x * 2 + 1 - zl, {"sp": s1}),
        ((1 - x) * 2 + 1 - zl, {"sp": s1, "fs": fx}),
    )
    arrive = (zl * 4 + fx, (1 - zl) * 4 + f, (1 - zl) * 4 + fx)
    def w_direct(m, j):
        h, where = direct[j]
        return remote(wl.at[m, :, head_columns(h)], wbuf.at[m, kbo], w_send, w_recv.at[m, j], where)

    def w_own_y(m):
        return remote(wl.at[m, :, head_columns(hq)], wbuf.at[m, kbo], w_send, w_recv.at[m, 3], {"fs": fy})

    def w_forward(m, j):
        part = wbuf.at[m, arrive[j]]
        return remote(part, part, w_send, w_recv.at[m, 3], {"fs": fy})

    def start_direct(m):
        for j in (2, 1, 0):
            w_direct(m, j).start()

    def forward_all(m):
        for j in range(3):
            drain_recv(wbuf.at[m, arrive[j]], w_recv.at[m, j])
            w_forward(m, j).start()

    def wait_across(m):
        drain_recv(wbuf.at[m, 0:4], w_recv.at[m, 3])

    load_w[0].wait()
    start_direct(0)
    w_own_y(0).start()
    load_w[1].wait()
    w_own_y(1).start()

    def shift_copy(xd, zd):
        zhd = xd + x - 2 * xd * x
        h = 2 * xd + zd
        return remote(
            shsend.at[h], shbuf.at[s], sh_send, sh_recv, {"sp": 2 * zhd + zd, "fs": 2 * y + xd}
        )

    def to_self(xd, zd):
        return jnp.logical_and(zh == 0, jnp.logical_and(x == xd, zl == zd))

    for h in range(NS):
        shsend[h] = shift_ref[0, h * G : (h + 1) * G, :]
    for xd in range(2):
        for zd in range(2):
            @pl.when(jnp.logical_not(to_self(xd, zd)))
            def _():
                shift_copy(xd, zd).start()

    @pl.when(zh == 0)
    def _():
        shbuf[s] = shsend[hq]

    stat.wait()
    mean = (square + stat_recv[:, 0:1]) * (1.0 / D)
    gain = gain_ref[:, pl.ds(pl.multiple_of(c * FW, FW), FW)]
    normed = (tok_ref[0].astype(jnp.float32) * lax.rsqrt(mean + 1e-06) * gain).astype(jnp.bfloat16)
    nbuf[...] = normed
    mine_half = c == zh
    q2 = 2 * (1 - zh) + zh
    order = (s, s1, q2, 2 * (1 - zh) + 1 - zh)
    duty = (zh, 1 - zh, zh, 1 - zh)
    near_s = 1 + c
    first_s = 2 - c
    near_core = jnp.where(s == first_s, c, 1 - c)

    parts = x_recv.shape[2]
    strip = L // parts

    def piece(n):
        return pl.ds(n * strip, strip)

    def x_copy(src, slot, q, n, where):
        return remote(src, xbuf.at[4 * slot + q, piece(n)], x_send, x_recv.at[slot, q, n], where)

    far_target = {"sp": near_s, "tp": near_core}
    pair_target = {"sp": s1, "tp": 1 - zh}

    def x_source(n, where):
        return x_copy(nbuf.at[piece(n)], x, s, n, where)

    def x_step(slot, i, n, where):
        q = order[i]
        return x_copy(xbuf.at[4 * slot + q, piece(n)], slot, q, n, where)

    def x_wait(slot, q, n):
        drain_recv(xbuf.at[4 * slot + q, piece(n)], x_recv.at[slot, q, n])

    relays = zl == 1 - zh

    @pl.when(mine_half)
    def _():
        xbuf[4 * x + s] = nbuf[...]
        for n in range(parts):
            for where in (pair_target, {"fs": fx}, partner):
                x_source(n, where).start()

    @pl.when(jnp.logical_not(mine_half))
    def _():
        for n in range(parts):
            x_source(n, far_target).start()

    def x_own(i):
        @pl.when(c == duty[i])
        def _():
            for n in range(parts):
                x_wait(x, order[i], n)
                if i >= 2:
                    @pl.when(relays)
                    def _():
                        x_step(x, i, n, {"sp": s1}).start()
                x_step(x, i, n, {"fs": fx}).start()
                x_step(x, i, n, partner).start()

    def x_other(i):
        @pl.when(c == duty[i])
        def _():
            for n in range(parts):
                x_wait(1 - x, order[i], n)
                x_step(1 - x, i, n, partner).start()

    def x_need(i):
        @pl.when(c != duty[i])
        def _():
            for n in range(parts):
                x_wait(x, order[i], n)

    def x_need_other(i):
        @pl.when(c != duty[i])
        def _():
            for n in range(parts):
                x_wait(1 - x, order[i], n)

    re16 = dre_ref[pl.ds(g0, G), :]
    im16 = dim_ref[pl.ds(g0, G), :]
    re16 = jnp.concatenate([re16, re16], axis=1)
    im16 = jnp.concatenate([im16, im16], axis=1)
    numer_re = small_expm1(re16) * jnp.cos(im16) - 2.0 * jnp.sin(0.5 * im16) ** 2
    numer_im = jnp.exp(re16) * jnp.sin(im16)
    modulus = re16 * re16 + im16 * im16
    coef[0] = re16
    coef[1] = im16
    coef[2] = (numer_re * re16 + numer_im * im16) / modulus
    coef[3] = (numer_im * re16 - numer_re * im16) / modulus
    for copy in own_p:
        copy.wait()
    lane = lax.broadcasted_iota(jnp.int32, (128, 16), 0)
    chan = lax.broadcasted_iota(jnp.int32, (128, 16), 1)
    steps = lax.broadcasted_iota(jnp.int32, (L, 128), 0).astype(jnp.float32) + 1.0

    def table(g, carry):
        zr = coef[0, pl.ds(g, 1), :]
        zi = coef[1, pl.ds(g, 1), :]
        step = jnp.exp(jnp.full((1, 128), logstep_ref[g0 + g], jnp.float32))
        cr = coef[2, pl.ds(g, 1), :] * step
        ci = coef[3, pl.ds(g, 1), :] * step
        angle = steps * zi
        cosine, sine = (jnp.cos(angle), jnp.sin(angle))
        shrink = jnp.exp(steps * zr)
        grow = jnp.exp(-(steps * zr))
        etab[0, g] = grow * (cosine * cr + sine * ci)
        etab[1, g] = grow * (cosine * ci - sine * cr)
        etab[2, g] = shrink * cosine
        etab[3, g] = shrink * sine
        pick = (lane == lax.rem(g, 8) * 16 + chan).astype(jnp.bfloat16)
        ir, ii = (inbuf[0, g], inbuf[1, g])
        raw = jnp.concatenate([ir, ii, -ii, ir], axis=1)
        hi, lo = split_pair(raw)
        bcat[g] = jnp.concatenate(
            [
                jnp.dot(pick, hi, preferred_element_type=jnp.float32).astype(jnp.bfloat16),
                jnp.dot(pick, lo, preferred_element_type=jnp.float32).astype(jnp.bfloat16),
            ],
            axis=0,
        )
        cr_, ci_ = (outbuf[0, g], outbuf[1, g])
        rawc = jnp.concatenate([cr_, -ci_, -ci_, -cr_], axis=1)
        hi, lo = split_pair(rawc)
        ccat[g] = jnp.concatenate(
            [
                jnp.dot(pick, hi, preferred_element_type=jnp.float32).astype(jnp.bfloat16),
                jnp.dot(pick, lo, preferred_element_type=jnp.float32).astype(jnp.bfloat16),
            ],
            axis=0,
        )
        return carry

    lax.fori_loop(0, G // 2, table, 0)
    forward_all(0)
    for m in (2, 3):
        load_w[m].wait()
        w_own_y(m).start()
    lax.fori_loop(G // 2, G, table, 0)
    x_own(1)
    x_own(2)
    x_own(3)
    start_direct(1)
    x_other(0)
    x_other(1)

    def weights(m):
        return wbuf[m].reshape(KW, HC)

    def y_copy(m, rows, i):
        return remote(ysend.at[m, rows], yrecv.at[m, rows], y_send, y_recv.at[m], {"sp": s2})

    def give_block(m, q, i):
        rows = pl.ds(pl.multiple_of(q * L, L), L)
        part = jnp.dot(xbuf[4 * give + q], weights(m), preferred_element_type=jnp.float32)
        ysend[m, rows] = part.astype(jnp.bfloat16)
        y_copy(m, rows, q).start()

    def give_all(m):
        def one(i, carry):
            rows = pl.ds(pl.multiple_of(i * 2 * L, 2 * L), 2 * L)
            part = jnp.dot(
                xbuf[pl.ds(4 * give + 2 * i, 2)].reshape(2 * L, KW), weights(m), preferred_element_type=jnp.float32
            )
            ysend[m, rows] = part.astype(jnp.bfloat16)
            y_copy(m, rows, i).start()
            return carry

        lax.fori_loop(0, 2, one, 0)

    def keep_all(m):
        def one(i, carry):
            rows = pl.ds(pl.multiple_of(i * 2 * L, 2 * L), 2 * L)
            ykeep[m, rows] = jnp.dot(
                xbuf[pl.ds(4 * keep + 2 * i, 2)].reshape(2 * L, KW), weights(m), preferred_element_type=jnp.float32
            )
            return carry

        lax.fori_loop(0, 2, one, 0)

    def finish(m):
        drain_recv(yrecv.at[m], y_recv.at[m])
        fin[m] = (ykeep[m] + yrecv[m].astype(jnp.float32)).astype(jnp.bfloat16)

    own_w[0].wait()
    wait_across(0)
    x_need(0)
    x_need(1)
    x_need_other(0)
    x_need_other(1)
    give_block(0, order[0], 0)
    give_block(0, order[1], 1)
    forward_all(1)
    x_other(2)
    x_other(3)
    start_direct(2)
    x_need(2)
    x_need(3)
    x_need_other(2)
    x_need_other(3)
    give_block(0, order[2], 2)
    give_block(0, order[3], 3)
    own_w[1].wait()
    wait_across(1)
    give_all(1)
    forward_all(2)
    start_direct(3)
    keep_all(0)
    keep_all(1)

    drain_four(drain_recv, shbuf, sh_recv)
    row_i = lax.broadcasted_iota(jnp.int32, (L, L), 0)
    col_i = lax.broadcasted_iota(jnp.int32, (L, L), 1)
    upper = (row_i <= col_i).astype(jnp.float32)
    for k in range(NS):
        srow[k] = jnp.dot(
            shbuf[k], upper, precision=lax.Precision.HIGHEST, preferred_element_type=jnp.float32
        )

    own_w[2].wait()
    wait_across(2)
    give_all(2)

    finish(0)
    sign = jnp.where(lax.broadcasted_iota(jnp.int32, (8, 128), 1) < 64, -1.0, 1.0)
    lower = row_i >= col_i

    def lane_block(b, carry):
        lanes = pl.ds(pl.multiple_of(b * 128, 128), 128)
        u = fin[0, :, lanes]
        uu = jnp.concatenate([u, u], axis=1)
        yacc[...] = jnp.zeros_like(yacc)

        def group(g8, inner):
            g = b * 8 + g8
            drives = jnp.dot(uu, bcat[g], preferred_element_type=jnp.float32)
            h = jnp.zeros((1, 128), jnp.float32)
            er, ei, fr, fi = (etab[0, g], etab[1, g], etab[2, g], etab[3, g])
            for k in range(NS):
                d = drives[k * L : (k + 1) * L]
                x = er * d[:, :128] + ei * d[:, 128:]
                xh, xl = split_pair(x)
                xx = jnp.concatenate([xh, xl], axis=1)
                rhs = jnp.concatenate([xx, xx], axis=0)
                sr = jnp.broadcast_to(srow[k, pl.ds(g, 1), :], (L, L))
                sc = sr.T
                mask = jnp.where(lower, jnp.exp(jnp.minimum(sc - sr, 0.0)), 0.0)
                mh, ml = split_pair(mask)
                w2 = jnp.dot(
                    jnp.concatenate([mh, ml], axis=1), rhs, preferred_element_type=jnp.float32
                )
                q = w2[:, :128] + w2[:, 128:] + jnp.exp(sc) * h
                p1 = q * fr
                p2 = q * fi
                tail = p1[L - 8 :] + sign * pltpu.roll(p2[L - 8 :], 64, 1)
                h = tail[7:8]
                ph, plow = split_pair(jnp.concatenate([p1, p2], axis=1))
                y2 = nt_dot(ph, ccat[g]) + nt_dot(plow, ccat[g])
                yacc[k * L : (k + 1) * L, :] += y2[:, :128] + y2[:, 128:]
            return inner

        lax.fori_loop(0, 8, group, 0)
        through = skip_ref[:, pl.ds(pl.multiple_of(hq * HC + b * 128, 128), 128)]
        out = (yacc[...] + through * u.astype(jnp.float32)).astype(jnp.bfloat16)
        for k in range(NS):
            stb[k, :, lanes] = out[k * L : (k + 1) * L]
        return carry

    half_blocks = HC // 256
    lax.fori_loop(0, half_blocks, lane_block, 0)
    forward_all(3)
    lax.fori_loop(half_blocks, HC // 128, lane_block, 0)
    own_w[3].wait()
    wait_across(3)
    give_all(3)

    def result_copy(src, dst, send, recv, d):
        return remote(src.at[d], dst.at[hq], send, recv, {"sp": d, "fs": home})

    def here(d):
        return jnp.logical_and(zh == 0, s == d)

    def send_results(src, dst, send, recv):
        for d in range(NS):
            @pl.when(jnp.logical_not(here(d)))
            def _():
                result_copy(src, dst, send, recv, d).start()

        @pl.when(zh == 0)
        def _():
            dst[hq] = src[s]

    def wait_results(dst, recv):
        drain_four(drain_recv, dst, recv)

    send_results(stb, sto, st_send, st_recv)
    keep_all(2)
    keep_all(3)

    hd = HC // 2
    finish(1)
    finish(2)
    lam = mix_ref[hq]
    totals = []
    for i in range(NS):
        width = (i + 1) * L
        for m in range(2):
            sc = nt_dot(
                fin[1, i * L : (i + 1) * L, m * hd : (m + 1) * hd], fin[2, 0:width, m * hd : (m + 1) * hd]
            ) * (hd ** (-0.5))
            qpos = lax.broadcasted_iota(jnp.int32, (L, width), 0) + i * L
            kpos = lax.broadcasted_iota(jnp.int32, (L, width), 1)
            allowed = kpos <= qpos
            sc = jnp.where(allowed, sc, -1e30)
            top = jnp.max(sc, axis=1, keepdims=True)
            weights_i = jnp.where(allowed, jnp.exp(sc - top), 0.0)
            total = jnp.sum(weights_i, axis=1, keepdims=True)
            wts[m, i * L : (i + 1) * L, 0:width] = weights_i.astype(jnp.bfloat16)
            totals.append(1.0 / total)
            logs = jnp.broadcast_to(top + jnp.log(total), (L, L)).T
            ltb[i, m : m + 1, :] = logs[0:1]
    send_results(ltb, lto, lt_send, lt_recv)
    finish(3)
    for i in range(NS):
        width = (i + 1) * L
        heads = [
            jnp.dot(
                wts[m, i * L : (i + 1) * L, 0:width], fin[3, 0:width, :], preferred_element_type=jnp.float32
            )
            * totals[2 * i + m]
            for m in range(2)
        ]
        raw = heads[0] - lam * heads[1]
        scale = lax.rsqrt(jnp.mean(raw * raw, axis=1, keepdims=True) + 1e-05)
        atb[i] = (raw * scale * hgain_ref[...]).astype(jnp.bfloat16)

    send_results(atb, ato, at_send, at_recv)

    for copy in big:
        copy.wait()
    tiles = poutb.shape[0]
    width = D // tiles
    def term(src, i, columns):
        lhs = jnp.concatenate([src[h] for h in range(NS)], axis=1)
        return jnp.dot(lhs, wo[i, :, columns], preferred_element_type=jnp.float32)

    def tile_columns(n):
        return pl.ds(pl.multiple_of(n * width, width), width)

    def state_tile(n, carry):
        acc[:, tile_columns(n)] = term(sto, 0, tile_columns(n))
        return carry

    wait_results(sto, st_recv)
    lax.fori_loop(0, tiles, state_tile, 0)
    wait_results(lto, lt_recv)
    logs_out = pltpu.make_async_copy(lto, logt_ref.at[0], o_sem.at[tiles])
    logs_out.start()
    drain_send(wbuf.at[:, 0:7], w_send)
    drain_send(ysend, y_send)

    @pl.when(relays)
    def _():
        drain_send(xbuf, x_send)

    @pl.when(jnp.logical_not(relays))
    def _():
        drain_send(xbuf.at[0:7], x_send)

    drain_four(drain_send, shsend, sh_send)
    drain_four(drain_send, stb, st_send)
    wait_results(ato, at_recv)
    rows = L // NT
    mine = pl.ds(pl.multiple_of(c * rows, rows), rows)

    def p_copy(n):
        theirs = pl.ds(pl.multiple_of((1 - c) * rows, rows), rows)
        return remote(poutb.at[n, theirs], precb.at[n], p_send, p_recv.at[n], partner)

    def attn_tile(n, carry):
        part = acc[:, tile_columns(n)] + term(ato, 1, tile_columns(n))
        poutb[n] = part.astype(jnp.bfloat16)
        p_copy(n).start()
        return carry

    lax.fori_loop(0, tiles, attn_tile, 0)

    def out_copy(n):
        return pltpu.make_async_copy(obuf.at[n], mixed_ref.at[0, :, tile_columns(n)], o_sem.at[n])

    def last_tile(n, carry):
        p_copy(n).wait_recv()
        obuf[n] = (poutb[n, mine, :].astype(jnp.float32) + precb[n].astype(jnp.float32)).astype(jnp.bfloat16)
        out_copy(n).start()
        return carry

    lax.fori_loop(0, tiles, last_tile, 0)
    for n in range(tiles):
        out_copy(n).wait()
    logs_out.wait()
    drain_send(precb, p_send)
    drain_four(drain_send, atb, at_send)
    drain_four(drain_send, ltb, lt_send)


def fused_device(sizes, *args):
    (tokens, norm_gain, ws, wq, wk, wv, dre, dim, logstep, shift, inre, inim, outre, outim, skip, mix, hgain, wos, woa) = args
    NS, NT, L, D, CW = sizes
    KW, KB, HC = (D // 2, ws.shape[0], CW // NS)
    SEQ, G = (NS * L, HC // 16)
    tiles, pieces = (4, 2)
    bf, f32 = (jnp.bfloat16, jnp.float32)
    V = pltpu.VMEM
    DMA = pltpu.SemaphoreType.DMA
    vmem = pl.BlockSpec(memory_space=pltpu.VMEM)
    smem = pl.BlockSpec(memory_space=pltpu.SMEM)
    hbm = pl.BlockSpec(memory_space=pl.ANY)
    scratch = [
        V((L, 128), f32),
        V((L, 128), f32),
        V((L, KW), bf),
        V((2 * NS, L, KW), bf),
        V((4, KB, CW), bf),
        V((4, KW // KB, KB, HC), bf),
        V((4, SEQ, HC), f32),
        V((4, SEQ, HC), bf),
        V((4, SEQ, HC), bf),
        V((4, SEQ, HC), bf),
        V((NS, G, L), f32),
        V((NS, G, L), f32),
        V((2, G, 16, 64), f32),
        V((2, G, 16, 64), f32),
        V((4, G, 128), f32),
        V((4, G, L, 128), f32),
        V((G, 256, 256), bf),
        V((G, 256, 256), bf),
        V((NS, G, L), f32),
        V((SEQ, 128), f32),
        V((2, SEQ, SEQ), bf),
        V((NS, L, HC), bf),
        V((NS, L, HC), bf),
        V((NS, L, HC), bf),
        V((NS, L, HC), bf),
        V((NS, 2, L), f32),
        V((NS, 2, L), f32),
        V((2, CW, D), bf),
        V((L, D), f32),
        V((tiles, L, D // tiles), bf),
        V((tiles, L // NT, D // tiles), bf),
        V((tiles, L // NT, D // tiles), bf),
        DMA((tiles + 1,)),
        DMA((4,)),
        DMA((2,)),
        DMA((4,)),
        DMA((4,)),
        DMA((2,)),
        DMA,
        DMA((2, NS, pieces)),
        DMA,
        DMA((4, 4)),
        DMA,
        DMA((4,)),
    ]
    scratch += [DMA] * 9
    scratch += [DMA((tiles,))]
    call = pl.pallas_call(
        functools.partial(fused_kernel, sizes),
        out_shape=(
            jax.ShapeDtypeStruct((1, L // NT, D), bf),
            jax.ShapeDtypeStruct((1, NS, 2, L), f32),
        ),
        in_specs=[vmem, vmem, hbm, hbm, hbm, hbm, vmem, vmem, smem, vmem, hbm, hbm, hbm, hbm, vmem, smem, vmem, hbm, hbm],
        out_specs=(hbm, hbm),
        scratch_shapes=scratch,
        compiler_params=pltpu.CompilerParams(
            collective_id=0, has_side_effects=True, vmem_limit_bytes=67043328
        ),
    )
    mixed, logs = call(
        tokens, norm_gain.reshape(1, -1), ws, wq, wk, wv, dre, dim, logstep, shift,
        inre.transpose(0, 2, 1), inim.transpose(0, 2, 1), outre, outim,
        skip.reshape(1, -1), mix, hgain.reshape(1, -1), wos, woa,
    )
    return pl.pallas_call(
        hand_over,
        out_shape=(
            jax.ShapeDtypeStruct(mixed.shape, mixed.dtype),
            jax.ShapeDtypeStruct(logs.shape, logs.dtype),
        ),
        in_specs=[hbm, hbm],
        out_specs=(hbm, hbm),
        scratch_shapes=[V(mixed.shape, bf), V(logs.shape, f32), DMA((5,)), DMA((5,))],
    )(mixed, logs)


def hand_over(mixed_ref, logs_ref, mixed_out, logs_out, mixed_buf, logs_buf, in_sem, out_sem):
    rows = mixed_buf.shape[1] // 4
    views = [
        tuple(ref.at[:, pl.ds(i * rows, rows)] for ref in (mixed_ref, mixed_buf, mixed_out)) for i in range(4)
    ]
    views.append((logs_ref, logs_buf, logs_out))
    loads = [pltpu.make_async_copy(v[0], v[1], in_sem.at[i]) for i, v in enumerate(views)]
    stores = [pltpu.make_async_copy(v[1], v[2], out_sem.at[i]) for i, v in enumerate(views)]
    for copy in loads:
        copy.start()
    for load, store in zip(loads, stores):
        load.wait()
        store.start()
    for copy in stores:
        copy.wait()


def choose_device(sp, fs, tp, *args):
    tokens, ws, dre, inre, mix = (args[0], args[2], args[6], args[10], args[15])
    L, D = (tokens.shape[1], ws.shape[0] * sp * fs)
    CW = ws.shape[1]
    fits = (
        sp == 4
        and fs == 4
        and tp == 2
        and mix.shape[0] == sp
        and L == 128
        and CW == sp * 256
        and dre.shape == (sp * 16, 64)
        and inre.shape[2] == 16
        and D == sp * 4 * ws.shape[0]
        and ws.shape[0] % 128 == 0
    )
    if fits:
        return fused_device((sp, tp, L, D, CW), *args)
    return per_device(*args)


def solution(mesh):
    in_specs = (
        P("fs", "sp", "tp"),
        P(),
        P(("sp", "fs"), "tp"),
        P(("sp", "fs"), "tp"),
        P(("sp", "fs"), "tp"),
        P(("sp", "fs"), "tp"),
        P("tp", None),
        P("tp", None),
        P("tp"),
        P("fs", "tp", "sp"),
        P("tp", None, None),
        P("tp", None, None),
        P("tp", None, None),
        P("tp", None, None),
        P("tp"),
        P("tp"),
        P(),
        P("tp", None),
        P("tp", None),
    )
    out_specs = (P("fs", ("sp", "tp"), None), P("fs", "tp", None, "sp"))
    body = functools.partial(choose_device, mesh.shape["sp"], mesh.shape["fs"], mesh.shape["tp"])
    return jax.shard_map(
        body, mesh=mesh, in_specs=in_specs, out_specs=out_specs, check_vma=False
    )
```

```python
import functools
import math

import jax
import jax.numpy as jnp
from jax import lax
from jax.experimental import pallas as pl
from jax.experimental.pallas import tpu as pltpu
from jax.sharding import PartitionSpec as P


def prefix(x, axis, combine, identity):
    size, here = (lax.axis_size(axis), lax.axis_index(axis))
    everything = jax.tree.map(lambda part: lax.all_gather(part, axis), x)
    start = jax.tree.map(
        lambda part, zero: jnp.broadcast_to(jnp.asarray(zero, part.dtype), part.shape), x, identity
    )

    def hop(k, before):
        reached = k < here
        new = combine(before, jax.tree.map(lambda part: part[k], everything))
        return jax.tree.map(lambda a, b: jnp.where(reached, a, b), new, before)

    return lax.fori_loop(0, size, hop, start)


def compose(earlier, later):
    early_scale_re, early_scale_im, early_shift_re, early_shift_im = earlier
    late_scale_re, late_scale_im, late_shift_re, late_shift_im = later
    scale_re = late_scale_re * early_scale_re - late_scale_im * early_scale_im
    scale_im = late_scale_re * early_scale_im + late_scale_im * early_scale_re
    shift_re = late_scale_re * early_shift_re - late_scale_im * early_shift_im + late_shift_re
    shift_im = late_scale_re * early_shift_im + late_scale_im * early_shift_re + late_shift_im
    return (scale_re, scale_im, shift_re, shift_im)


def state_branch(
    state_in,
    decay_re,
    decay_im,
    log_step,
    decay_shift,
    in_re,
    in_im,
    output_real,
    output_imaginary,
    skip,
):
    upper_limit = lax.Precision.HIGHEST
    tok_rows = state_in.shape[0]
    group_count, state_size = decay_re.shape
    group_width = in_re.shape[2]
    flat_width = group_count * state_size
    step_size = jnp.exp(log_step)[:, None]
    numer_re = jnp.expm1(decay_re) * jnp.cos(decay_im) - 2.0 * jnp.sin(0.5 * decay_im) ** 2
    numer_im = jnp.exp(decay_re) * jnp.sin(decay_im)
    modulus = decay_re * decay_re + decay_im * decay_im
    coef_re = step_size * (numer_re * decay_re + numer_im * decay_im) / modulus
    coef_im = step_size * (numer_im * decay_re - numer_re * decay_im) / modulus
    matrix_re = coef_re[..., None] * in_re - coef_im[..., None] * in_im
    matrix_im = coef_re[..., None] * in_im + coef_im[..., None] * in_re
    inputs = state_in.astype(jnp.float32).reshape(tok_rows, group_count, group_width)
    flat_shape = (tok_rows, flat_width)
    drive_re = jnp.einsum("gpc,tgc->tgp", matrix_re, inputs, precision=upper_limit).reshape(
        flat_shape
    )
    drive_im = jnp.einsum("gpc,tgc->tgp", matrix_im, inputs, precision=upper_limit).reshape(
        flat_shape
    )
    magnitude = jnp.exp(decay_re[None] + decay_shift[0].T[:, :, None])
    factor_re = (magnitude * jnp.cos(decay_im)[None]).reshape(flat_shape)
    factor_im = (magnitude * jnp.sin(decay_im)[None]).reshape(flat_shape)
    span = math.gcd(tok_rows, 16)
    block_count = tok_rows // span

    def to_blocks(values):
        return values.reshape(block_count, span, flat_width).transpose(1, 0, 2)

    rows_in = tuple((to_blocks(values) for values in (factor_re, factor_im, drive_re, drive_im)))
    ones_blocks = jnp.ones((block_count, flat_width), jnp.float32)
    zero_blocks = jnp.zeros((block_count, flat_width), jnp.float32)

    def row_step(carry, row):
        joined = compose(carry, row)
        return (joined, joined)

    block_totals, local = lax.scan(
        row_step, (ones_blocks, zero_blocks, zero_blocks, zero_blocks), rows_in
    )
    ones_row = jnp.ones((flat_width,), jnp.float32)
    zero_row = jnp.zeros((flat_width,), jnp.float32)

    def block_step(carry, row):
        return (compose(carry, row), carry)

    totals, before = lax.scan(block_step, (ones_row, zero_row, zero_row, zero_row), block_totals)
    carried = prefix(totals, "sp", compose, (ones_row, zero_row, zero_row, zero_row))
    start_re, start_im = (carried[2], carried[3])
    enter_re = before[0] * start_re[None] - before[1] * start_im[None] + before[2]
    enter_im = before[0] * start_im[None] + before[1] * start_re[None] + before[3]
    state_real = local[2] + local[0] * enter_re[None] - local[1] * enter_im[None]
    state_imaginary = local[3] + local[0] * enter_im[None] + local[1] * enter_re[None]
    group_layout_shape = (tok_rows, group_count, state_size)
    state_real = state_real.transpose(1, 0, 2).reshape(group_layout_shape)
    state_imaginary = state_imaginary.transpose(1, 0, 2).reshape(group_layout_shape)
    result = (
        jnp.einsum("hsv,jhv->jhs", output_real, state_real, precision=upper_limit)
        - jnp.einsum("hsv,jhv->jhs", output_imaginary, state_imaginary, precision=upper_limit)
        + skip.reshape(group_count, group_width)[None] * inputs
    )
    return result.reshape(tok_rows, group_count * group_width).astype(jnp.bfloat16)


def attention_branch(queries, keys_local, values_local, mix_weight, head_gain):
    tok_rows = queries.shape[0]
    head_count = mix_weight.shape[0]
    head_dim = queries.shape[1] // (2 * head_count)
    value_dim = values_local.shape[1] // head_count
    scale = head_dim ** (-0.5)
    first_pos = lax.axis_index("sp") * tok_rows
    query_pos = first_pos + jnp.arange(tok_rows, dtype=jnp.int32)
    query_heads = queries.reshape(tok_rows, head_count, 2, head_dim)
    initial = (
        jnp.full((head_count, 2, tok_rows), -1e30, jnp.float32),
        jnp.zeros((head_count, 2, tok_rows), jnp.float32),
        jnp.zeros((head_count, 2, tok_rows, value_dim), jnp.float32),
    )
    key_piece = lax.all_gather(keys_local, "sp", axis=0, tiled=True)
    value_piece = lax.all_gather(values_local, "sp", axis=0, tiled=True)
    count = key_piece.shape[0]
    block = math.gcd(count, 512)

    def one_block(index, inner):
        run_max, run_total, run_accum = inner
        offset = index * block
        key_block = lax.dynamic_slice_in_dim(key_piece, offset, block, 0).reshape(
            block, head_count, 2, head_dim
        )
        value_block = lax.dynamic_slice_in_dim(value_piece, offset, block, 0).reshape(
            block, head_count, value_dim
        )
        key_pos = offset + jnp.arange(block, dtype=jnp.int32)
        scores = (
            jnp.einsum(
                "qhmd,khmd->hmqk", query_heads, key_block, preferred_element_type=jnp.float32
            )
            * scale
        )
        allowed = key_pos[None, :] <= query_pos[:, None]
        masked = jnp.where(allowed, scores, -1e30)
        new_max = jnp.maximum(run_max, jnp.max(masked, axis=-1))
        weights = jnp.where(allowed, jnp.exp(masked - new_max[..., None]), 0.0)
        rescale = jnp.exp(run_max - new_max)
        new_total = run_total * rescale + jnp.sum(weights, axis=-1)
        product = jnp.einsum(
            "hmqk,khd->hmqd",
            weights.astype(jnp.bfloat16),
            value_block,
            preferred_element_type=jnp.float32,
        )
        return (new_max, new_total, run_accum * rescale[..., None] + product)

    def visit(inner):
        return lax.fori_loop(0, count // block, one_block, inner)

    def keep_carry(inner):
        return inner

    maxima, totals, accum = lax.cond(
        jnp.int32(0) <= first_pos + tok_rows - 1, visit, keep_carry, initial
    )
    log_totals = maxima + jnp.log(totals)
    head_raw = (
        accum[:, 0] / totals[:, 0, :, None]
        - mix_weight[:, None, None] * accum[:, 1] / totals[:, 1, :, None]
    )
    normed_heads = (
        head_raw
        * lax.rsqrt(jnp.mean(head_raw * head_raw, axis=-1, keepdims=True) + 1e-05)
        * head_gain
    )
    attn_out = (
        normed_heads.transpose(1, 0, 2)
        .reshape(tok_rows, head_count * value_dim)
        .astype(jnp.bfloat16)
    )
    return (attn_out, log_totals)


def per_device(
    tokens,
    norm_gain,
    w_state_in,
    w_query,
    w_key,
    w_value,
    decay_re,
    decay_im,
    log_step,
    decay_shift,
    in_re,
    in_im,
    output_real,
    output_imaginary,
    skip,
    mix_weight,
    head_gain,
    w_out_state,
    w_out_attn,
):
    whole = lax.all_gather(tokens, "tp", axis=2, tiled=True)[0]
    floats = whole.astype(jnp.float32)
    normed = (
        floats * lax.rsqrt(jnp.mean(floats * floats, axis=-1, keepdims=True) + 1e-06) * norm_gain
    ).astype(jnp.bfloat16)
    pieces = (
        lax.all_gather(w_state_in, ("sp", "fs"), axis=0, tiled=True),
        lax.all_gather(w_query, ("sp", "fs"), axis=0, tiled=True),
        lax.all_gather(w_key, ("sp", "fs"), axis=0, tiled=True),
        lax.all_gather(w_value, ("sp", "fs"), axis=0, tiled=True),
    )
    sums = tuple((jnp.dot(normed, piece, preferred_element_type=jnp.float32) for piece in pieces))
    state_in = sums[0].astype(jnp.bfloat16)
    queries = sums[1].astype(jnp.bfloat16)
    keys_local = sums[2].astype(jnp.bfloat16)
    values_local = sums[3].astype(jnp.bfloat16)
    attn_out, log_totals = attention_branch(
        queries, keys_local, values_local, mix_weight, head_gain
    )
    state_out = state_branch(
        state_in,
        decay_re,
        decay_im,
        log_step,
        decay_shift,
        in_re,
        in_im,
        output_real,
        output_imaginary,
        skip,
    )
    summed = lax.psum_scatter(
        (
            jnp.dot(state_out, w_out_state, preferred_element_type=jnp.float32)
            + jnp.dot(attn_out, w_out_attn, preferred_element_type=jnp.float32)
        ).astype(jnp.bfloat16),
        "tp",
        scatter_dimension=0,
        tiled=True,
    )
    return (summed[None], log_totals[None])


def nt_dot(a, b):
    return lax.dot_general(a, b, (((1,), (1,)), ((), ())), preferred_element_type=jnp.float32)


def split_pair(x):
    high = x.astype(jnp.bfloat16)
    low = (x - high.astype(jnp.float32)).astype(jnp.bfloat16)
    return (high, low)


def small_expm1(x):
    total = jnp.ones_like(x)
    for n in range(9, 1, -1):
        total = 1.0 + total * x * (1.0 / n)
    return total * x


def fused_kernel(
    sizes,
    tok_ref,
    gain_ref,
    ws_ref,
    wq_ref,
    wk_ref,
    wv_ref,
    dre_ref,
    dim_ref,
    logstep_ref,
    shift_ref,
    inre_ref,
    inim_ref,
    outre_ref,
    outim_ref,
    skip_ref,
    mix_ref,
    hgain_ref,
    wos_ref,
    woa_ref,
    mixed_ref,
    logt_ref,
    stat_send,
    stat_recv,
    nbuf,
    xbuf,
    wl,
    wbuf,
    ykeep,
    ysend,
    yrecv,
    fin,
    shsend,
    shbuf,
    inbuf,
    outbuf,
    coef,
    etab,
    bcat,
    ccat,
    srow,
    yacc,
    wts,
    stb,
    atb,
    sto,
    ato,
    ltb,
    lto,
    wo,
    acc,
    poutb,
    precb,
    obuf,
    o_sem,
    loc_sem,
    wo_sem,
    w_loc,
    w_own,
    stat_sem,
    x_send,
    x_recv,
    w_send,
    w_recv,
    y_send,
    y_recv,
    sh_send,
    sh_recv,
    st_send,
    st_recv,
    at_send,
    at_recv,
    lt_send,
    lt_recv,
    p_send,
    p_recv,
):
    NS, NT, L, D, CW = sizes
    KW = D // 2
    KB = D // (NS * 4)
    FW = D // NT
    HC = CW // NS
    SEQ = NS * L
    G = HC // 16
    MESH = pl.DeviceIdType.MESH
    s, f, c = (lax.axis_index("sp"), lax.axis_index("fs"), lax.axis_index("tp"))
    zh, zl = (s // 2, lax.rem(s, 2))
    y, x = (f // 2, lax.rem(f, 2))
    s1 = s + 1 - 2 * zl
    s2 = lax.rem(s + 2, NS)
    fx = f + 1 - 2 * x
    fy = lax.rem(f + 2, 4)
    fd = 3 - f
    keep = zh + x - 2 * zh * x
    give = 1 - keep
    hq = 2 * x + zl
    home = 2 * y + keep
    partner = {"tp": 1 - c}

    def remote(src, dst, send, recv, where):
        return pltpu.make_async_remote_copy(
            src_ref=src, dst_ref=dst, send_sem=send, recv_sem=recv, device_id=where, device_id_type=MESH
        )

    def drain_send(part, sem):
        remote(part, part, sem, stat_sem.at[1], partner).wait_send()

    def drain_recv(part, sem):
        remote(part, part, stat_sem.at[0], sem, partner).wait_recv()

    def drain_four(drain, ref, sem):
        @pl.when(zh == 0)
        def _():
            drain(ref.at[0 : NS - 1], sem)

        @pl.when(zh == 1)
        def _():
            drain(ref, sem)

    g0 = pl.multiple_of(hq * G, G)
    kbo = zl * 4 + f

    def head_columns(h):
        return pl.ds(pl.multiple_of(h * HC, HC), HC)

    w_refs = (ws_ref, wq_ref, wk_ref, wv_ref)
    load_w = [pltpu.make_async_copy(ref, wl.at[m], w_loc.at[m]) for m, ref in enumerate(w_refs)]
    for copy in load_w:
        copy.start()
    own_w = [
        pltpu.make_async_copy(ref.at[:, head_columns(hq)], wbuf.at[m, kbo], w_own.at[m])
        for m, ref in enumerate(w_refs)
    ]
    for copy in own_w:
        copy.start()
    own_p = [
        pltpu.make_async_copy(ref.at[pl.ds(g0, G)], dst, loc_sem.at[i])
        for i, (ref, dst) in enumerate(
            (
                (inre_ref, inbuf.at[0]),
                (inim_ref, inbuf.at[1]),
                (outre_ref, outbuf.at[0]),
                (outim_ref, outbuf.at[1]),
            )
        )
    ]
    for copy in own_p:
        copy.start()
    big = [pltpu.make_async_copy(ref, wo.at[i], wo_sem.at[i]) for i, ref in enumerate((wos_ref, woa_ref))]
    for copy in big:
        copy.start()

    barrier = pltpu.get_barrier_semaphore()
    pl.semaphore_signal(barrier, inc=1, device_id={"fs": fy}, device_id_type=MESH)
    for k in range(NS):
        for there in (f, fx):
            for core in (c, 1 - c):
                if k == 0 and there is f and core is c:
                    continue
                pl.semaphore_signal(
                    barrier,
                    inc=1,
                    device_id={"sp": lax.rem(s + k, NS), "fs": there, "tp": core},
                    device_id_type=MESH,
                )
    tokens = tok_ref[0].astype(jnp.float32)
    square = jnp.sum(tokens * tokens, axis=1, keepdims=True)
    stat_send[...] = jnp.broadcast_to(square, (L, 128))
    pl.semaphore_wait(barrier, 4 * NS)
    stat = remote(stat_send, stat_recv, stat_sem.at[0], stat_sem.at[1], partner)
    stat.start()

    direct = (
        ((1 - x) * 2 + zl, {"fs": fx}),
        (x * 2 + 1 - zl, {"sp": s1}),
        ((1 - x) * 2 + 1 - zl, {"sp": s1, "fs": fx}),
    )
    arrive = (zl * 4 + fx, (1 - zl) * 4 + f, (1 - zl) * 4 + fx)
    def w_direct(m, j):
        h, where = direct[j]
        return remote(wl.at[m, :, head_columns(h)], wbuf.at[m, kbo], w_send, w_recv.at[m, j], where)

    def w_own_y(m):
        return remote(wl.at[m, :, head_columns(hq)], wbuf.at[m, kbo], w_send, w_recv.at[m, 3], {"fs": fy})

    def w_forward(m, j):
        part = wbuf.at[m, arrive[j]]
        return remote(part, part, w_send, w_recv.at[m, 3], {"fs": fy})

    def start_direct(m):
        for j in (2, 1, 0):
            w_direct(m, j).start()

    def forward_all(m):
        for j in range(3):
            drain_recv(wbuf.at[m, arrive[j]], w_recv.at[m, j])
            w_forward(m, j).start()

    def wait_across(m):
        drain_recv(wbuf.at[m, 0:4], w_recv.at[m, 3])

    load_w[0].wait()
    start_direct(0)
    w_own_y(0).start()
    load_w[1].wait()
    w_own_y(1).start()

    def shift_copy(xd, zd):
        zhd = xd + x - 2 * xd * x
        h = 2 * xd + zd
        return remote(
            shsend.at[h], shbuf.at[s], sh_send, sh_recv, {"sp": 2 * zhd + zd, "fs": 2 * y + xd}
        )

    def to_self(xd, zd):
        return jnp.logical_and(zh == 0, jnp.logical_and(x == xd, zl == zd))

    for h in range(NS):
        shsend[h] = shift_ref[0, h * G : (h + 1) * G, :]
    for xd in range(2):
        for zd in range(2):
            @pl.when(jnp.logical_not(to_self(xd, zd)))
            def _():
                shift_copy(xd, zd).start()

    @pl.when(zh == 0)
    def _():
        shbuf[s] = shsend[hq]

    stat.wait()
    mean = (square + stat_recv[:, 0:1]) * (1.0 / D)
    gain = gain_ref[:, pl.ds(pl.multiple_of(c * FW, FW), FW)]
    normed = (tok_ref[0].astype(jnp.float32) * lax.rsqrt(mean + 1e-06) * gain).astype(jnp.bfloat16)
    nbuf[...] = normed
    mine_half = c == zh
    q2 = 2 * (1 - zh) + zh
    order = (s, s1, q2, 2 * (1 - zh) + 1 - zh)
    duty = (zh, 1 - zh, zh, 1 - zh)
    near_s = 1 + c
    first_s = 2 - c
    near_core = jnp.where(s == first_s, c, 1 - c)

    parts = x_recv.shape[2]
    strip = L // parts

    def piece(n):
        return pl.ds(n * strip, strip)

    def x_copy(src, slot, q, n, where):
        return remote(src, xbuf.at[4 * slot + q, piece(n)], x_send, x_recv.at[slot, q, n], where)

    far_target = {"sp": near_s, "tp": near_core}
    pair_target = {"sp": s1, "tp": 1 - zh}

    def x_source(n, where):
        return x_copy(nbuf.at[piece(n)], x, s, n, where)

    def x_step(slot, i, n, where):
        q = order[i]
        return x_copy(xbuf.at[4 * slot + q, piece(n)], slot, q, n, where)

    def x_wait(slot, q, n):
        drain_recv(xbuf.at[4 * slot + q, piece(n)], x_recv.at[slot, q, n])

    relays = zl == 1 - zh

    @pl.when(mine_half)
    def _():
        xbuf[4 * x + s] = nbuf[...]
        for n in range(parts):
            for where in (pair_target, {"fs": fx}, partner):
                x_source(n, where).start()

    @pl.when(jnp.logical_not(mine_half))
    def _():
        for n in range(parts):
            x_source(n, far_target).start()

    def x_own(i):
        @pl.when(c == duty[i])
        def _():
            for n in range(parts):
                x_wait(x, order[i], n)
                if i >= 2:
                    @pl.when(relays)
                    def _():
                        x_step(x, i, n, {"sp": s1}).start()
                x_step(x, i, n, {"fs": fx}).start()
                x_step(x, i, n, partner).start()

    def x_other(i):
        @pl.when(c == duty[i])
        def _():
            for n in range(parts):
                x_wait(1 - x, order[i], n)
                x_step(1 - x, i, n, partner).start()

    def x_need(i):
        @pl.when(c != duty[i])
        def _():
            for n in range(parts):
                x_wait(x, order[i], n)

    def x_need_other(i):
        @pl.when(c != duty[i])
        def _():
            for n in range(parts):
                x_wait(1 - x, order[i], n)

    re16 = dre_ref[pl.ds(g0, G), :]
    im16 = dim_ref[pl.ds(g0, G), :]
    re16 = jnp.concatenate([re16, re16], axis=1)
    im16 = jnp.concatenate([im16, im16], axis=1)
    numer_re = small_expm1(re16) * jnp.cos(im16) - 2.0 * jnp.sin(0.5 * im16) ** 2
    numer_im = jnp.exp(re16) * jnp.sin(im16)
    modulus = re16 * re16 + im16 * im16
    coef[0] = re16
    coef[1] = im16
    coef[2] = (numer_re * re16 + numer_im * im16) / modulus
    coef[3] = (numer_im * re16 - numer_re * im16) / modulus
    for copy in own_p:
        copy.wait()
    lane = lax.broadcasted_iota(jnp.int32, (128, 16), 0)
    chan = lax.broadcasted_iota(jnp.int32, (128, 16), 1)
    steps = lax.broadcasted_iota(jnp.int32, (L, 128), 0).astype(jnp.float32) + 1.0

    def table(g, carry):
        zr = coef[0, pl.ds(g, 1), :]
        zi = coef[1, pl.ds(g, 1), :]
        step = jnp.exp(jnp.full((1, 128), logstep_ref[g0 + g], jnp.float32))
        cr = coef[2, pl.ds(g, 1), :] * step
        ci = coef[3, pl.ds(g, 1), :] * step
        angle = steps * zi
        cosine, sine = (jnp.cos(angle), jnp.sin(angle))
        shrink = jnp.exp(steps * zr)
        grow = jnp.exp(-(steps * zr))
        etab[0, g] = grow * (cosine * cr + sine * ci)
        etab[1, g] = grow * (cosine * ci - sine * cr)
        etab[2, g] = shrink * cosine
        etab[3, g] = shrink * sine
        pick = (lane == lax.rem(g, 8) * 16 + chan).astype(jnp.bfloat16)
        ir, ii = (inbuf[0, g], inbuf[1, g])
        raw = jnp.concatenate([ir, ii, -ii, ir], axis=1)
        hi, lo = split_pair(raw)
        bcat[g] = jnp.concatenate(
            [
                jnp.dot(pick, hi, preferred_element_type=jnp.float32).astype(jnp.bfloat16),
                jnp.dot(pick, lo, preferred_element_type=jnp.float32).astype(jnp.bfloat16),
            ],
            axis=0,
        )
        cr_, ci_ = (outbuf[0, g], outbuf[1, g])
        rawc = jnp.concatenate([cr_, -ci_, -ci_, -cr_], axis=1)
        hi, lo = split_pair(rawc)
        ccat[g] = jnp.concatenate(
            [
                jnp.dot(pick, hi, preferred_element_type=jnp.float32).astype(jnp.bfloat16),
                jnp.dot(pick, lo, preferred_element_type=jnp.float32).astype(jnp.bfloat16),
            ],
            axis=0,
        )
        return carry

    lax.fori_loop(0, G // 2, table, 0)
    forward_all(0)
    for m in (2, 3):
        load_w[m].wait()
        w_own_y(m).start()
    lax.fori_loop(G // 2, G, table, 0)
    x_own(1)
    x_own(2)
    x_own(3)
    start_direct(1)
    x_other(0)
    x_other(1)

    def weights(m):
        return wbuf[m].reshape(KW, HC)

    def y_copy(m, rows, i):
        return remote(ysend.at[m, rows], yrecv.at[m, rows], y_send, y_recv.at[m], {"sp": s2})

    def give_block(m, q, i):
        rows = pl.ds(pl.multiple_of(q * L, L), L)
        part = jnp.dot(xbuf[4 * give + q], weights(m), preferred_element_type=jnp.float32)
        ysend[m, rows] = part.astype(jnp.bfloat16)
        y_copy(m, rows, q).start()

    def give_all(m):
        def one(i, carry):
            rows = pl.ds(pl.multiple_of(i * 2 * L, 2 * L), 2 * L)
            part = jnp.dot(
                xbuf[pl.ds(4 * give + 2 * i, 2)].reshape(2 * L, KW), weights(m), preferred_element_type=jnp.float32
            )
            ysend[m, rows] = part.astype(jnp.bfloat16)
            y_copy(m, rows, i).start()
            return carry

        lax.fori_loop(0, 2, one, 0)

    def keep_all(m):
        def one(i, carry):
            rows = pl.ds(pl.multiple_of(i * 2 * L, 2 * L), 2 * L)
            ykeep[m, rows] = jnp.dot(
                xbuf[pl.ds(4 * keep + 2 * i, 2)].reshape(2 * L, KW), weights(m), preferred_element_type=jnp.float32
            )
            return carry

        lax.fori_loop(0, 2, one, 0)

    def finish(m):
        drain_recv(yrecv.at[m], y_recv.at[m])
        fin[m] = (ykeep[m] + yrecv[m].astype(jnp.float32)).astype(jnp.bfloat16)

    own_w[0].wait()
    wait_across(0)
    x_need(0)
    x_need(1)
    x_need_other(0)
    x_need_other(1)
    give_block(0, order[0], 0)
    give_block(0, order[1], 1)
    forward_all(1)
    start_direct(2)
    x_other(2)
    x_other(3)
    x_need(2)
    x_need(3)
    x_need_other(2)
    x_need_other(3)
    give_block(0, order[2], 2)
    give_block(0, order[3], 3)
    own_w[1].wait()
    wait_across(1)
    give_all(1)
    forward_all(2)
    start_direct(3)
    keep_all(0)
    keep_all(1)

    drain_four(drain_recv, shbuf, sh_recv)
    row_i = lax.broadcasted_iota(jnp.int32, (L, L), 0)
    col_i = lax.broadcasted_iota(jnp.int32, (L, L), 1)
    upper = (row_i <= col_i).astype(jnp.float32)
    for k in range(NS):
        srow[k] = jnp.dot(
            shbuf[k], upper, precision=lax.Precision.HIGHEST, preferred_element_type=jnp.float32
        )

    own_w[2].wait()
    wait_across(2)
    give_all(2)

    finish(0)
    sign = jnp.where(lax.broadcasted_iota(jnp.int32, (8, 128), 1) < 64, -1.0, 1.0)
    lower = row_i >= col_i

    def lane_block(b, carry):
        lanes = pl.ds(pl.multiple_of(b * 128, 128), 128)
        u = fin[0, :, lanes]
        uu = jnp.concatenate([u, u], axis=1)
        yacc[...] = jnp.zeros_like(yacc)

        def group(g8, inner):
            g = b * 8 + g8
            drives = jnp.dot(uu, bcat[g], preferred_element_type=jnp.float32)
            h = jnp.zeros((1, 128), jnp.float32)
            er, ei, fr, fi = (etab[0, g], etab[1, g], etab[2, g], etab[3, g])
            for k in range(NS):
                d = drives[k * L : (k + 1) * L]
                x = er * d[:, :128] + ei * d[:, 128:]
                xh, xl = split_pair(x)
                xx = jnp.concatenate([xh, xl], axis=1)
                rhs = jnp.concatenate([xx, xx], axis=0)
                sr = jnp.broadcast_to(srow[k, pl.ds(g, 1), :], (L, L))
                sc = sr.T
                mask = jnp.where(lower, jnp.exp(jnp.minimum(sc - sr, 0.0)), 0.0)
                mh, ml = split_pair(mask)
                w2 = jnp.dot(
                    jnp.concatenate([mh, ml], axis=1), rhs, preferred_element_type=jnp.float32
                )
                q = w2[:, :128] + w2[:, 128:] + jnp.exp(sc) * h
                p1 = q * fr
                p2 = q * fi
                tail = p1[L - 8 :] + sign * pltpu.roll(p2[L - 8 :], 64, 1)
                h = tail[7:8]
                ph, plow = split_pair(jnp.concatenate([p1, p2], axis=1))
                y2 = nt_dot(ph, ccat[g]) + nt_dot(plow, ccat[g])
                yacc[k * L : (k + 1) * L, :] += y2[:, :128] + y2[:, 128:]
            return inner

        lax.fori_loop(0, 8, group, 0)
        through = skip_ref[:, pl.ds(pl.multiple_of(hq * HC + b * 128, 128), 128)]
        out = (yacc[...] + through * u.astype(jnp.float32)).astype(jnp.bfloat16)
        for k in range(NS):
            stb[k, :, lanes] = out[k * L : (k + 1) * L]
        return carry

    half_blocks = HC // 256
    lax.fori_loop(0, half_blocks, lane_block, 0)
    forward_all(3)
    lax.fori_loop(half_blocks, HC // 128, lane_block, 0)
    own_w[3].wait()
    wait_across(3)
    give_all(3)

    def result_copy(src, dst, send, recv, d):
        return remote(src.at[d], dst.at[hq], send, recv, {"sp": d, "fs": home})

    def here(d):
        return jnp.logical_and(zh == 0, s == d)

    def send_results(src, dst, send, recv):
        for d in (3 - 3 * zh, 2 - zh, s1, s):
            @pl.when(jnp.logical_not(here(d)))
            def _():
                result_copy(src, dst, send, recv, d).start()

        @pl.when(zh == 0)
        def _():
            dst[hq] = src[s]

    def wait_results(dst, recv):
        drain_four(drain_recv, dst, recv)

    send_results(stb, sto, st_send, st_recv)
    keep_all(2)
    keep_all(3)

    hd = HC // 2
    finish(1)
    finish(2)
    lam = mix_ref[hq]
    totals = []
    for i in range(NS):
        width = (i + 1) * L
        for m in range(2):
            sc = nt_dot(
                fin[1, i * L : (i + 1) * L, m * hd : (m + 1) * hd], fin[2, 0:width, m * hd : (m + 1) * hd]
            ) * (hd ** (-0.5))
            qpos = lax.broadcasted_iota(jnp.int32, (L, width), 0) + i * L
            kpos = lax.broadcasted_iota(jnp.int32, (L, width), 1)
            allowed = kpos <= qpos
            sc = jnp.where(allowed, sc, -1e30)
            top = jnp.max(sc, axis=1, keepdims=True)
            weights_i = jnp.where(allowed, jnp.exp(sc - top), 0.0)
            total = jnp.sum(weights_i, axis=1, keepdims=True)
            wts[m, i * L : (i + 1) * L, 0:width] = weights_i.astype(jnp.bfloat16)
            totals.append(1.0 / total)
            logs = jnp.broadcast_to(top + jnp.log(total), (L, L)).T
            ltb[i, m : m + 1, :] = logs[0:1]
    send_results(ltb, lto, lt_send, lt_recv)
    finish(3)
    for i in range(NS):
        width = (i + 1) * L
        heads = [
            jnp.dot(
                wts[m, i * L : (i + 1) * L, 0:width], fin[3, 0:width, :], preferred_element_type=jnp.float32
            )
            * totals[2 * i + m]
            for m in range(2)
        ]
        raw = heads[0] - lam * heads[1]
        scale = lax.rsqrt(jnp.mean(raw * raw, axis=1, keepdims=True) + 1e-05)
        atb[i] = (raw * scale * hgain_ref[...]).astype(jnp.bfloat16)

    send_results(atb, ato, at_send, at_recv)

    for copy in big:
        copy.wait()
    tiles = poutb.shape[0]
    width = D // tiles
    def term(src, i, columns):
        lhs = jnp.concatenate([src[h] for h in range(NS)], axis=1)
        return jnp.dot(lhs, wo[i, :, columns], preferred_element_type=jnp.float32)

    def tile_columns(n):
        return pl.ds(pl.multiple_of(n * width, width), width)

    def state_tile(n, carry):
        acc[:, tile_columns(n)] = term(sto, 0, tile_columns(n))
        return carry

    wait_results(sto, st_recv)
    lax.fori_loop(0, tiles, state_tile, 0)
    wait_results(lto, lt_recv)
    logs_out = pltpu.make_async_copy(lto, logt_ref.at[0], o_sem.at[tiles])
    logs_out.start()
    drain_send(wbuf.at[:, 0:7], w_send)
    drain_send(ysend, y_send)

    @pl.when(relays)
    def _():
        drain_send(xbuf, x_send)

    @pl.when(jnp.logical_not(relays))
    def _():
        drain_send(xbuf.at[0:7], x_send)

    drain_four(drain_send, shsend, sh_send)
    drain_four(drain_send, stb, st_send)
    wait_results(ato, at_recv)
    rows = L // NT
    mine = pl.ds(pl.multiple_of(c * rows, rows), rows)

    def p_copy(n):
        theirs = pl.ds(pl.multiple_of((1 - c) * rows, rows), rows)
        return remote(poutb.at[n, theirs], precb.at[n], p_send, p_recv.at[n], partner)

    def attn_tile(n, carry):
        part = acc[:, tile_columns(n)] + term(ato, 1, tile_columns(n))
        poutb[n] = part.astype(jnp.bfloat16)
        p_copy(n).start()
        return carry

    lax.fori_loop(0, tiles, attn_tile, 0)

    def out_copy(n):
        return pltpu.make_async_copy(obuf.at[n], mixed_ref.at[0, :, tile_columns(n)], o_sem.at[n])

    def last_tile(n, carry):
        p_copy(n).wait_recv()
        obuf[n] = (poutb[n, mine, :].astype(jnp.float32) + precb[n].astype(jnp.float32)).astype(jnp.bfloat16)
        out_copy(n).start()
        return carry

    lax.fori_loop(0, tiles, last_tile, 0)
    for n in range(tiles):
        out_copy(n).wait()
    logs_out.wait()
    drain_send(precb, p_send)
    drain_four(drain_send, atb, at_send)
    drain_four(drain_send, ltb, lt_send)


def fused_device(sizes, *args):
    (tokens, norm_gain, ws, wq, wk, wv, dre, dim, logstep, shift, inre, inim, outre, outim, skip, mix, hgain, wos, woa) = args
    NS, NT, L, D, CW = sizes
    KW, KB, HC = (D // 2, ws.shape[0], CW // NS)
    SEQ, G = (NS * L, HC // 16)
    tiles, pieces = (4, 2)
    bf, f32 = (jnp.bfloat16, jnp.float32)
    V = pltpu.VMEM
    DMA = pltpu.SemaphoreType.DMA
    vmem = pl.BlockSpec(memory_space=pltpu.VMEM)
    smem = pl.BlockSpec(memory_space=pltpu.SMEM)
    hbm = pl.BlockSpec(memory_space=pl.ANY)
    scratch = [
        V((L, 128), f32),
        V((L, 128), f32),
        V((L, KW), bf),
        V((2 * NS, L, KW), bf),
        V((4, KB, CW), bf),
        V((4, KW // KB, KB, HC), bf),
        V((4, SEQ, HC), f32),
        V((4, SEQ, HC), bf),
        V((4, SEQ, HC), bf),
        V((4, SEQ, HC), bf),
        V((NS, G, L), f32),
        V((NS, G, L), f32),
        V((2, G, 16, 64), f32),
        V((2, G, 16, 64), f32),
        V((4, G, 128), f32),
        V((4, G, L, 128), f32),
        V((G, 256, 256), bf),
        V((G, 256, 256), bf),
        V((NS, G, L), f32),
        V((SEQ, 128), f32),
        V((2, SEQ, SEQ), bf),
        V((NS, L, HC), bf),
        V((NS, L, HC), bf),
        V((NS, L, HC), bf),
        V((NS, L, HC), bf),
        V((NS, 2, L), f32),
        V((NS, 2, L), f32),
        V((2, CW, D), bf),
        V((L, D), f32),
        V((tiles, L, D // tiles), bf),
        V((tiles, L // NT, D // tiles), bf),
        V((tiles, L // NT, D // tiles), bf),
        DMA((tiles + 1,)),
        DMA((4,)),
        DMA((2,)),
        DMA((4,)),
        DMA((4,)),
        DMA((2,)),
        DMA,
        DMA((2, NS, pieces)),
        DMA,
        DMA((4, 4)),
        DMA,
        DMA((4,)),
    ]
    scratch += [DMA] * 9
    scratch += [DMA((tiles,))]
    call = pl.pallas_call(
        functools.partial(fused_kernel, sizes),
        out_shape=(
            jax.ShapeDtypeStruct((1, L // NT, D), bf),
            jax.ShapeDtypeStruct((1, NS, 2, L), f32),
        ),
        in_specs=[vmem, vmem, hbm, hbm, hbm, hbm, vmem, vmem, smem, vmem, hbm, hbm, hbm, hbm, vmem, smem, vmem, hbm, hbm],
        out_specs=(hbm, hbm),
        scratch_shapes=scratch,
        compiler_params=pltpu.CompilerParams(
            collective_id=0, has_side_effects=True, vmem_limit_bytes=67043328
        ),
    )
    mixed, logs = call(
        tokens, norm_gain.reshape(1, -1), ws, wq, wk, wv, dre, dim, logstep, shift,
        inre.transpose(0, 2, 1), inim.transpose(0, 2, 1), outre, outim,
        skip.reshape(1, -1), mix, hgain.reshape(1, -1), wos, woa,
    )
    return pl.pallas_call(
        hand_over,
        out_shape=(
            jax.ShapeDtypeStruct(mixed.shape, mixed.dtype),
            jax.ShapeDtypeStruct(logs.shape, logs.dtype),
        ),
        in_specs=[hbm, hbm],
        out_specs=(hbm, hbm),
        scratch_shapes=[V(mixed.shape, bf), V(logs.shape, f32), DMA((5,)), DMA((5,))],
    )(mixed, logs)


def hand_over(mixed_ref, logs_ref, mixed_out, logs_out, mixed_buf, logs_buf, in_sem, out_sem):
    rows = mixed_buf.shape[1] // 4
    views = [
        tuple(ref.at[:, pl.ds(i * rows, rows)] for ref in (mixed_ref, mixed_buf, mixed_out)) for i in range(4)
    ]
    views.append((logs_ref, logs_buf, logs_out))
    loads = [pltpu.make_async_copy(v[0], v[1], in_sem.at[i]) for i, v in enumerate(views)]
    stores = [pltpu.make_async_copy(v[1], v[2], out_sem.at[i]) for i, v in enumerate(views)]
    for copy in loads:
        copy.start()
    for load, store in zip(loads, stores):
        load.wait()
        store.start()
    for copy in stores:
        copy.wait()


def choose_device(sp, fs, tp, *args):
    tokens, ws, dre, inre, mix = (args[0], args[2], args[6], args[10], args[15])
    L, D = (tokens.shape[1], ws.shape[0] * sp * fs)
    CW = ws.shape[1]
    fits = (
        sp == 4
        and fs == 4
        and tp == 2
        and mix.shape[0] == sp
        and L == 128
        and CW == sp * 256
        and dre.shape == (sp * 16, 64)
        and inre.shape[2] == 16
        and D == sp * 4 * ws.shape[0]
        and ws.shape[0] % 128 == 0
    )
    if fits:
        return fused_device((sp, tp, L, D, CW), *args)
    return per_device(*args)


def solution(mesh):
    in_specs = (
        P("fs", "sp", "tp"),
        P(),
        P(("sp", "fs"), "tp"),
        P(("sp", "fs"), "tp"),
        P(("sp", "fs"), "tp"),
        P(("sp", "fs"), "tp"),
        P("tp", None),
        P("tp", None),
        P("tp"),
        P("fs", "tp", "sp"),
        P("tp", None, None),
        P("tp", None, None),
        P("tp", None, None),
        P("tp", None, None),
        P("tp"),
        P("tp"),
        P(),
        P("tp", None),
        P("tp", None),
    )
    out_specs = (P("fs", ("sp", "tp"), None), P("fs", "tp", None, "sp"))
    body = functools.partial(choose_device, mesh.shape["sp"], mesh.shape["fs"], mesh.shape["tp"])
    return jax.shard_map(
        body, mesh=mesh, in_specs=in_specs, out_specs=out_specs, check_vma=False
    )
```

```python
import functools
import math

import jax
import jax.numpy as jnp
from jax import lax
from jax.experimental import pallas as pl
from jax.experimental.pallas import tpu as pltpu
from jax.sharding import PartitionSpec as P


def prefix(x, axis, combine, identity):
    size, here = (lax.axis_size(axis), lax.axis_index(axis))
    everything = jax.tree.map(lambda part: lax.all_gather(part, axis), x)
    start = jax.tree.map(
        lambda part, zero: jnp.broadcast_to(jnp.asarray(zero, part.dtype), part.shape), x, identity
    )

    def hop(k, before):
        reached = k < here
        new = combine(before, jax.tree.map(lambda part: part[k], everything))
        return jax.tree.map(lambda a, b: jnp.where(reached, a, b), new, before)

    return lax.fori_loop(0, size, hop, start)


def compose(earlier, later):
    early_scale_re, early_scale_im, early_shift_re, early_shift_im = earlier
    late_scale_re, late_scale_im, late_shift_re, late_shift_im = later
    scale_re = late_scale_re * early_scale_re - late_scale_im * early_scale_im
    scale_im = late_scale_re * early_scale_im + late_scale_im * early_scale_re
    shift_re = late_scale_re * early_shift_re - late_scale_im * early_shift_im + late_shift_re
    shift_im = late_scale_re * early_shift_im + late_scale_im * early_shift_re + late_shift_im
    return (scale_re, scale_im, shift_re, shift_im)


def state_branch(
    state_in,
    decay_re,
    decay_im,
    log_step,
    decay_shift,
    in_re,
    in_im,
    output_real,
    output_imaginary,
    skip,
):
    upper_limit = lax.Precision.HIGHEST
    tok_rows = state_in.shape[0]
    group_count, state_size = decay_re.shape
    group_width = in_re.shape[2]
    flat_width = group_count * state_size
    step_size = jnp.exp(log_step)[:, None]
    numer_re = jnp.expm1(decay_re) * jnp.cos(decay_im) - 2.0 * jnp.sin(0.5 * decay_im) ** 2
    numer_im = jnp.exp(decay_re) * jnp.sin(decay_im)
    modulus = decay_re * decay_re + decay_im * decay_im
    coef_re = step_size * (numer_re * decay_re + numer_im * decay_im) / modulus
    coef_im = step_size * (numer_im * decay_re - numer_re * decay_im) / modulus
    matrix_re = coef_re[..., None] * in_re - coef_im[..., None] * in_im
    matrix_im = coef_re[..., None] * in_im + coef_im[..., None] * in_re
    inputs = state_in.astype(jnp.float32).reshape(tok_rows, group_count, group_width)
    flat_shape = (tok_rows, flat_width)
    drive_re = jnp.einsum("gpc,tgc->tgp", matrix_re, inputs, precision=upper_limit).reshape(
        flat_shape
    )
    drive_im = jnp.einsum("gpc,tgc->tgp", matrix_im, inputs, precision=upper_limit).reshape(
        flat_shape
    )
    magnitude = jnp.exp(decay_re[None] + decay_shift[0].T[:, :, None])
    factor_re = (magnitude * jnp.cos(decay_im)[None]).reshape(flat_shape)
    factor_im = (magnitude * jnp.sin(decay_im)[None]).reshape(flat_shape)
    span = math.gcd(tok_rows, 16)
    block_count = tok_rows // span

    def to_blocks(values):
        return values.reshape(block_count, span, flat_width).transpose(1, 0, 2)

    rows_in = tuple((to_blocks(values) for values in (factor_re, factor_im, drive_re, drive_im)))
    ones_blocks = jnp.ones((block_count, flat_width), jnp.float32)
    zero_blocks = jnp.zeros((block_count, flat_width), jnp.float32)

    def row_step(carry, row):
        joined = compose(carry, row)
        return (joined, joined)

    block_totals, local = lax.scan(
        row_step, (ones_blocks, zero_blocks, zero_blocks, zero_blocks), rows_in
    )
    ones_row = jnp.ones((flat_width,), jnp.float32)
    zero_row = jnp.zeros((flat_width,), jnp.float32)

    def block_step(carry, row):
        return (compose(carry, row), carry)

    totals, before = lax.scan(block_step, (ones_row, zero_row, zero_row, zero_row), block_totals)
    carried = prefix(totals, "sp", compose, (ones_row, zero_row, zero_row, zero_row))
    start_re, start_im = (carried[2], carried[3])
    enter_re = before[0] * start_re[None] - before[1] * start_im[None] + before[2]
    enter_im = before[0] * start_im[None] + before[1] * start_re[None] + before[3]
    state_real = local[2] + local[0] * enter_re[None] - local[1] * enter_im[None]
    state_imaginary = local[3] + local[0] * enter_im[None] + local[1] * enter_re[None]
    group_layout_shape = (tok_rows, group_count, state_size)
    state_real = state_real.transpose(1, 0, 2).reshape(group_layout_shape)
    state_imaginary = state_imaginary.transpose(1, 0, 2).reshape(group_layout_shape)
    result = (
        jnp.einsum("hsv,jhv->jhs", output_real, state_real, precision=upper_limit)
        - jnp.einsum("hsv,jhv->jhs", output_imaginary, state_imaginary, precision=upper_limit)
        + skip.reshape(group_count, group_width)[None] * inputs
    )
    return result.reshape(tok_rows, group_count * group_width).astype(jnp.bfloat16)


def attention_branch(queries, keys_local, values_local, mix_weight, head_gain):
    tok_rows = queries.shape[0]
    head_count = mix_weight.shape[0]
    head_dim = queries.shape[1] // (2 * head_count)
    value_dim = values_local.shape[1] // head_count
    scale = head_dim ** (-0.5)
    first_pos = lax.axis_index("sp") * tok_rows
    query_pos = first_pos + jnp.arange(tok_rows, dtype=jnp.int32)
    query_heads = queries.reshape(tok_rows, head_count, 2, head_dim)
    initial = (
        jnp.full((head_count, 2, tok_rows), -1e30, jnp.float32),
        jnp.zeros((head_count, 2, tok_rows), jnp.float32),
        jnp.zeros((head_count, 2, tok_rows, value_dim), jnp.float32),
    )
    key_piece = lax.all_gather(keys_local, "sp", axis=0, tiled=True)
    value_piece = lax.all_gather(values_local, "sp", axis=0, tiled=True)
    count = key_piece.shape[0]
    block = math.gcd(count, 512)

    def one_block(index, inner):
        run_max, run_total, run_accum = inner
        offset = index * block
        key_block = lax.dynamic_slice_in_dim(key_piece, offset, block, 0).reshape(
            block, head_count, 2, head_dim
        )
        value_block = lax.dynamic_slice_in_dim(value_piece, offset, block, 0).reshape(
            block, head_count, value_dim
        )
        key_pos = offset + jnp.arange(block, dtype=jnp.int32)
        scores = (
            jnp.einsum(
                "qhmd,khmd->hmqk", query_heads, key_block, preferred_element_type=jnp.float32
            )
            * scale
        )
        allowed = key_pos[None, :] <= query_pos[:, None]
        masked = jnp.where(allowed, scores, -1e30)
        new_max = jnp.maximum(run_max, jnp.max(masked, axis=-1))
        weights = jnp.where(allowed, jnp.exp(masked - new_max[..., None]), 0.0)
        rescale = jnp.exp(run_max - new_max)
        new_total = run_total * rescale + jnp.sum(weights, axis=-1)
        product = jnp.einsum(
            "hmqk,khd->hmqd",
            weights.astype(jnp.bfloat16),
            value_block,
            preferred_element_type=jnp.float32,
        )
        return (new_max, new_total, run_accum * rescale[..., None] + product)

    def visit(inner):
        return lax.fori_loop(0, count // block, one_block, inner)

    def keep_carry(inner):
        return inner

    maxima, totals, accum = lax.cond(
        jnp.int32(0) <= first_pos + tok_rows - 1, visit, keep_carry, initial
    )
    log_totals = maxima + jnp.log(totals)
    head_raw = (
        accum[:, 0] / totals[:, 0, :, None]
        - mix_weight[:, None, None] * accum[:, 1] / totals[:, 1, :, None]
    )
    normed_heads = (
        head_raw
        * lax.rsqrt(jnp.mean(head_raw * head_raw, axis=-1, keepdims=True) + 1e-05)
        * head_gain
    )
    attn_out = (
        normed_heads.transpose(1, 0, 2)
        .reshape(tok_rows, head_count * value_dim)
        .astype(jnp.bfloat16)
    )
    return (attn_out, log_totals)


def per_device(
    tokens,
    norm_gain,
    w_state_in,
    w_query,
    w_key,
    w_value,
    decay_re,
    decay_im,
    log_step,
    decay_shift,
    in_re,
    in_im,
    output_real,
    output_imaginary,
    skip,
    mix_weight,
    head_gain,
    w_out_state,
    w_out_attn,
):
    whole = lax.all_gather(tokens, "tp", axis=2, tiled=True)[0]
    floats = whole.astype(jnp.float32)
    normed = (
        floats * lax.rsqrt(jnp.mean(floats * floats, axis=-1, keepdims=True) + 1e-06) * norm_gain
    ).astype(jnp.bfloat16)
    pieces = (
        lax.all_gather(w_state_in, ("sp", "fs"), axis=0, tiled=True),
        lax.all_gather(w_query, ("sp", "fs"), axis=0, tiled=True),
        lax.all_gather(w_key, ("sp", "fs"), axis=0, tiled=True),
        lax.all_gather(w_value, ("sp", "fs"), axis=0, tiled=True),
    )
    sums = tuple((jnp.dot(normed, piece, preferred_element_type=jnp.float32) for piece in pieces))
    state_in = sums[0].astype(jnp.bfloat16)
    queries = sums[1].astype(jnp.bfloat16)
    keys_local = sums[2].astype(jnp.bfloat16)
    values_local = sums[3].astype(jnp.bfloat16)
    attn_out, log_totals = attention_branch(
        queries, keys_local, values_local, mix_weight, head_gain
    )
    state_out = state_branch(
        state_in,
        decay_re,
        decay_im,
        log_step,
        decay_shift,
        in_re,
        in_im,
        output_real,
        output_imaginary,
        skip,
    )
    summed = lax.psum_scatter(
        (
            jnp.dot(state_out, w_out_state, preferred_element_type=jnp.float32)
            + jnp.dot(attn_out, w_out_attn, preferred_element_type=jnp.float32)
        ).astype(jnp.bfloat16),
        "tp",
        scatter_dimension=0,
        tiled=True,
    )
    return (summed[None], log_totals[None])


def nt_dot(a, b):
    return lax.dot_general(a, b, (((1,), (1,)), ((), ())), preferred_element_type=jnp.float32)


def split_pair(x):
    high = x.astype(jnp.bfloat16)
    low = (x - high.astype(jnp.float32)).astype(jnp.bfloat16)
    return (high, low)


def small_expm1(x):
    total = jnp.ones_like(x)
    for n in range(9, 1, -1):
        total = 1.0 + total * x * (1.0 / n)
    return total * x


def fused_kernel(
    sizes,
    tok_ref,
    gain_ref,
    ws_ref,
    wq_ref,
    wk_ref,
    wv_ref,
    dre_ref,
    dim_ref,
    logstep_ref,
    shift_ref,
    inre_ref,
    inim_ref,
    outre_ref,
    outim_ref,
    skip_ref,
    mix_ref,
    hgain_ref,
    wos_ref,
    woa_ref,
    mixed_ref,
    logt_ref,
    stat_send,
    stat_recv,
    nbuf,
    xbuf,
    wl,
    wbuf,
    ykeep,
    ysend,
    yrecv,
    fin,
    shsend,
    shbuf,
    inbuf,
    outbuf,
    coef,
    etab,
    bcat,
    ccat,
    srow,
    yacc,
    wts,
    stb,
    atb,
    sto,
    ato,
    ltb,
    lto,
    wo,
    acc,
    poutb,
    precb,
    obuf,
    o_sem,
    loc_sem,
    wo_sem,
    w_loc,
    w_own,
    stat_sem,
    x_send,
    x_recv,
    w_send,
    w_recv,
    y_send,
    y_recv,
    sh_send,
    sh_recv,
    st_send,
    st_recv,
    at_send,
    at_recv,
    lt_send,
    lt_recv,
    p_send,
    p_recv,
):
    NS, NT, L, D, CW = sizes
    KW = D // 2
    KB = D // (NS * 4)
    FW = D // NT
    HC = CW // NS
    SEQ = NS * L
    G = HC // 16
    MESH = pl.DeviceIdType.MESH
    s, f, c = (lax.axis_index("sp"), lax.axis_index("fs"), lax.axis_index("tp"))
    zh, zl = (s // 2, lax.rem(s, 2))
    y, x = (f // 2, lax.rem(f, 2))
    s1 = s + 1 - 2 * zl
    s2 = lax.rem(s + 2, NS)
    fx = f + 1 - 2 * x
    fy = lax.rem(f + 2, 4)
    fd = 3 - f
    keep = zh + x - 2 * zh * x
    give = 1 - keep
    hq = 2 * x + zl
    home = 2 * y + keep
    partner = {"tp": 1 - c}

    def remote(src, dst, send, recv, where):
        return pltpu.make_async_remote_copy(
            src_ref=src, dst_ref=dst, send_sem=send, recv_sem=recv, device_id=where, device_id_type=MESH
        )

    def drain_send(part, sem):
        remote(part, part, sem, stat_sem.at[1], partner).wait_send()

    def drain_recv(part, sem):
        remote(part, part, stat_sem.at[0], sem, partner).wait_recv()

    def drain_four(drain, ref, sem):
        @pl.when(zh == 0)
        def _():
            drain(ref.at[0 : NS - 1], sem)

        @pl.when(zh == 1)
        def _():
            drain(ref, sem)

    g0 = pl.multiple_of(hq * G, G)
    kbo = zl * 4 + f

    def head_columns(h):
        return pl.ds(pl.multiple_of(h * HC, HC), HC)

    w_refs = (ws_ref, wq_ref, wk_ref, wv_ref)
    load_w = [pltpu.make_async_copy(ref, wl.at[m], w_loc.at[m]) for m, ref in enumerate(w_refs)]
    for copy in load_w:
        copy.start()
    own_w = [
        pltpu.make_async_copy(ref.at[:, head_columns(hq)], wbuf.at[m, kbo], w_own.at[m])
        for m, ref in enumerate(w_refs)
    ]
    for copy in own_w:
        copy.start()
    own_p = [
        pltpu.make_async_copy(ref.at[pl.ds(g0, G)], dst, loc_sem.at[i])
        for i, (ref, dst) in enumerate(
            (
                (inre_ref, inbuf.at[0]),
                (inim_ref, inbuf.at[1]),
                (outre_ref, outbuf.at[0]),
                (outim_ref, outbuf.at[1]),
            )
        )
    ]
    for copy in own_p:
        copy.start()
    big = [pltpu.make_async_copy(ref, wo.at[i], wo_sem.at[i]) for i, ref in enumerate((wos_ref, woa_ref))]
    for copy in big:
        copy.start()

    barrier = pltpu.get_barrier_semaphore()
    pl.semaphore_signal(barrier, inc=1, device_id={"fs": fy}, device_id_type=MESH)
    for k in range(NS):
        for there in (f, fx):
            for core in (c, 1 - c):
                if k == 0 and there is f and core is c:
                    continue
                pl.semaphore_signal(
                    barrier,
                    inc=1,
                    device_id={"sp": lax.rem(s + k, NS), "fs": there, "tp": core},
                    device_id_type=MESH,
                )
    tokens = tok_ref[0].astype(jnp.float32)
    square = jnp.sum(tokens * tokens, axis=1, keepdims=True)
    stat_send[...] = jnp.broadcast_to(square, (L, 128))
    pl.semaphore_wait(barrier, 4 * NS)
    stat = remote(stat_send, stat_recv, stat_sem.at[0], stat_sem.at[1], partner)
    stat.start()

    direct = (
        ((1 - x) * 2 + zl, {"fs": fx}),
        (x * 2 + 1 - zl, {"sp": s1}),
        ((1 - x) * 2 + 1 - zl, {"sp": s1, "fs": fx}),
    )
    arrive = (zl * 4 + fx, (1 - zl) * 4 + f, (1 - zl) * 4 + fx)
    def w_direct(m, j):
        h, where = direct[j]
        return remote(wl.at[m, :, head_columns(h)], wbuf.at[m, kbo], w_send, w_recv.at[m, j], where)

    def w_own_y(m):
        return remote(wl.at[m, :, head_columns(hq)], wbuf.at[m, kbo], w_send, w_recv.at[m, 3], {"fs": fy})

    def w_forward(m, j):
        part = wbuf.at[m, arrive[j]]
        return remote(part, part, w_send, w_recv.at[m, 3], {"fs": fy})

    def start_direct(m):
        for j in (2, 1, 0):
            w_direct(m, j).start()

    def forward_all(m):
        for j in range(3):
            drain_recv(wbuf.at[m, arrive[j]], w_recv.at[m, j])
            w_forward(m, j).start()

    def wait_across(m):
        drain_recv(wbuf.at[m, 0:4], w_recv.at[m, 3])

    load_w[0].wait()
    start_direct(0)
    w_own_y(0).start()
    load_w[1].wait()
    w_own_y(1).start()

    def shift_copy(xd, zd):
        zhd = xd + x - 2 * xd * x
        h = 2 * xd + zd
        return remote(
            shsend.at[h], shbuf.at[s], sh_send, sh_recv, {"sp": 2 * zhd + zd, "fs": 2 * y + xd}
        )

    def to_self(xd, zd):
        return jnp.logical_and(zh == 0, jnp.logical_and(x == xd, zl == zd))

    for h in range(NS):
        shsend[h] = shift_ref[0, h * G : (h + 1) * G, :]
    for xd in range(2):
        for zd in range(2):
            @pl.when(jnp.logical_not(to_self(xd, zd)))
            def _():
                shift_copy(xd, zd).start()

    @pl.when(zh == 0)
    def _():
        shbuf[s] = shsend[hq]

    stat.wait()
    mean = (square + stat_recv[:, 0:1]) * (1.0 / D)
    gain = gain_ref[:, pl.ds(pl.multiple_of(c * FW, FW), FW)]
    normed = (tok_ref[0].astype(jnp.float32) * lax.rsqrt(mean + 1e-06) * gain).astype(jnp.bfloat16)
    nbuf[...] = normed
    mine_half = c == zh
    q2 = 2 * (1 - zh) + zh
    order = (s, s1, q2, 2 * (1 - zh) + 1 - zh)
    duty = (zh, 1 - zh, zh, 1 - zh)
    near_s = 1 + c
    first_s = 2 - c
    near_core = jnp.where(s == first_s, c, 1 - c)

    parts = x_recv.shape[2]
    strip = L // parts

    def piece(n):
        return pl.ds(n * strip, strip)

    def x_copy(src, slot, q, n, where):
        return remote(src, xbuf.at[4 * slot + q, piece(n)], x_send, x_recv.at[slot, q, n], where)

    far_target = {"sp": near_s, "tp": near_core}
    pair_target = {"sp": s1, "tp": 1 - zh}

    def x_source(n, where):
        return x_copy(nbuf.at[piece(n)], x, s, n, where)

    def x_step(slot, i, n, where):
        q = order[i]
        return x_copy(xbuf.at[4 * slot + q, piece(n)], slot, q, n, where)

    def x_wait(slot, q, n):
        drain_recv(xbuf.at[4 * slot + q, piece(n)], x_recv.at[slot, q, n])

    relays = zl == 1 - zh

    @pl.when(mine_half)
    def _():
        xbuf[4 * x + s] = nbuf[...]
        for n in range(parts):
            for where in (pair_target, {"fs": fx}, partner):
                x_source(n, where).start()

    @pl.when(jnp.logical_not(mine_half))
    def _():
        for n in range(parts):
            x_source(n, far_target).start()

    def x_own(i):
        @pl.when(c == duty[i])
        def _():
            for n in range(parts):
                x_wait(x, order[i], n)
                if i >= 2:
                    @pl.when(relays)
                    def _():
                        x_step(x, i, n, {"sp": s1}).start()
                x_step(x, i, n, {"fs": fx}).start()
                x_step(x, i, n, partner).start()

    def x_other(i):
        @pl.when(c == duty[i])
        def _():
            for n in range(parts):
                x_wait(1 - x, order[i], n)
                x_step(1 - x, i, n, partner).start()

    def x_need(i):
        @pl.when(c != duty[i])
        def _():
            for n in range(parts):
                x_wait(x, order[i], n)

    def x_need_other(i):
        @pl.when(c != duty[i])
        def _():
            for n in range(parts):
                x_wait(1 - x, order[i], n)

    re16 = dre_ref[pl.ds(g0, G), :]
    im16 = dim_ref[pl.ds(g0, G), :]
    re16 = jnp.concatenate([re16, re16], axis=1)
    im16 = jnp.concatenate([im16, im16], axis=1)
    numer_re = small_expm1(re16) * jnp.cos(im16) - 2.0 * jnp.sin(0.5 * im16) ** 2
    numer_im = jnp.exp(re16) * jnp.sin(im16)
    modulus = re16 * re16 + im16 * im16
    coef[0] = re16
    coef[1] = im16
    coef[2] = (numer_re * re16 + numer_im * im16) / modulus
    coef[3] = (numer_im * re16 - numer_re * im16) / modulus
    for copy in own_p:
        copy.wait()
    lane = lax.broadcasted_iota(jnp.int32, (128, 16), 0)
    chan = lax.broadcasted_iota(jnp.int32, (128, 16), 1)
    steps = lax.broadcasted_iota(jnp.int32, (L, 128), 0).astype(jnp.float32) + 1.0

    def table(g, carry):
        zr = coef[0, pl.ds(g, 1), :]
        zi = coef[1, pl.ds(g, 1), :]
        step = jnp.exp(jnp.full((1, 128), logstep_ref[g0 + g], jnp.float32))
        cr = coef[2, pl.ds(g, 1), :] * step
        ci = coef[3, pl.ds(g, 1), :] * step
        angle = steps * zi
        cosine, sine = (jnp.cos(angle), jnp.sin(angle))
        shrink = jnp.exp(steps * zr)
        grow = jnp.exp(-(steps * zr))
        etab[0, g] = grow * (cosine * cr + sine * ci)
        etab[1, g] = grow * (cosine * ci - sine * cr)
        etab[2, g] = shrink * cosine
        etab[3, g] = shrink * sine
        pick = (lane == lax.rem(g, 8) * 16 + chan).astype(jnp.bfloat16)
        ir, ii = (inbuf[0, g], inbuf[1, g])
        raw = jnp.concatenate([ir, ii, -ii, ir], axis=1)
        hi, lo = split_pair(raw)
        bcat[g] = jnp.concatenate(
            [
                jnp.dot(pick, hi, preferred_element_type=jnp.float32).astype(jnp.bfloat16),
                jnp.dot(pick, lo, preferred_element_type=jnp.float32).astype(jnp.bfloat16),
            ],
            axis=0,
        )
        cr_, ci_ = (outbuf[0, g], outbuf[1, g])
        rawc = jnp.concatenate([cr_, -ci_, -ci_, -cr_], axis=1)
        hi, lo = split_pair(rawc)
        ccat[g] = jnp.concatenate(
            [
                jnp.dot(pick, hi, preferred_element_type=jnp.float32).astype(jnp.bfloat16),
                jnp.dot(pick, lo, preferred_element_type=jnp.float32).astype(jnp.bfloat16),
            ],
            axis=0,
        )
        return carry

    lax.fori_loop(0, G // 2, table, 0)
    forward_all(0)
    for m in (2, 3):
        load_w[m].wait()
        w_own_y(m).start()
    lax.fori_loop(G // 2, G, table, 0)
    x_own(1)
    x_own(2)
    x_own(3)
    start_direct(1)
    x_other(0)
    x_other(1)

    def weights(m):
        return wbuf[m].reshape(KW, HC)

    def y_copy(m, rows, i):
        return remote(ysend.at[m, rows], yrecv.at[m, rows], y_send, y_recv.at[m], {"sp": s2})

    def give_block(m, q, i):
        rows = pl.ds(pl.multiple_of(q * L, L), L)
        part = jnp.dot(xbuf[4 * give + q], weights(m), preferred_element_type=jnp.float32)
        ysend[m, rows] = part.astype(jnp.bfloat16)
        y_copy(m, rows, q).start()

    def give_all(m):
        def one(i, carry):
            rows = pl.ds(pl.multiple_of(i * 2 * L, 2 * L), 2 * L)
            part = jnp.dot(
                xbuf[pl.ds(4 * give + 2 * i, 2)].reshape(2 * L, KW), weights(m), preferred_element_type=jnp.float32
            )
            ysend[m, rows] = part.astype(jnp.bfloat16)
            y_copy(m, rows, i).start()
            return carry

        lax.fori_loop(0, 2, one, 0)

    def keep_all(m):
        def one(i, carry):
            rows = pl.ds(pl.multiple_of(i * 2 * L, 2 * L), 2 * L)
            ykeep[m, rows] = jnp.dot(
                xbuf[pl.ds(4 * keep + 2 * i, 2)].reshape(2 * L, KW), weights(m), preferred_element_type=jnp.float32
            )
            return carry

        lax.fori_loop(0, 2, one, 0)

    def finish(m):
        drain_recv(yrecv.at[m], y_recv.at[m])
        fin[m] = (ykeep[m] + yrecv[m].astype(jnp.float32)).astype(jnp.bfloat16)

    own_w[0].wait()
    wait_across(0)
    x_need(0)
    x_need(1)
    x_need_other(0)
    x_need_other(1)
    give_block(0, order[0], 0)
    give_block(0, order[1], 1)
    forward_all(1)
    start_direct(2)
    x_other(2)
    x_other(3)
    x_need(2)
    x_need(3)
    x_need_other(2)
    x_need_other(3)
    give_block(0, order[2], 2)
    give_block(0, order[3], 3)
    own_w[1].wait()
    wait_across(1)
    give_all(1)
    forward_all(2)
    start_direct(3)
    keep_all(0)
    keep_all(1)

    drain_four(drain_recv, shbuf, sh_recv)
    row_i = lax.broadcasted_iota(jnp.int32, (L, L), 0)
    col_i = lax.broadcasted_iota(jnp.int32, (L, L), 1)
    upper = (row_i <= col_i).astype(jnp.float32)
    for k in range(NS):
        srow[k] = jnp.dot(
            shbuf[k], upper, precision=lax.Precision.HIGHEST, preferred_element_type=jnp.float32
        )

    own_w[2].wait()
    wait_across(2)
    give_all(2)

    finish(0)
    sign = jnp.where(lax.broadcasted_iota(jnp.int32, (8, 128), 1) < 64, -1.0, 1.0)
    lower = row_i >= col_i

    def lane_block(b, carry):
        lanes = pl.ds(pl.multiple_of(b * 128, 128), 128)
        u = fin[0, :, lanes]
        uu = jnp.concatenate([u, u], axis=1)
        yacc[...] = jnp.zeros_like(yacc)

        def group(g8, inner):
            g = b * 8 + g8
            drives = jnp.dot(uu, bcat[g], preferred_element_type=jnp.float32)
            h = jnp.zeros((1, 128), jnp.float32)
            er, ei, fr, fi = (etab[0, g], etab[1, g], etab[2, g], etab[3, g])
            for k in range(NS):
                d = drives[k * L : (k + 1) * L]
                x = er * d[:, :128] + ei * d[:, 128:]
                xh, xl = split_pair(x)
                xx = jnp.concatenate([xh, xl], axis=1)
                rhs = jnp.concatenate([xx, xx], axis=0)
                sr = jnp.broadcast_to(srow[k, pl.ds(g, 1), :], (L, L))
                sc = sr.T
                mask = jnp.where(lower, jnp.exp(jnp.minimum(sc - sr, 0.0)), 0.0)
                mh, ml = split_pair(mask)
                w2 = jnp.dot(
                    jnp.concatenate([mh, ml], axis=1), rhs, preferred_element_type=jnp.float32
                )
                q = w2[:, :128] + w2[:, 128:] + jnp.exp(sc) * h
                p1 = q * fr
                p2 = q * fi
                tail = p1[L - 8 :] + sign * pltpu.roll(p2[L - 8 :], 64, 1)
                h = tail[7:8]
                ph, plow = split_pair(jnp.concatenate([p1, p2], axis=1))
                y2 = nt_dot(ph, ccat[g]) + nt_dot(plow, ccat[g])
                yacc[k * L : (k + 1) * L, :] += y2[:, :128] + y2[:, 128:]
            return inner

        lax.fori_loop(0, 8, group, 0)
        through = skip_ref[:, pl.ds(pl.multiple_of(hq * HC + b * 128, 128), 128)]
        out = (yacc[...] + through * u.astype(jnp.float32)).astype(jnp.bfloat16)
        for k in range(NS):
            stb[k, :, lanes] = out[k * L : (k + 1) * L]
        return carry

    half_blocks = HC // 256
    lax.fori_loop(0, half_blocks, lane_block, 0)
    forward_all(3)
    lax.fori_loop(half_blocks, HC // 128, lane_block, 0)
    own_w[3].wait()
    wait_across(3)
    give_all(3)

    def result_copy(src, dst, send, recv, d):
        return remote(src.at[d], dst.at[hq], send, recv, {"sp": d, "fs": home})

    def here(d):
        return jnp.logical_and(zh == 0, s == d)

    def send_results(src, dst, send, recv):
        for d in (3 - 3 * zh, 2 - zh, s1, s):
            @pl.when(jnp.logical_not(here(d)))
            def _():
                result_copy(src, dst, send, recv, d).start()

        @pl.when(zh == 0)
        def _():
            dst[hq] = src[s]

    def wait_results(dst, recv):
        drain_four(drain_recv, dst, recv)

    send_results(stb, sto, st_send, st_recv)
    keep_all(2)
    keep_all(3)

    hd = HC // 2
    finish(1)
    finish(2)
    lam = mix_ref[hq]
    totals = []
    for i in range(NS):
        width = (i + 1) * L
        for m in range(2):
            sc = nt_dot(
                fin[1, i * L : (i + 1) * L, m * hd : (m + 1) * hd], fin[2, 0:width, m * hd : (m + 1) * hd]
            ) * (hd ** (-0.5))
            qpos = lax.broadcasted_iota(jnp.int32, (L, width), 0) + i * L
            kpos = lax.broadcasted_iota(jnp.int32, (L, width), 1)
            allowed = kpos <= qpos
            sc = jnp.where(allowed, sc, -1e30)
            top = jnp.max(sc, axis=1, keepdims=True)
            weights_i = jnp.where(allowed, jnp.exp(sc - top), 0.0)
            total = jnp.sum(weights_i, axis=1, keepdims=True)
            wts[m, i * L : (i + 1) * L, 0:width] = weights_i.astype(jnp.bfloat16)
            totals.append(1.0 / total)
            logs = jnp.broadcast_to(top + jnp.log(total), (L, L)).T
            ltb[i, m : m + 1, :] = logs[0:1]
    send_results(ltb, lto, lt_send, lt_recv)
    finish(3)
    for i in range(NS):
        width = (i + 1) * L
        heads = [
            jnp.dot(
                wts[m, i * L : (i + 1) * L, 0:width], fin[3, 0:width, :], preferred_element_type=jnp.float32
            )
            * totals[2 * i + m]
            for m in range(2)
        ]
        raw = heads[0] - lam * heads[1]
        scale = lax.rsqrt(jnp.mean(raw * raw, axis=1, keepdims=True) + 1e-05)
        atb[i] = (raw * scale * hgain_ref[...]).astype(jnp.bfloat16)

    send_results(atb, ato, at_send, at_recv)

    for copy in big:
        copy.wait()
    tiles = poutb.shape[0]
    width = D // tiles
    def term(src, i, columns):
        lhs = jnp.concatenate([src[h] for h in range(NS)], axis=1)
        return jnp.dot(lhs, wo[i, :, columns], preferred_element_type=jnp.float32)

    def tile_columns(n):
        return pl.ds(pl.multiple_of(n * width, width), width)

    def state_tile(n, carry):
        acc[:, tile_columns(n)] = term(sto, 0, tile_columns(n))
        return carry

    wait_results(sto, st_recv)
    lax.fori_loop(0, tiles, state_tile, 0)
    wait_results(lto, lt_recv)
    logs_out = pltpu.make_async_copy(lto, logt_ref.at[0], o_sem.at[tiles])
    logs_out.start()
    drain_send(wbuf.at[:, 0:7], w_send)
    drain_send(ysend, y_send)

    @pl.when(relays)
    def _():
        drain_send(xbuf, x_send)

    @pl.when(jnp.logical_not(relays))
    def _():
        drain_send(xbuf.at[0:7], x_send)

    drain_four(drain_send, shsend, sh_send)
    drain_four(drain_send, stb, st_send)
    wait_results(ato, at_recv)
    rows = L // NT
    mine = pl.ds(pl.multiple_of(c * rows, rows), rows)

    def p_copy(n):
        theirs = pl.ds(pl.multiple_of((1 - c) * rows, rows), rows)
        return remote(poutb.at[n, theirs], precb.at[n], p_send, p_recv.at[n], partner)

    def attn_tile(n, carry):
        part = acc[:, tile_columns(n)] + term(ato, 1, tile_columns(n))
        poutb[n] = part.astype(jnp.bfloat16)
        p_copy(n).start()
        return carry

    lax.fori_loop(0, tiles, attn_tile, 0)

    def out_copy(n):
        return pltpu.make_async_copy(obuf.at[n], mixed_ref.at[0, :, tile_columns(n)], o_sem.at[n])

    def last_tile(n, carry):
        p_copy(n).wait_recv()
        obuf[n] = (poutb[n, mine, :].astype(jnp.float32) + precb[n].astype(jnp.float32)).astype(jnp.bfloat16)
        out_copy(n).start()
        return carry

    lax.fori_loop(0, tiles, last_tile, 0)
    for n in range(tiles):
        out_copy(n).wait()
    logs_out.wait()
    drain_send(precb, p_send)
    drain_four(drain_send, atb, at_send)
    drain_four(drain_send, ltb, lt_send)


def fused_device(sizes, *args):
    (tokens, norm_gain, ws, wq, wk, wv, dre, dim, logstep, shift, inre, inim, outre, outim, skip, mix, hgain, wos, woa) = args
    NS, NT, L, D, CW = sizes
    KW, KB, HC = (D // 2, ws.shape[0], CW // NS)
    SEQ, G = (NS * L, HC // 16)
    tiles, pieces = (2, 2)
    bf, f32 = (jnp.bfloat16, jnp.float32)
    V = pltpu.VMEM
    DMA = pltpu.SemaphoreType.DMA
    vmem = pl.BlockSpec(memory_space=pltpu.VMEM)
    smem = pl.BlockSpec(memory_space=pltpu.SMEM)
    hbm = pl.BlockSpec(memory_space=pl.ANY)
    scratch = [
        V((L, 128), f32),
        V((L, 128), f32),
        V((L, KW), bf),
        V((2 * NS, L, KW), bf),
        V((4, KB, CW), bf),
        V((4, KW // KB, KB, HC), bf),
        V((4, SEQ, HC), f32),
        V((4, SEQ, HC), bf),
        V((4, SEQ, HC), bf),
        V((4, SEQ, HC), bf),
        V((NS, G, L), f32),
        V((NS, G, L), f32),
        V((2, G, 16, 64), f32),
        V((2, G, 16, 64), f32),
        V((4, G, 128), f32),
        V((4, G, L, 128), f32),
        V((G, 256, 256), bf),
        V((G, 256, 256), bf),
        V((NS, G, L), f32),
        V((SEQ, 128), f32),
        V((2, SEQ, SEQ), bf),
        V((NS, L, HC), bf),
        V((NS, L, HC), bf),
        V((NS, L, HC), bf),
        V((NS, L, HC), bf),
        V((NS, 2, L), f32),
        V((NS, 2, L), f32),
        V((2, CW, D), bf),
        V((L, D), f32),
        V((tiles, L, D // tiles), bf),
        V((tiles, L // NT, D // tiles), bf),
        V((tiles, L // NT, D // tiles), bf),
        DMA((tiles + 1,)),
        DMA((4,)),
        DMA((2,)),
        DMA((4,)),
        DMA((4,)),
        DMA((2,)),
        DMA,
        DMA((2, NS, pieces)),
        DMA,
        DMA((4, 4)),
        DMA,
        DMA((4,)),
    ]
    scratch += [DMA] * 9
    scratch += [DMA((tiles,))]
    call = pl.pallas_call(
        functools.partial(fused_kernel, sizes),
        out_shape=(
            jax.ShapeDtypeStruct((1, L // NT, D), bf),
            jax.ShapeDtypeStruct((1, NS, 2, L), f32),
        ),
        in_specs=[vmem, vmem, hbm, hbm, hbm, hbm, vmem, vmem, smem, vmem, hbm, hbm, hbm, hbm, vmem, smem, vmem, hbm, hbm],
        out_specs=(hbm, hbm),
        scratch_shapes=scratch,
        compiler_params=pltpu.CompilerParams(
            collective_id=0, has_side_effects=True, vmem_limit_bytes=67043328
        ),
    )
    mixed, logs = call(
        tokens, norm_gain.reshape(1, -1), ws, wq, wk, wv, dre, dim, logstep, shift,
        inre.transpose(0, 2, 1), inim.transpose(0, 2, 1), outre, outim,
        skip.reshape(1, -1), mix, hgain.reshape(1, -1), wos, woa,
    )
    return pl.pallas_call(
        hand_over,
        out_shape=(
            jax.ShapeDtypeStruct(mixed.shape, mixed.dtype),
            jax.ShapeDtypeStruct(logs.shape, logs.dtype),
        ),
        in_specs=[hbm, hbm],
        out_specs=(hbm, hbm),
        scratch_shapes=[V(mixed.shape, bf), V(logs.shape, f32), DMA((3,)), DMA((3,))],
    )(mixed, logs)


def hand_over(mixed_ref, logs_ref, mixed_out, logs_out, mixed_buf, logs_buf, in_sem, out_sem):
    rows = mixed_buf.shape[1] // 2
    views = [
        tuple(ref.at[:, pl.ds(i * rows, rows)] for ref in (mixed_ref, mixed_buf, mixed_out)) for i in range(2)
    ]
    views.append((logs_ref, logs_buf, logs_out))
    loads = [pltpu.make_async_copy(v[0], v[1], in_sem.at[i]) for i, v in enumerate(views)]
    stores = [pltpu.make_async_copy(v[1], v[2], out_sem.at[i]) for i, v in enumerate(views)]
    for copy in loads:
        copy.start()
    for load, store in zip(loads, stores):
        load.wait()
        store.start()
    for copy in stores:
        copy.wait()


def choose_device(sp, fs, tp, *args):
    tokens, ws, dre, inre, mix = (args[0], args[2], args[6], args[10], args[15])
    L, D = (tokens.shape[1], ws.shape[0] * sp * fs)
    CW = ws.shape[1]
    fits = (
        sp == 4
        and fs == 4
        and tp == 2
        and mix.shape[0] == sp
        and L == 128
        and CW == sp * 256
        and dre.shape == (sp * 16, 64)
        and inre.shape[2] == 16
        and D == sp * 4 * ws.shape[0]
        and ws.shape[0] % 128 == 0
    )
    if fits:
        return fused_device((sp, tp, L, D, CW), *args)
    return per_device(*args)


def solution(mesh):
    in_specs = (
        P("fs", "sp", "tp"),
        P(),
        P(("sp", "fs"), "tp"),
        P(("sp", "fs"), "tp"),
        P(("sp", "fs"), "tp"),
        P(("sp", "fs"), "tp"),
        P("tp", None),
        P("tp", None),
        P("tp"),
        P("fs", "tp", "sp"),
        P("tp", None, None),
        P("tp", None, None),
        P("tp", None, None),
        P("tp", None, None),
        P("tp"),
        P("tp"),
        P(),
        P("tp", None),
        P("tp", None),
    )
    out_specs = (P("fs", ("sp", "tp"), None), P("fs", "tp", None, "sp"))
    body = functools.partial(choose_device, mesh.shape["sp"], mesh.shape["fs"], mesh.shape["tp"])
    return jax.shard_map(
        body, mesh=mesh, in_specs=in_specs, out_specs=out_specs, check_vma=False
    )
```
